32 devices in a mesh: sp: 8 (over z, y), tp: 4 (over x, core).
Axes of the slice: x: 2, y: 2, z: 4, core: 2. Of those that a mesh axis runs over, the one named last changes fastest.
Arguments:
- latent: bfloat16 [4096, 2048], P(('sp', 'tp')), may hold values from -6 to 6
- context: bfloat16 [512, 2048], P('sp'), may hold values from -6 to 6
- condition: float32 [2048], replicated, may hold values from -6 to 6
- context_condition: float32 [2048], replicated, may hold values from -6 to 6
- norm_gain: float32 [2048], replicated, may hold values from 0.1 to 1.9
- shift_weight: bfloat16 [2048, 2048], P('sp', 'tp'), may hold values from -0.21875 to 0.21875
- scale_weight: bfloat16 [2048, 2048], P('sp', 'tp'), may hold values from -0.21875 to 0.21875
- gate_weight: bfloat16 [2048, 2048], P('sp', 'tp'), may hold values from -0.21875 to 0.21875
- query_weight: bfloat16 [2048, 1024], P(None, 'tp'), may hold values from -1 to 1
- key_weight: bfloat16 [2048, 512], P(None, 'tp'), may hold values from -1 to 1
- value_weight: bfloat16 [2048, 512], P(None, 'tp'), may hold values from -0.125 to 0.125
- query_gain: float32 [64], replicated, may hold values from 0.1 to 7.8
- key_gain: float32 [64], replicated, may hold values from 0.1 to 7.8
- output_weight: bfloat16 [1024, 2048], replicated, may hold values from -1 to 1
Outputs:
- updated: bfloat16 [4096, 2048], P(('sp', 'tp'))
The draws below stay inside these ranges and needn't reach their ends.
All inputs are finite; a program needn't handle non-finite values.
Results may differ from the reference program's by a relative error of at most 0.012.
The reference program's roundings to bfloat16 on the way count: a program that leaves them out, or rounds other values in their place, can miss the bound.
Values may be sent and summed in bfloat16 or wider, within the bound.
No kernel may reach another device: no remote copies, remote signals or barrier semaphores. Data moves between devices by JAX's collectives and lax.ppermute only.
A program may use at most 64 MiB of HBM per device.

```python
import math
import jax
import jax.numpy as jnp
from jax import lax

D = 2048
HQ = 16
KVH = 8
CHANNEL_SPAN = 64
GRID_W = 64
PREFIX_ITEMS = 512
HIDDEN_ITEMS = 4096


def query_base(key):
    return jax.random.truncated_normal(jax.random.fold_in(key, 101), -6.0, 6.0, (D, HQ * CHANNEL_SPAN), jnp.float32) * D ** (-0.5)


def draw_query_weight(key, part):
    return query_base(key).astype(jnp.bfloat16)


def draw_key_weight(key, part):
    fresh = jax.random.truncated_normal(jax.random.fold_in(key, 102), -6.0, 6.0, (D, KVH * CHANNEL_SPAN), jnp.float32) * D ** (-0.5)
    return fresh.astype(jnp.bfloat16)


def gain_draw(key, salt):
    return 3.0 * (1.0 + 0.18 * jax.random.truncated_normal(jax.random.fold_in(key, salt), -5.0, 5.0, (CHANNEL_SPAN,), jnp.float32))


def draw_query_gain(key, part):
    return gain_draw(key, 103)


def draw_key_gain(key, part):
    return gain_draw(key, 104)


def draw_output_weight(key, part):
    base = jax.random.truncated_normal(jax.random.fold_in(key, 105), -6.0, 6.0, (HQ * CHANNEL_SPAN, D), jnp.float32)
    return (base * (HQ * CHANNEL_SPAN) ** (-0.5)).astype(jnp.bfloat16)


def steps_of(own_key, dims, pieces, low, largest):
    loudness = 1.0
    for dim, parts in pieces:
        draws = jax.random.uniform(jax.random.fold_in(jax.random.fold_in(own_key, 6), dim), (parts,), jnp.float32, low / len(pieces), largest / len(pieces))
        loudness = loudness * jnp.repeat(jnp.exp(draws), dims[dim] // parts).reshape((-1,) + (1,) * (len(dims) - 1 - dim))
    return loudness


def scatter_about(key, extent, deviation, most, shards=(), kind=jnp.bfloat16):
    entries = deviation * jax.random.normal(key, extent, jnp.float32)
    if shards:
        entries = entries * steps_of(key, extent, shards, -0.22, 0.18)
    return jnp.clip(entries, -most, most).astype(kind)


def setup_inputs(seed: int = 0) -> dict:
    keys = jax.random.split(jax.random.key(seed), 15)
    latent = scatter_about(keys[0], (HIDDEN_ITEMS, D), 1.0, 6.0, ((0, 32),))
    context = scatter_about(keys[1], (PREFIX_ITEMS, D), 1.0, 6.0, ((0, 8),))
    condition = scatter_about(keys[2], (D,), 1.0, 6.0, (), jnp.float32)
    context_condition = scatter_about(keys[3], (D,), 1.0, 6.0, (), jnp.float32)
    norm_gain = jnp.clip(1.0 + 0.18 * jax.random.normal(keys[4], (D,), jnp.float32), 0.1, 1.9)
    shift_weight = scatter_about(keys[5], (D, D), (D // 3) ** -0.5, 0.21875, ((0, 8), (1, 4)))
    scale_weight = scatter_about(keys[6], (D, D), (D // 3) ** -0.5, 0.21875, ((0, 8), (1, 4)))
    gate_weight = scatter_about(keys[7], (D, D), (D // 3) ** -0.5, 0.21875, ((0, 8), (1, 4)))
    query_weight = draw_query_weight(jax.random.fold_in(keys[14], 71), 0)
    key_weight = draw_key_weight(jax.random.fold_in(keys[14], 71), 0)
    value_weight = scatter_about(keys[10], (D, KVH * CHANNEL_SPAN), D ** -0.5, 0.125, ((1, 4),))
    query_gain = draw_query_gain(jax.random.fold_in(keys[14], 71), 0)
    key_gain = draw_key_gain(jax.random.fold_in(keys[14], 71), 0)
    output_weight = draw_output_weight(jax.random.fold_in(keys[14], 71), 0)
    return {"latent": latent, "context": context, "condition": condition, "context_condition": context_condition, "norm_gain": norm_gain, "shift_weight": shift_weight, "scale_weight": scale_weight, "gate_weight": gate_weight, "query_weight": query_weight, "key_weight": key_weight, "value_weight": value_weight, "query_gain": query_gain, "key_gain": key_gain, "output_weight": output_weight}


epsilon = 1e-06
rope_base = 10000.0

def modulate(tok_rows, norm_gain, shift_row, scale_row):
    wide = tok_rows.astype(jnp.float32)
    normed = wide * lax.rsqrt(lax.optimization_barrier(jnp.mean(wide * wide, axis=-1, keepdims=True)) + epsilon)
    return (normed * norm_gain * (1.0 + scale_row) + shift_row).astype(jnp.bfloat16)

def headnorm(raw, gain, heads):
    field = raw.reshape(raw.shape[0], heads, -1)
    return field * lax.rsqrt(lax.optimization_barrier(jnp.mean(field * field, axis=-1, keepdims=True)) + epsilon) * gain

def rotate(field, places):
    count = field.shape[0]
    heads = field.shape[1]
    quarter = field.shape[2] // 4
    grid_row = (places // GRID_W).astype(jnp.float32)
    grid_col = (places % GRID_W).astype(jnp.float32)
    inverse = rope_base ** (-jnp.arange(quarter, dtype=jnp.float32) / quarter)
    angles = jnp.stack([grid_row[:, None] * inverse, grid_col[:, None] * inverse], axis=1)[:, None]
    cosine = jnp.cos(angles)
    sine = jnp.sin(angles)
    matcher_content_couples = field.reshape(count, heads, 2, 2, quarter)
    first = matcher_content_couples[:, :, :, 0]
    second = matcher_content_couples[:, :, :, 1]
    turned = jnp.stack([first * cosine - second * sine, second * cosine + first * sine], axis=3)
    return turned.reshape(count, heads, 4 * quarter)

def reference(latent, context, condition, context_condition, norm_gain, shift_weight, scale_weight, gate_weight, query_weight, key_weight, value_weight, query_gain, key_gain, output_weight):
    activated = jax.nn.silu(jnp.stack([condition, context_condition])).astype(jnp.bfloat16)
    shifts = jnp.dot(activated, shift_weight, preferred_element_type=jnp.float32)
    scales = jnp.dot(activated, scale_weight, preferred_element_type=jnp.float32)
    gates = jnp.dot(activated, gate_weight, preferred_element_type=jnp.float32)
    hidden = modulate(latent, norm_gain, shifts[0], scales[0])
    context_hidden = modulate(context, norm_gain, shifts[1], scales[1])
    places = jnp.arange(HIDDEN_ITEMS, dtype=jnp.int32)
    probe_entries = rotate(headnorm(jnp.dot(hidden, query_weight, preferred_element_type=jnp.float32), query_gain, HQ), places).astype(jnp.bfloat16)
    latent_keys = rotate(headnorm(jnp.dot(hidden, key_weight, preferred_element_type=jnp.float32), key_gain, KVH), places).astype(jnp.bfloat16)
    latent_values = jnp.dot(hidden, value_weight, preferred_element_type=jnp.float32).astype(jnp.bfloat16).reshape(HIDDEN_ITEMS, KVH, CHANNEL_SPAN)
    context_keys = headnorm(jnp.dot(context_hidden, key_weight, preferred_element_type=jnp.float32), key_gain, KVH).astype(jnp.bfloat16)
    context_values = jnp.dot(context_hidden, value_weight, preferred_element_type=jnp.float32).astype(jnp.bfloat16).reshape(PREFIX_ITEMS, KVH, CHANNEL_SPAN)
    matcher_pieces = jnp.concatenate([context_keys, latent_keys], axis=0).astype(jnp.float32)
    value_rows = jnp.concatenate([context_values, latent_values], axis=0).astype(jnp.float32)
    prefix_mapped = math.log(HIDDEN_ITEMS / (2.0 * PREFIX_ITEMS))
    similarity_offset = jnp.concatenate([jnp.full((PREFIX_ITEMS,), prefix_mapped, jnp.float32), jnp.zeros((HIDDEN_ITEMS,), jnp.float32)])
    group_size = HQ // KVH
    group_extent = math.gcd(HIDDEN_ITEMS, 256)
    grouped = probe_entries.reshape(HIDDEN_ITEMS // group_extent, group_extent, KVH, group_size, CHANNEL_SPAN)

    def one_block(probe_segment):
        similarity_matrix = jnp.einsum('dmvk,hmk->dmvh', probe_segment.astype(jnp.float32), matcher_pieces) * CHANNEL_SPAN ** (-0.5) + similarity_offset
        row_peak = lax.optimization_barrier(jnp.max(similarity_matrix, axis=-1, keepdims=True))
        shares = jnp.exp(similarity_matrix - row_peak)
        row_total = lax.optimization_barrier(jnp.sum(shares, axis=-1))
        rounded = lax.optimization_barrier(shares.astype(jnp.bfloat16)).astype(jnp.float32)
        weighted = jnp.einsum('qkgn,nkd->qkgd', rounded, value_rows)
        return (weighted / row_total[..., None]).astype(jnp.bfloat16)
    attended = lax.map(one_block, grouped).reshape(HIDDEN_ITEMS, HQ * CHANNEL_SPAN)
    projected = jnp.dot(attended, output_weight, preferred_element_type=jnp.float32)
    return (latent.astype(jnp.float32) + gates[0] * projected).astype(jnp.bfloat16)
```

```python
import math

import jax
import jax.numpy as jnp
from jax import lax
from jax.experimental import pallas as pl
from jax.experimental.pallas import tpu as pltpu
from jax.sharding import PartitionSpec as P

CHANNEL_SPAN = 64
GRID_W = 64


epsilon = 1e-06
rope_base = 10000.0


def modulate(tok_rows, norm_gain, shift_row, scale_row):
    wide = tok_rows.astype(jnp.float32)
    normed = wide * lax.rsqrt(jnp.mean(wide * wide, axis=-1, keepdims=True) + epsilon)
    return (normed * norm_gain * (1.0 + scale_row) + shift_row).astype(jnp.bfloat16)


def headnorm(raw, gain, heads):
    field = raw.reshape(raw.shape[0], heads, -1)
    return field * lax.rsqrt(jnp.mean(field * field, axis=-1, keepdims=True) + epsilon) * gain


def rotate(field, places):
    count = field.shape[0]
    heads = field.shape[1]
    quarter = field.shape[2] // 4
    grid_row = (places // GRID_W).astype(jnp.float32)
    grid_col = (places % GRID_W).astype(jnp.float32)
    inverse = rope_base ** (-jnp.arange(quarter, dtype=jnp.float32) / quarter)
    angles = jnp.stack([grid_row[:, None] * inverse, grid_col[:, None] * inverse], axis=1)[:, None]
    cosine = jnp.cos(angles)
    sine = jnp.sin(angles)
    matcher_content_couples = field.reshape(count, heads, 2, 2, quarter)
    first = matcher_content_couples[:, :, :, 0]
    second = matcher_content_couples[:, :, :, 1]
    turned = jnp.stack([first * cosine - second * sine, second * cosine + first * sine], axis=3)
    return turned.reshape(count, heads, 4 * quarter)


def process_probe_group(
    accumulator_carry, probe_entries, matcher_content_couples, similarity_offset
):
    row_peak, row_total, weighted = accumulator_carry
    kv_heads = probe_entries.shape[1]
    head_size = probe_entries.shape[3]
    pair_width = kv_heads * head_size
    matcher_pieces = matcher_content_couples[:, :pair_width].reshape(
        matcher_content_couples.shape[0], kv_heads, head_size
    )
    value_rows = matcher_content_couples[:, pair_width:].reshape(
        matcher_content_couples.shape[0], kv_heads, head_size
    )
    similarity_matrix = (
        jnp.einsum(
            "dmvk,hmk->dmvh", probe_entries, matcher_pieces, preferred_element_type=jnp.float32
        )
        * head_size ** (-0.5)
        + similarity_offset
    )
    new_peak = jnp.maximum(row_peak, jnp.max(similarity_matrix, axis=-1))
    shares = jnp.exp(similarity_matrix - new_peak[..., None])
    shrink = jnp.exp(row_peak - new_peak)
    row_total = row_total * shrink + jnp.sum(shares, axis=-1)
    weighted = weighted * shrink[..., None] + jnp.einsum(
        "qkgn,nkd->qkgd",
        shares.astype(jnp.bfloat16),
        value_rows,
        preferred_element_type=jnp.float32,
    )
    return (new_peak, row_total, weighted)


def group_walker(accumulator_carry, probe_entries, matcher_content_couples, similarity_offset):
    pair_count = matcher_content_couples.shape[0]
    probe_group_total = -(-pair_count // 2048)
    while pair_count % probe_group_total:
        probe_group_total += 1
    if probe_group_total == 1:
        return process_probe_group(
            accumulator_carry, probe_entries, matcher_content_couples, similarity_offset
        )
    group_extent = pair_count // probe_group_total

    def scan_step(inner, slices):
        return (process_probe_group(inner, probe_entries, slices[0], slices[1]), None)

    result, unused = lax.scan(
        scan_step,
        accumulator_carry,
        (
            matcher_content_couples.reshape(
                probe_group_total, group_extent, matcher_content_couples.shape[1]
            ),
            similarity_offset.reshape(probe_group_total, group_extent),
        ),
    )
    return result


def general_device(
    latent,
    context,
    condition,
    context_condition,
    norm_gain,
    shift_weight,
    scale_weight,
    gate_weight,
    query_weight,
    key_weight,
    value_weight,
    query_gain,
    key_gain,
    output_weight,
):
    head_split = lax.axis_size("tp")
    seq_index = lax.axis_index("sp")
    head_index = lax.axis_index("tp")
    row_slab = shift_weight.shape[0]
    columns = shift_weight.shape[1]
    conditions = jnp.stack([condition, context_condition])
    activated = jax.nn.silu(
        lax.dynamic_slice_in_dim(conditions, seq_index * row_slab, row_slab, 1)
    ).astype(jnp.bfloat16)
    part_shift = jnp.dot(activated, shift_weight, preferred_element_type=jnp.float32)
    part_scale = jnp.dot(activated, scale_weight, preferred_element_type=jnp.float32)
    part_gate = jnp.dot(activated, gate_weight, preferred_element_type=jnp.float32)

    def widen(member):
        blank = jnp.zeros((2, columns * head_split), jnp.float32)
        return lax.dynamic_update_slice_in_dim(blank, member, head_index * columns, 1)

    shifts, scales, gates = lax.psum(
        (widen(part_shift), widen(part_scale), widen(part_gate)), ("sp", "tp")
    )
    own_rows = latent.shape[0]
    tok_count = own_rows * head_split
    ctx_rows = context.shape[0]
    hidden = modulate(latent, norm_gain, shifts[0], scales[0])
    context_hidden = modulate(context, norm_gain, shifts[1], scales[1])
    q_heads = query_weight.shape[1] // CHANNEL_SPAN
    kv_heads = key_weight.shape[1] // CHANNEL_SPAN
    group_size = q_heads // kv_heads
    q_width = q_heads * CHANNEL_SPAN
    kv_width = kv_heads * CHANNEL_SPAN
    joined_weight = jnp.concatenate([query_weight, key_weight, value_weight], axis=1)
    projected = jnp.dot(
        lax.all_gather(hidden, "tp", axis=0, tiled=True),
        joined_weight,
        preferred_element_type=jnp.float32,
    )
    places = seq_index * tok_count + jnp.arange(tok_count, dtype=jnp.int32)
    probe_entries = rotate(headnorm(projected[:, :q_width], query_gain, q_heads), places).astype(
        jnp.bfloat16
    )
    probe_entries = probe_entries.reshape(tok_count, kv_heads, group_size, CHANNEL_SPAN)
    latent_keys = rotate(
        headnorm(projected[:, q_width : q_width + kv_width], key_gain, kv_heads), places
    ).astype(jnp.bfloat16)
    latent_values = projected[:, q_width + kv_width :].astype(jnp.bfloat16)
    own_pairs = jnp.concatenate([latent_keys.reshape(tok_count, kv_width), latent_values], axis=1)
    ctx_projected = jnp.dot(
        context_hidden, joined_weight[:, q_width:], preferred_element_type=jnp.float32
    )
    ctx_keys = (
        headnorm(ctx_projected[:, :kv_width], key_gain, kv_heads)
        .astype(jnp.bfloat16)
        .reshape(ctx_rows, kv_width)
    )
    ctx_pairs = jnp.concatenate(
        [ctx_keys, ctx_projected[:, kv_width:].astype(jnp.bfloat16)], axis=1
    )
    prefix_mapped = math.log(tok_count / (2.0 * ctx_rows))
    stat_shape = (tok_count, kv_heads, group_size)
    start_state = (
        jnp.full(stat_shape, -jnp.inf, jnp.float32),
        jnp.zeros(stat_shape, jnp.float32),
        jnp.zeros(stat_shape + (CHANNEL_SPAN,), jnp.float32),
    )
    ctx_whole = lax.all_gather(ctx_pairs, "sp", axis=0, tiled=True)
    ctx_state = group_walker(
        start_state,
        probe_entries,
        ctx_whole,
        jnp.full((ctx_whole.shape[0],), prefix_mapped, jnp.float32),
    )
    key_piece = lax.all_gather(own_pairs, "sp", axis=0, tiled=True)
    final_state = group_walker(
        ctx_state, probe_entries, key_piece, jnp.zeros((key_piece.shape[0],), jnp.float32)
    )
    row_peak, row_total, weighted = final_state
    attended = (weighted / row_total[..., None]).astype(jnp.bfloat16).reshape(tok_count, q_width)
    branch = jnp.dot(
        lax.all_to_all(attended, "tp", split_axis=0, concat_axis=1, tiled=True),
        output_weight,
        preferred_element_type=jnp.float32,
    )
    return (latent.astype(jnp.float32) + gates[0] * branch).astype(jnp.bfloat16)


LOG2E = math.log2(math.e)


def whole_spec():
    return pl.BlockSpec(memory_space=pltpu.VMEM)


def kernel_call(body, out_shape, count, flops, scratch=()):
    return pl.pallas_call(
        body,
        out_shape=out_shape,
        in_specs=[whole_spec()] * count,
        out_specs=jax.tree.map(lambda unused: whole_spec(), out_shape),
        scratch_shapes=list(scratch),
        cost_estimate=pl.CostEstimate(flops=flops, transcendentals=0, bytes_accessed=0),
        compiler_params=pltpu.CompilerParams(vmem_limit_bytes=48 * 1024 * 1024),
    )


def modulation_body(first_ref, second_ref, shift_ref, scale_ref, gate_ref, out_ref):
    seq_index = lax.axis_index("sp")
    rows = lax.broadcasted_iota(jnp.int32, (16, first_ref.shape[1]), 0)
    pair = jnp.where(
        rows == 0, first_ref[pl.ds(seq_index, 1), :], second_ref[pl.ds(seq_index, 1), :]
    )
    activated = (pair / (1.0 + jnp.exp(-pair))).astype(jnp.bfloat16)
    for place, ref in ((0, shift_ref), (2, scale_ref), (4, gate_ref)):
        part = jnp.dot(activated, ref[...], preferred_element_type=jnp.float32)
        out_ref[place : place + 2, :] = part[0:2]
    out_ref[6:8, :] = jnp.zeros((2, out_ref.shape[1]), jnp.float32)


def turn(field, cosine, sine):
    quarter = field.shape[0] // 4
    pieces = [field[i * quarter : (i + 1) * quarter] for i in range(4)]
    swapped = jnp.concatenate([pieces[1], pieces[0], pieces[3], pieces[2]], axis=0)
    return field * cosine + swapped * sine


def projection_body(
    heads,
    kv_heads,
    own_ref,
    core_ref,
    far_ref,
    both_ref,
    context_ref,
    mod_ref,
    gain_ref,
    query_ref,
    key_ref,
    value_ref,
    query_gain_ref,
    key_gain_ref,
    cosine_ref,
    sine_ref,
    q_out,
    kv_out,
):
    span = CHANNEL_SPAN
    group = heads // kv_heads

    def vector(row):
        return jnp.concatenate([mod_ref[i, row : row + 1, :] for i in range(mod_ref.shape[0])], axis=1)

    gain = gain_ref[...]

    def hidden_of(ref, row):
        wide = ref[...].astype(jnp.float32)
        scaled = wide * lax.rsqrt(jnp.mean(wide * wide, axis=-1, keepdims=True) + epsilon)
        return (scaled * (gain * (1.0 + vector(2 + row))) + vector(row)).astype(jnp.bfloat16)

    def normed(raw, head_gain):
        return raw * lax.rsqrt(jnp.mean(raw * raw, axis=0, keepdims=True) + epsilon) * head_gain

    q_out[...] = jnp.zeros_like(q_out)
    query_gain = query_gain_ref[...]
    key_gain = key_gain_ref[...]
    blocks = (own_ref, core_ref, far_ref, both_ref)
    own_rows = own_ref.shape[0]
    tok_count = own_rows * len(blocks)
    for j, ref in enumerate(blocks):
        hidden = hidden_of(ref, 0)
        cosine = cosine_ref[j]
        sine = sine_ref[j]
        queries = jnp.dot(hidden, query_ref[...], preferred_element_type=jnp.float32).T
        for h in range(heads):
            turned = turn(normed(queries[h * span : (h + 1) * span], query_gain), cosine, sine)
            kv, g = h // group, h % group
            lane = g * tok_count + j * own_rows
            q_out[kv, kv * span : (kv + 1) * span, lane : lane + own_rows] = turned.astype(jnp.bfloat16)
        keys = jnp.dot(hidden, key_ref[...], preferred_element_type=jnp.float32).T
        made = [
            turn(normed(keys[h * span : (h + 1) * span], key_gain), cosine, sine)
            for h in range(kv_heads)
        ]
        kv_out[j] = jnp.concatenate(made, axis=0).T.astype(jnp.bfloat16)
        values = jnp.dot(hidden, value_ref[...], preferred_element_type=jnp.float32)
        kv_out[len(blocks) + j] = values.T.astype(jnp.bfloat16)
    hidden = hidden_of(context_ref, 1)
    ctx_rows = context_ref.shape[0]
    keys = jnp.dot(hidden, key_ref[...], preferred_element_type=jnp.float32).T
    made = [normed(keys[h * span : (h + 1) * span], key_gain) for h in range(kv_heads)]
    kv_out[2 * len(blocks), 0:ctx_rows, :] = jnp.concatenate(made, axis=0).T.astype(jnp.bfloat16)
    kv_out[2 * len(blocks), ctx_rows : 2 * ctx_rows, :] = jnp.dot(
        hidden, value_ref[...], preferred_element_type=jnp.float32
    ).astype(jnp.bfloat16)


def attention_body(blocks, first, last, offset, q_tile, *refs):
    q_ref = refs[0]
    kv_refs = refs[1 : 1 + blocks]
    refs = refs[1 + blocks :]
    if not first:
        peak_in, total_in, sum_in = refs[:3]
        refs = refs[3:]
    kv_heads, width, lanes = q_ref.shape
    span = width // kv_heads
    scale = span ** (-0.5) * LOG2E
    parts = (kv_refs[0].shape[0] - 1) // 2
    ctx_rows = kv_refs[0].shape[1] // 2
    for h in range(kv_heads):
        rows = slice(h * span, (h + 1) * span)
        for lane in range(0, lanes, q_tile):
            cut = slice(lane, lane + q_tile)
            query = q_ref[h, :, cut]
            state = None
            if not first:
                state = (peak_in[h, :, cut], total_in[h, :, cut], sum_in[h, :, cut])
            for ref in kv_refs:
                keys = jnp.concatenate([ref[j] for j in range(parts)], axis=0)
                values = jnp.concatenate([ref[parts + j, rows, :] for j in range(parts)], axis=1)
                ctx_keys = ref[2 * parts, 0:ctx_rows, :]
                ctx_values = ref[2 * parts, ctx_rows : 2 * ctx_rows, rows].T
                for k, v, extra in ((keys, values, 0.0), (ctx_keys, ctx_values, offset * LOG2E)):
                    score = jnp.dot(k, query, preferred_element_type=jnp.float32) * scale
                    if extra:
                        score = score + extra
                    peak = jnp.max(score, axis=0, keepdims=True)
                    if state is not None:
                        peak = jnp.maximum(peak, state[0])
                    shares = jnp.exp2(score - peak)
                    total = jnp.sum(shares, axis=0, keepdims=True)
                    weighted = jnp.dot(
                        v, shares.astype(jnp.bfloat16), preferred_element_type=jnp.float32
                    )
                    if state is not None:
                        shrink = jnp.exp2(state[0] - peak)
                        total = total + state[1] * shrink
                        weighted = weighted + state[2] * shrink
                    state = (peak, total, weighted)
            if last:
                (out_ref,) = refs
                attended = (state[2] / state[1]).astype(jnp.bfloat16)
                own_rows = out_ref.shape[2]
                group_lanes = own_rows * out_ref.shape[0]
                for at in range(0, q_tile, own_rows):
                    g, j = (lane + at) // group_lanes, (lane + at) % group_lanes // own_rows
                    head = h * (lanes // group_lanes) + g
                    out_ref[j, head * span : (head + 1) * span, :] = attended[:, at : at + own_rows]
            else:
                peak_out, total_out, sum_out = refs
                peak_out[h, :, cut] = state[0]
                total_out[h, :, cut] = state[1]
                sum_out[h, :, cut] = state[2]


def attend(state, probes, pairs, offset, own_rows, last):
    kv_heads, width, lanes = probes.shape
    span = width // kv_heads
    keys = sum(p.shape[0] // 2 * p.shape[1] + p.shape[1] // 2 for p in pairs)
    inputs = [probes, *pairs] + list(state or ())
    if last:
        tp = lanes * kv_heads
        out = jax.ShapeDtypeStruct(last, jnp.bfloat16)
    else:
        stat = jax.ShapeDtypeStruct((kv_heads, 1, lanes), jnp.float32)
        out = [stat, stat, jax.ShapeDtypeStruct((kv_heads, span, lanes), jnp.float32)]

    def body(*refs):
        attention_body(len(pairs), state is None, bool(last), offset, 256, *refs)

    return kernel_call(body, out, len(inputs), 4 * kv_heads * lanes * keys * span)(*inputs)


def output_body(latent_ref, mod_ref, weight_ref, *refs):
    out_ref, lhs_ref = refs[-2:]
    parts = refs[:-2]
    head_index = lax.axis_index("tp")
    rows = parts[0].shape[0]
    for j, ref in enumerate(parts):
        at = pl.multiple_of(jnp.bitwise_xor(head_index, j) * rows, rows)
        lhs_ref[pl.ds(at, rows), :] = ref[...]
    lhs = lhs_ref[...].T
    columns = mod_ref.shape[2]
    for i in range(mod_ref.shape[0]):
        cut = slice(i * columns, (i + 1) * columns)
        branch = jnp.dot(lhs, weight_ref[:, cut], preferred_element_type=jnp.float32)
        gate = mod_ref[i, 4:5, :]
        out_ref[:, cut] = (latent_ref[:, cut].astype(jnp.float32) + gate * branch).astype(
            jnp.bfloat16
        )


def xor_move(member, axis, mask):
    size = lax.axis_size(axis)
    return lax.ppermute(member, axis, [(i, i ^ mask) for i in range(size)])


def ring_move(member, step):
    size = lax.axis_size("sp")
    return lax.ppermute(member, "sp", [(i, (i + step) % size) for i in range(size)])


def tables(seq_index, head_index, own_rows, head_split):
    quarter = CHANNEL_SPAN // 4
    blocks = jnp.bitwise_xor(jnp.arange(head_split, dtype=jnp.int32), head_index)
    places = (
        seq_index * own_rows * head_split
        + blocks[:, None] * own_rows
        + jnp.arange(own_rows, dtype=jnp.int32)
    )
    inverse = rope_base ** (-jnp.arange(quarter, dtype=jnp.float32) / quarter)
    grid_row = (places // GRID_W).astype(jnp.float32)[:, None, :] * inverse[:, None]
    grid_col = (places % GRID_W).astype(jnp.float32)[:, None, :] * inverse[:, None]
    row_sine, col_sine = jnp.sin(grid_row), jnp.sin(grid_col)
    row_cosine, col_cosine = jnp.cos(grid_row), jnp.cos(grid_col)
    cosine = jnp.concatenate([row_cosine, row_cosine, col_cosine, col_cosine], axis=1)
    sine = jnp.concatenate([-row_sine, row_sine, -col_sine, col_sine], axis=1)
    return cosine, sine


def fast_device(
    latent,
    context,
    condition,
    context_condition,
    norm_gain,
    shift_weight,
    scale_weight,
    gate_weight,
    query_weight,
    key_weight,
    value_weight,
    query_gain,
    key_gain,
    output_weight,
):
    head_split = lax.axis_size("tp")
    seq_split = lax.axis_size("sp")
    seq_index = lax.axis_index("sp")
    head_index = lax.axis_index("tp")
    row_slab, columns = shift_weight.shape
    own_rows, depth = latent.shape
    ctx_rows = context.shape[0]
    tok_count = own_rows * head_split
    q_heads = query_weight.shape[1] // CHANNEL_SPAN
    kv_heads = key_weight.shape[1] // CHANNEL_SPAN

    far = xor_move(latent, "tp", 2)
    near = xor_move(latent, "tp", 1)
    part = kernel_call(
        modulation_body, jax.ShapeDtypeStruct((8, columns), jnp.float32), 5, 10**7
    )(
        condition.reshape(seq_split, row_slab),
        context_condition.reshape(seq_split, row_slab),
        shift_weight,
        scale_weight,
        gate_weight,
    )
    mask = seq_split // 2
    while mask:
        part = part + xor_move(part, "sp", mask)
        mask //= 2
    modulation = lax.all_gather(part, "tp", axis=0, tiled=False)
    both = xor_move(far, "tp", 1)
    cosine, sine = tables(seq_index, head_index, own_rows, head_split)
    probes, own_pairs = kernel_call(
        lambda *refs: projection_body(q_heads, kv_heads, *refs),
        [
            jax.ShapeDtypeStruct(
                (kv_heads, kv_heads * CHANNEL_SPAN, q_heads // kv_heads * tok_count), jnp.bfloat16
            ),
            jax.ShapeDtypeStruct((2 * head_split + 1, own_rows, own_rows), jnp.bfloat16),
        ],
        14,
        4 * tok_count * depth * (q_heads + 2 * kv_heads) * CHANNEL_SPAN,
    )(
        latent,
        near,
        far,
        both,
        context,
        modulation,
        norm_gain.reshape(1, depth),
        query_weight,
        key_weight,
        value_weight,
        query_gain.reshape(CHANNEL_SPAN, 1),
        key_gain.reshape(CHANNEL_SPAN, 1),
        cosine,
        sine,
    )
    offset = math.log(tok_count / (2.0 * ctx_rows))
    near_pairs = xor_move(own_pairs, "sp", 1)
    up = ring_move(own_pairs, 2)
    down = ring_move(own_pairs, -2)
    near_up = xor_move(up, "sp", 1)
    near_down = xor_move(down, "sp", 1)
    across = ring_move(up, 2)
    near_across = xor_move(across, "sp", 1)
    state = attend(None, probes, [own_pairs], offset, own_rows, None)
    state = attend(state, probes, [near_pairs], offset, own_rows, None)
    state = attend(state, probes, [up], offset, own_rows, None)
    state = attend(state, probes, [down, near_up], offset, own_rows, None)
    state = attend(state, probes, [across, near_down], offset, own_rows, None)
    attended = attend(
        state,
        probes,
        [near_across],
        offset,
        own_rows,
        (head_split, q_heads * CHANNEL_SPAN, own_rows),
    )
    parts = [attended[0]] + [xor_move(attended[j], "tp", j) for j in range(1, head_split)]
    width = q_heads * CHANNEL_SPAN
    return kernel_call(
        output_body,
        jax.ShapeDtypeStruct(latent.shape, jnp.bfloat16),
        3 + head_split,
        2 * own_rows * depth * width * head_split,
        [pltpu.VMEM((width * head_split, own_rows), jnp.bfloat16)],
    )(latent, modulation, output_weight, *parts)


def suits(mesh, latent, context, query_weight, key_weight):
    seq_split, head_split = mesh.shape["sp"], mesh.shape["tp"]
    own_rows = latent.shape[0] // (seq_split * head_split)
    ctx_rows = context.shape[0] // seq_split
    kv_heads = key_weight.shape[1] // CHANNEL_SPAN // head_split
    return (
        seq_split == 8
        and head_split == 4
        and own_rows == 2 * CHANNEL_SPAN
        and ctx_rows == CHANNEL_SPAN
        and kv_heads == 2
        and query_weight.shape[1] == 2 * key_weight.shape[1]
    )


def solution(mesh):
    in_specs = (
        P(("sp", "tp"), None),
        P("sp", None),
        P(),
        P(),
        P(),
        P("sp", "tp"),
        P("sp", "tp"),
        P("sp", "tp"),
        P(None, "tp"),
        P(None, "tp"),
        P(None, "tp"),
        P(),
        P(),
        P(),
    )
    out_specs = P(("sp", "tp"), None)

    def program(*args):
        fast = suits(mesh, args[0], args[1], args[8], args[9])
        return jax.shard_map(
            fast_device if fast else general_device,
            mesh=mesh,
            in_specs=in_specs,
            out_specs=out_specs,
            check_vma=False,
        )(*args)

    return program
```

```python
import math

import jax
import jax.numpy as jnp
from jax import lax
from jax.experimental import pallas as pl
from jax.experimental.pallas import tpu as pltpu
from jax.sharding import PartitionSpec as P

CHANNEL_SPAN = 64
GRID_W = 64


epsilon = 1e-06
rope_base = 10000.0


def modulate(tok_rows, norm_gain, shift_row, scale_row):
    wide = tok_rows.astype(jnp.float32)
    normed = wide * lax.rsqrt(jnp.mean(wide * wide, axis=-1, keepdims=True) + epsilon)
    return (normed * norm_gain * (1.0 + scale_row) + shift_row).astype(jnp.bfloat16)


def headnorm(raw, gain, heads):
    field = raw.reshape(raw.shape[0], heads, -1)
    return field * lax.rsqrt(jnp.mean(field * field, axis=-1, keepdims=True) + epsilon) * gain


def rotate(field, places):
    count = field.shape[0]
    heads = field.shape[1]
    quarter = field.shape[2] // 4
    grid_row = (places // GRID_W).astype(jnp.float32)
    grid_col = (places % GRID_W).astype(jnp.float32)
    inverse = rope_base ** (-jnp.arange(quarter, dtype=jnp.float32) / quarter)
    angles = jnp.stack([grid_row[:, None] * inverse, grid_col[:, None] * inverse], axis=1)[:, None]
    cosine = jnp.cos(angles)
    sine = jnp.sin(angles)
    matcher_content_couples = field.reshape(count, heads, 2, 2, quarter)
    first = matcher_content_couples[:, :, :, 0]
    second = matcher_content_couples[:, :, :, 1]
    turned = jnp.stack([first * cosine - second * sine, second * cosine + first * sine], axis=3)
    return turned.reshape(count, heads, 4 * quarter)


def process_probe_group(
    accumulator_carry, probe_entries, matcher_content_couples, similarity_offset
):
    row_peak, row_total, weighted = accumulator_carry
    kv_heads = probe_entries.shape[1]
    head_size = probe_entries.shape[3]
    pair_width = kv_heads * head_size
    matcher_pieces = matcher_content_couples[:, :pair_width].reshape(
        matcher_content_couples.shape[0], kv_heads, head_size
    )
    value_rows = matcher_content_couples[:, pair_width:].reshape(
        matcher_content_couples.shape[0], kv_heads, head_size
    )
    similarity_matrix = (
        jnp.einsum(
            "dmvk,hmk->dmvh", probe_entries, matcher_pieces, preferred_element_type=jnp.float32
        )
        * head_size ** (-0.5)
        + similarity_offset
    )
    new_peak = jnp.maximum(row_peak, jnp.max(similarity_matrix, axis=-1))
    shares = jnp.exp(similarity_matrix - new_peak[..., None])
    shrink = jnp.exp(row_peak - new_peak)
    row_total = row_total * shrink + jnp.sum(shares, axis=-1)
    weighted = weighted * shrink[..., None] + jnp.einsum(
        "qkgn,nkd->qkgd",
        shares.astype(jnp.bfloat16),
        value_rows,
        preferred_element_type=jnp.float32,
    )
    return (new_peak, row_total, weighted)


def group_walker(accumulator_carry, probe_entries, matcher_content_couples, similarity_offset):
    pair_count = matcher_content_couples.shape[0]
    probe_group_total = -(-pair_count // 2048)
    while pair_count % probe_group_total:
        probe_group_total += 1
    if probe_group_total == 1:
        return process_probe_group(
            accumulator_carry, probe_entries, matcher_content_couples, similarity_offset
        )
    group_extent = pair_count // probe_group_total

    def scan_step(inner, slices):
        return (process_probe_group(inner, probe_entries, slices[0], slices[1]), None)

    result, unused = lax.scan(
        scan_step,
        accumulator_carry,
        (
            matcher_content_couples.reshape(
                probe_group_total, group_extent, matcher_content_couples.shape[1]
            ),
            similarity_offset.reshape(probe_group_total, group_extent),
        ),
    )
    return result


def general_device(
    latent,
    context,
    condition,
    context_condition,
    norm_gain,
    shift_weight,
    scale_weight,
    gate_weight,
    query_weight,
    key_weight,
    value_weight,
    query_gain,
    key_gain,
    output_weight,
):
    head_split = lax.axis_size("tp")
    seq_index = lax.axis_index("sp")
    head_index = lax.axis_index("tp")
    row_slab = shift_weight.shape[0]
    columns = shift_weight.shape[1]
    conditions = jnp.stack([condition, context_condition])
    activated = jax.nn.silu(
        lax.dynamic_slice_in_dim(conditions, seq_index * row_slab, row_slab, 1)
    ).astype(jnp.bfloat16)
    part_shift = jnp.dot(activated, shift_weight, preferred_element_type=jnp.float32)
    part_scale = jnp.dot(activated, scale_weight, preferred_element_type=jnp.float32)
    part_gate = jnp.dot(activated, gate_weight, preferred_element_type=jnp.float32)

    def widen(member):
        blank = jnp.zeros((2, columns * head_split), jnp.float32)
        return lax.dynamic_update_slice_in_dim(blank, member, head_index * columns, 1)

    shifts, scales, gates = lax.psum(
        (widen(part_shift), widen(part_scale), widen(part_gate)), ("sp", "tp")
    )
    own_rows = latent.shape[0]
    tok_count = own_rows * head_split
    ctx_rows = context.shape[0]
    hidden = modulate(latent, norm_gain, shifts[0], scales[0])
    context_hidden = modulate(context, norm_gain, shifts[1], scales[1])
    q_heads = query_weight.shape[1] // CHANNEL_SPAN
    kv_heads = key_weight.shape[1] // CHANNEL_SPAN
    group_size = q_heads // kv_heads
    q_width = q_heads * CHANNEL_SPAN
    kv_width = kv_heads * CHANNEL_SPAN
    joined_weight = jnp.concatenate([query_weight, key_weight, value_weight], axis=1)
    projected = jnp.dot(
        lax.all_gather(hidden, "tp", axis=0, tiled=True),
        joined_weight,
        preferred_element_type=jnp.float32,
    )
    places = seq_index * tok_count + jnp.arange(tok_count, dtype=jnp.int32)
    probe_entries = rotate(headnorm(projected[:, :q_width], query_gain, q_heads), places).astype(
        jnp.bfloat16
    )
    probe_entries = probe_entries.reshape(tok_count, kv_heads, group_size, CHANNEL_SPAN)
    latent_keys = rotate(
        headnorm(projected[:, q_width : q_width + kv_width], key_gain, kv_heads), places
    ).astype(jnp.bfloat16)
    latent_values = projected[:, q_width + kv_width :].astype(jnp.bfloat16)
    own_pairs = jnp.concatenate([latent_keys.reshape(tok_count, kv_width), latent_values], axis=1)
    ctx_projected = jnp.dot(
        context_hidden, joined_weight[:, q_width:], preferred_element_type=jnp.float32
    )
    ctx_keys = (
        headnorm(ctx_projected[:, :kv_width], key_gain, kv_heads)
        .astype(jnp.bfloat16)
        .reshape(ctx_rows, kv_width)
    )
    ctx_pairs = jnp.concatenate(
        [ctx_keys, ctx_projected[:, kv_width:].astype(jnp.bfloat16)], axis=1
    )
    prefix_mapped = math.log(tok_count / (2.0 * ctx_rows))
    stat_shape = (tok_count, kv_heads, group_size)
    start_state = (
        jnp.full(stat_shape, -jnp.inf, jnp.float32),
        jnp.zeros(stat_shape, jnp.float32),
        jnp.zeros(stat_shape + (CHANNEL_SPAN,), jnp.float32),
    )
    ctx_whole = lax.all_gather(ctx_pairs, "sp", axis=0, tiled=True)
    ctx_state = group_walker(
        start_state,
        probe_entries,
        ctx_whole,
        jnp.full((ctx_whole.shape[0],), prefix_mapped, jnp.float32),
    )
    key_piece = lax.all_gather(own_pairs, "sp", axis=0, tiled=True)
    final_state = group_walker(
        ctx_state, probe_entries, key_piece, jnp.zeros((key_piece.shape[0],), jnp.float32)
    )
    row_peak, row_total, weighted = final_state
    attended = (weighted / row_total[..., None]).astype(jnp.bfloat16).reshape(tok_count, q_width)
    branch = jnp.dot(
        lax.all_to_all(attended, "tp", split_axis=0, concat_axis=1, tiled=True),
        output_weight,
        preferred_element_type=jnp.float32,
    )
    return (latent.astype(jnp.float32) + gates[0] * branch).astype(jnp.bfloat16)


LOG2E = math.log2(math.e)


def whole_spec():
    return pl.BlockSpec(memory_space=pltpu.VMEM)


def kernel_call(body, out_shape, count, flops, scratch=()):
    return pl.pallas_call(
        body,
        out_shape=out_shape,
        in_specs=[whole_spec()] * count,
        out_specs=jax.tree.map(lambda unused: whole_spec(), out_shape),
        scratch_shapes=list(scratch),
        cost_estimate=pl.CostEstimate(flops=flops, transcendentals=0, bytes_accessed=0),
        compiler_params=pltpu.CompilerParams(vmem_limit_bytes=48 * 1024 * 1024),
    )


def modulation_body(first_ref, second_ref, shift_hbm, scale_hbm, gate_hbm, out_ref, *scratch):
    sems = scratch[-1]
    copies = []
    for i, (source, target) in enumerate(zip((shift_hbm, scale_hbm, gate_hbm), scratch)):
        copies.append(pltpu.make_async_copy(source, target, sems.at[i]))
        copies[-1].start()
    row_slab = shift_hbm.shape[0]
    cut = pl.ds(pl.multiple_of(lax.axis_index("sp") * row_slab, row_slab), row_slab)
    rows = lax.broadcasted_iota(jnp.int32, (16, row_slab), 0)
    pair = jnp.where(rows == 0, first_ref[:, cut], second_ref[:, cut])
    activated = (pair / (1.0 + jnp.exp(-pair))).astype(jnp.bfloat16)
    out_ref[6:8, :] = jnp.zeros((2, out_ref.shape[1]), jnp.float32)
    for i in range(3):
        copies[i].wait()
        part = jnp.dot(activated, scratch[i][...], preferred_element_type=jnp.float32)
        out_ref[2 * i : 2 * i + 2, :] = part[0:2]


def fetch_body(count, *refs):
    sems = refs[-1]
    copies = []
    for i in range(count):
        copies.append(pltpu.make_async_copy(refs[1 + i], refs[1 + count + i], sems.at[i]))
        copies[-1].start()
    for copy in copies:
        copy.wait()


def fetch(after, *arrays):
    count = len(arrays)
    hbm = pl.BlockSpec(memory_space=pltpu.HBM)
    return pl.pallas_call(
        lambda *refs: fetch_body(count, *refs),
        out_shape=[jax.ShapeDtypeStruct(a.shape, a.dtype) for a in arrays],
        in_specs=[hbm] * (1 + count),
        out_specs=[whole_spec()] * count,
        scratch_shapes=[pltpu.SemaphoreType.DMA((count,))],
        cost_estimate=pl.CostEstimate(flops=10**9, transcendentals=0, bytes_accessed=0),
        compiler_params=pltpu.CompilerParams(vmem_limit_bytes=48 * 1024 * 1024),
    )(after, *arrays)


def turn(field, cosine, sine):
    quarter = field.shape[0] // 4
    pieces = [field[i * quarter : (i + 1) * quarter] for i in range(4)]
    swapped = jnp.concatenate([pieces[1], pieces[0], pieces[3], pieces[2]], axis=0)
    return field * cosine + swapped * sine


def projection_body(
    heads,
    kv_heads,
    own_ref,
    core_ref,
    far_ref,
    both_ref,
    context_ref,
    mod_ref,
    gain_ref,
    query_ref,
    key_ref,
    value_ref,
    query_gain_ref,
    key_gain_ref,
    cosine_ref,
    sine_ref,
    q_out,
    kv_out,
):
    span = CHANNEL_SPAN
    group = heads // kv_heads

    def vector(row):
        return jnp.concatenate([mod_ref[i, row : row + 1, :] for i in range(mod_ref.shape[0])], axis=1)

    gain = gain_ref[...]

    def hidden_of(ref, row):
        wide = ref[...].astype(jnp.float32)
        scaled = wide * lax.rsqrt(jnp.mean(wide * wide, axis=-1, keepdims=True) + epsilon)
        return (scaled * (gain * (1.0 + vector(2 + row))) + vector(row)).astype(jnp.bfloat16)

    def normed(raw, head_gain):
        return raw * lax.rsqrt(jnp.mean(raw * raw, axis=0, keepdims=True) + epsilon) * head_gain

    q_out[...] = jnp.zeros_like(q_out)
    def upright(ref):
        return jnp.broadcast_to(ref[...], (8, span)).T[:, 0:1]

    query_gain = upright(query_gain_ref)
    key_gain = upright(key_gain_ref)
    blocks = (own_ref, core_ref, far_ref, both_ref)
    own_rows = own_ref.shape[0]
    tok_count = own_rows * len(blocks)
    for j, ref in enumerate(blocks):
        hidden = hidden_of(ref, 0)
        cosine = cosine_ref[j]
        sine = sine_ref[j]
        queries = jnp.dot(hidden, query_ref[...], preferred_element_type=jnp.float32).T
        for h in range(heads):
            turned = turn(normed(queries[h * span : (h + 1) * span], query_gain), cosine, sine)
            kv, g = h // group, h % group
            lane = g * tok_count + j * own_rows
            q_out[kv, kv * span : (kv + 1) * span, lane : lane + own_rows] = turned.astype(jnp.bfloat16)
        keys = jnp.dot(hidden, key_ref[...], preferred_element_type=jnp.float32).T
        made = [
            turn(normed(keys[h * span : (h + 1) * span], key_gain), cosine, sine)
            for h in range(kv_heads)
        ]
        kv_out[j] = jnp.concatenate(made, axis=0).T.astype(jnp.bfloat16)
        values = jnp.dot(hidden, value_ref[...], preferred_element_type=jnp.float32)
        kv_out[len(blocks) + j] = values.T.astype(jnp.bfloat16)
    hidden = hidden_of(context_ref, 1)
    ctx_rows = context_ref.shape[0]
    keys = jnp.dot(hidden, key_ref[...], preferred_element_type=jnp.float32).T
    made = [normed(keys[h * span : (h + 1) * span], key_gain) for h in range(kv_heads)]
    kv_out[2 * len(blocks), 0:ctx_rows, :] = jnp.concatenate(made, axis=0).T.astype(jnp.bfloat16)
    kv_out[2 * len(blocks), ctx_rows : 2 * ctx_rows, :] = jnp.dot(
        hidden, value_ref[...], preferred_element_type=jnp.float32
    ).astype(jnp.bfloat16)


def attention_body(blocks, first, last, offset, q_tile, *refs):
    q_ref = refs[0]
    kv_refs = refs[1 : 1 + blocks]
    refs = refs[1 + blocks :]
    if not first:
        peak_in, total_in, sum_in = refs[:3]
        refs = refs[3:]
    kv_heads, width, lanes = q_ref.shape
    span = width // kv_heads
    scale = span ** (-0.5) * LOG2E
    parts = (kv_refs[0].shape[0] - 1) // 2
    ctx_rows = kv_refs[0].shape[1] // 2
    chunks = []
    for ref in kv_refs:
        half = parts // 2
        chunks += [(ref, range(half), False), (ref, range(half, parts), True)]
    tiles = [
        (h, lane, chunk)
        for chunk in chunks
        for h in range(kv_heads)
        for lane in range(0, lanes, q_tile)
    ]
    states = {}

    def scores(tile):
        h, lane, (ref, places, context) = tile
        keys = [ref[j] for j in places]
        if context:
            keys.append(ref[2 * parts, 0:ctx_rows, :])
        query = q_ref[h, :, lane : lane + q_tile]
        found = jnp.dot(jnp.concatenate(keys, axis=0), query, preferred_element_type=jnp.float32)
        found = found * scale
        if context:
            rows = found.shape[0] - ctx_rows
            found = jnp.concatenate([found[:rows], found[rows:] + offset * LOG2E], axis=0)
        return found

    def soften(tile, found):
        h, lane, unused = tile
        peak = jnp.max(found, axis=0, keepdims=True)
        old = states.get((h, lane))
        if old is None and not first:
            cut = slice(lane, lane + q_tile)
            old = (peak_in[h, :, cut], total_in[h, :, cut], sum_in[h, :, cut])
        if old is not None:
            peak = jnp.maximum(peak, old[0])
        shares = jnp.exp2(found - peak)
        total = jnp.sum(shares, axis=0, keepdims=True)
        shrink = None
        if old is not None:
            shrink = jnp.exp2(old[0] - peak)
            total = total + old[1] * shrink
        states[(h, lane)] = (peak, total, old[2] if old is not None else None)
        return shares.astype(jnp.bfloat16), shrink

    def gather(tile, shares, shrink):
        h, lane, (ref, places, context) = tile
        rows = slice(h * span, (h + 1) * span)
        values = [ref[parts + j, rows, :] for j in places]
        if context:
            values.append(ref[2 * parts, ctx_rows : 2 * ctx_rows, :].T[rows])
        weighted = jnp.dot(
            jnp.concatenate(values, axis=1), shares, preferred_element_type=jnp.float32
        )
        peak, total, old = states[(h, lane)]
        if shrink is not None:
            weighted = weighted + old * shrink
        states[(h, lane)] = (peak, total, weighted)

    following = scores(tiles[0])
    waiting = None
    for i, tile in enumerate(tiles):
        found = following
        if i + 1 < len(tiles):
            following = scores(tiles[i + 1])
        shares, shrink = soften(tile, found)
        if waiting:
            gather(*waiting)
        waiting = (tile, shares, shrink)
    gather(*waiting)
    for (h, lane), (peak, total, weighted) in states.items():
        cut = slice(lane, lane + q_tile)
        if last:
            (out_ref,) = refs
            attended = (weighted / total).astype(jnp.bfloat16)
            own_rows = out_ref.shape[2]
            group_lanes = own_rows * out_ref.shape[0]
            for at in range(0, q_tile, own_rows):
                g, j = (lane + at) // group_lanes, (lane + at) % group_lanes // own_rows
                head = h * (lanes // group_lanes) + g
                out_ref[j, head * span : (head + 1) * span, :] = attended[:, at : at + own_rows]
        else:
            peak_out, total_out, sum_out = refs
            peak_out[h, :, cut] = peak
            total_out[h, :, cut] = total
            sum_out[h, :, cut] = weighted


def attend(state, probes, pairs, offset, own_rows, last):
    kv_heads, width, lanes = probes.shape
    span = width // kv_heads
    keys = sum(p.shape[0] // 2 * p.shape[1] + p.shape[1] // 2 for p in pairs)
    inputs = [probes, *pairs] + list(state or ())
    if last:
        tp = lanes * kv_heads
        out = jax.ShapeDtypeStruct(last, jnp.bfloat16)
    else:
        stat = jax.ShapeDtypeStruct((kv_heads, 1, lanes), jnp.float32)
        out = [stat, stat, jax.ShapeDtypeStruct((kv_heads, span, lanes), jnp.float32)]

    def body(*refs):
        attention_body(len(pairs), state is None, bool(last), offset, 512, *refs)

    return kernel_call(body, out, len(inputs), 40 * kv_heads * lanes * keys * span)(*inputs)


def output_body(latent_ref, mod_ref, weight_ref, *refs):
    out_ref, lhs_ref = refs[-2:]
    parts = refs[:-2]
    head_index = lax.axis_index("tp")
    rows = parts[0].shape[0]
    for j, ref in enumerate(parts):
        at = pl.multiple_of(jnp.bitwise_xor(head_index, j) * rows, rows)
        lhs_ref[pl.ds(at, rows), :] = ref[...]
    lhs = lhs_ref[...].T
    columns = mod_ref.shape[2]
    for i in range(mod_ref.shape[0]):
        cut = slice(i * columns, (i + 1) * columns)
        branch = jnp.dot(lhs, weight_ref[:, cut], preferred_element_type=jnp.float32)
        gate = mod_ref[i, 4:5, :]
        out_ref[:, cut] = (latent_ref[:, cut].astype(jnp.float32) + gate * branch).astype(
            jnp.bfloat16
        )


def xor_move(member, axis, mask):
    size = lax.axis_size(axis)
    return lax.ppermute(member, axis, [(i, i ^ mask) for i in range(size)])


def ring_move(member, step):
    size = lax.axis_size("sp")
    return lax.ppermute(member, "sp", [(i, (i + step) % size) for i in range(size)])


def tables(seq_index, head_index, own_rows, head_split):
    quarter = CHANNEL_SPAN // 4
    blocks = jnp.bitwise_xor(jnp.arange(head_split, dtype=jnp.int32), head_index)
    places = (
        seq_index * own_rows * head_split
        + blocks[:, None] * own_rows
        + jnp.arange(own_rows, dtype=jnp.int32)
    )
    inverse = rope_base ** (-jnp.arange(quarter, dtype=jnp.float32) / quarter)
    grid_row = (places // GRID_W).astype(jnp.float32)[:, None, :] * inverse[:, None]
    grid_col = (places % GRID_W).astype(jnp.float32)[:, None, :] * inverse[:, None]
    row_sine, col_sine = jnp.sin(grid_row), jnp.sin(grid_col)
    row_cosine, col_cosine = jnp.cos(grid_row), jnp.cos(grid_col)
    cosine = jnp.concatenate([row_cosine, row_cosine, col_cosine, col_cosine], axis=1)
    sine = jnp.concatenate([-row_sine, row_sine, -col_sine, col_sine], axis=1)
    return cosine, sine


def fast_device(
    latent,
    context,
    condition,
    context_condition,
    norm_gain,
    shift_weight,
    scale_weight,
    gate_weight,
    query_weight,
    key_weight,
    value_weight,
    query_gain,
    key_gain,
    output_weight,
):
    head_split = lax.axis_size("tp")
    seq_split = lax.axis_size("sp")
    seq_index = lax.axis_index("sp")
    head_index = lax.axis_index("tp")
    row_slab, columns = shift_weight.shape
    own_rows, depth = latent.shape
    ctx_rows = context.shape[0]
    tok_count = own_rows * head_split
    q_heads = query_weight.shape[1] // CHANNEL_SPAN
    kv_heads = key_weight.shape[1] // CHANNEL_SPAN

    far = xor_move(latent, "tp", 2)
    near = xor_move(latent, "tp", 1)
    hbm = pl.BlockSpec(memory_space=pltpu.HBM)
    part = pl.pallas_call(
        modulation_body,
        out_shape=jax.ShapeDtypeStruct((8, columns), jnp.float32),
        in_specs=[whole_spec()] * 2 + [hbm] * 3,
        out_specs=whole_spec(),
        scratch_shapes=[pltpu.VMEM((row_slab, columns), jnp.bfloat16)] * 3
        + [pltpu.SemaphoreType.DMA((3,))],
        cost_estimate=pl.CostEstimate(flops=10**8, transcendentals=0, bytes_accessed=0),
    )(
        condition.reshape(1, depth),
        context_condition.reshape(1, depth),
        shift_weight,
        scale_weight,
        gate_weight,
    )
    own, context, query_weight, key_weight, value_weight, output_weight = fetch(
        part, latent, context, query_weight, key_weight, value_weight, output_weight
    )
    mask = seq_split // 2
    while mask:
        part = part + xor_move(part, "sp", mask)
        mask //= 2
    modulation = lax.all_gather(part, "tp", axis=0, tiled=False)
    both = xor_move(far, "tp", 1)
    cosine, sine = tables(seq_index, head_index, own_rows, head_split)
    probes, own_pairs = kernel_call(
        lambda *refs: projection_body(q_heads, kv_heads, *refs),
        [
            jax.ShapeDtypeStruct(
                (kv_heads, kv_heads * CHANNEL_SPAN, q_heads // kv_heads * tok_count), jnp.bfloat16
            ),
            jax.ShapeDtypeStruct((2 * head_split + 1, own_rows, own_rows), jnp.bfloat16),
        ],
        14,
        4 * tok_count * depth * (q_heads + 2 * kv_heads) * CHANNEL_SPAN,
    )(
        own,
        near,
        far,
        both,
        context,
        modulation,
        norm_gain.reshape(1, depth),
        query_weight,
        key_weight,
        value_weight,
        query_gain.reshape(1, CHANNEL_SPAN),
        key_gain.reshape(1, CHANNEL_SPAN),
        cosine,
        sine,
    )
    offset = math.log(tok_count / (2.0 * ctx_rows))
    near_pairs = xor_move(own_pairs, "sp", 1)
    up = ring_move(own_pairs, 2)
    down = ring_move(own_pairs, -2)
    near_up = xor_move(up, "sp", 1)
    near_down = xor_move(down, "sp", 1)
    across = ring_move(up, 2)
    near_across = xor_move(across, "sp", 1)
    state = attend(None, probes, [own_pairs], offset, own_rows, None)
    state = attend(state, probes, [near_pairs], offset, own_rows, None)
    state = attend(state, probes, [up], offset, own_rows, None)
    state = attend(state, probes, [down, near_up], offset, own_rows, None)
    state = attend(state, probes, [across, near_down], offset, own_rows, None)
    attended = attend(
        state,
        probes,
        [near_across],
        offset,
        own_rows,
        (head_split, q_heads * CHANNEL_SPAN, own_rows),
    )
    parts = [attended[0]] + [xor_move(attended[j], "tp", j) for j in range(1, head_split)]
    width = q_heads * CHANNEL_SPAN
    return kernel_call(
        output_body,
        jax.ShapeDtypeStruct(latent.shape, jnp.bfloat16),
        3 + head_split,
        2 * own_rows * depth * width * head_split,
        [pltpu.VMEM((width * head_split, own_rows), jnp.bfloat16)],
    )(own, modulation, output_weight, *parts)


def suits(mesh, latent, context, query_weight, key_weight):
    seq_split, head_split = mesh.shape["sp"], mesh.shape["tp"]
    own_rows = latent.shape[0] // (seq_split * head_split)
    ctx_rows = context.shape[0] // seq_split
    kv_heads = key_weight.shape[1] // CHANNEL_SPAN // head_split
    return (
        seq_split == 8
        and head_split == 4
        and own_rows == 2 * CHANNEL_SPAN
        and ctx_rows == CHANNEL_SPAN
        and kv_heads == 2
        and query_weight.shape[1] == 2 * key_weight.shape[1]
    )


def solution(mesh):
    in_specs = (
        P(("sp", "tp"), None),
        P("sp", None),
        P(),
        P(),
        P(),
        P("sp", "tp"),
        P("sp", "tp"),
        P("sp", "tp"),
        P(None, "tp"),
        P(None, "tp"),
        P(None, "tp"),
        P(),
        P(),
        P(),
    )
    out_specs = P(("sp", "tp"), None)

    def program(*args):
        fast = suits(mesh, args[0], args[1], args[8], args[9])
        return jax.shard_map(
            fast_device if fast else general_device,
            mesh=mesh,
            in_specs=in_specs,
            out_specs=out_specs,
            check_vma=False,
        )(*args)

    return program
```

```python
import math

import jax
import jax.numpy as jnp
from jax import lax
from jax.experimental import pallas as pl
from jax.experimental.pallas import tpu as pltpu
from jax.sharding import PartitionSpec as P


CHANNEL_SPAN = 64
GRID_W = 64


epsilon = 1e-06
rope_base = 10000.0


def modulate(tok_rows, norm_gain, shift_row, scale_row):
    wide = tok_rows.astype(jnp.float32)
    normed = wide * lax.rsqrt(jnp.mean(wide * wide, axis=-1, keepdims=True) + epsilon)
    return (normed * norm_gain * (1.0 + scale_row) + shift_row).astype(jnp.bfloat16)


def headnorm(raw, gain, heads):
    field = raw.reshape(raw.shape[0], heads, -1)
    return field * lax.rsqrt(jnp.mean(field * field, axis=-1, keepdims=True) + epsilon) * gain


def rotate(field, places):
    count = field.shape[0]
    heads = field.shape[1]
    quarter = field.shape[2] // 4
    grid_row = (places // GRID_W).astype(jnp.float32)
    grid_col = (places % GRID_W).astype(jnp.float32)
    inverse = rope_base ** (-jnp.arange(quarter, dtype=jnp.float32) / quarter)
    angles = jnp.stack([grid_row[:, None] * inverse, grid_col[:, None] * inverse], axis=1)[:, None]
    cosine = jnp.cos(angles)
    sine = jnp.sin(angles)
    matcher_content_couples = field.reshape(count, heads, 2, 2, quarter)
    first = matcher_content_couples[:, :, :, 0]
    second = matcher_content_couples[:, :, :, 1]
    turned = jnp.stack([first * cosine - second * sine, second * cosine + first * sine], axis=3)
    return turned.reshape(count, heads, 4 * quarter)


def process_probe_group(
    accumulator_carry, probe_entries, matcher_content_couples, similarity_offset
):
    row_peak, row_total, weighted = accumulator_carry
    kv_heads = probe_entries.shape[1]
    head_size = probe_entries.shape[3]
    pair_width = kv_heads * head_size
    matcher_pieces = matcher_content_couples[:, :pair_width].reshape(
        matcher_content_couples.shape[0], kv_heads, head_size
    )
    value_rows = matcher_content_couples[:, pair_width:].reshape(
        matcher_content_couples.shape[0], kv_heads, head_size
    )
    similarity_matrix = (
        jnp.einsum(
            "dmvk,hmk->dmvh", probe_entries, matcher_pieces, preferred_element_type=jnp.float32
        )
        * head_size ** (-0.5)
        + similarity_offset
    )
    new_peak = jnp.maximum(row_peak, jnp.max(similarity_matrix, axis=-1))
    shares = jnp.exp(similarity_matrix - new_peak[..., None])
    shrink = jnp.exp(row_peak - new_peak)
    row_total = row_total * shrink + jnp.sum(shares, axis=-1)
    weighted = weighted * shrink[..., None] + jnp.einsum(
        "qkgn,nkd->qkgd",
        shares.astype(jnp.bfloat16),
        value_rows,
        preferred_element_type=jnp.float32,
    )
    return (new_peak, row_total, weighted)


def group_walker(accumulator_carry, probe_entries, matcher_content_couples, similarity_offset):
    pair_count = matcher_content_couples.shape[0]
    probe_group_total = -(-pair_count // 2048)
    while pair_count % probe_group_total:
        probe_group_total += 1
    if probe_group_total == 1:
        return process_probe_group(
            accumulator_carry, probe_entries, matcher_content_couples, similarity_offset
        )
    group_extent = pair_count // probe_group_total

    def scan_step(inner, slices):
        return (process_probe_group(inner, probe_entries, slices[0], slices[1]), None)

    result, _ = lax.scan(
        scan_step,
        accumulator_carry,
        (
            matcher_content_couples.reshape(
                probe_group_total, group_extent, matcher_content_couples.shape[1]
            ),
            similarity_offset.reshape(probe_group_total, group_extent),
        ),
    )
    return result


def general_device(
    latent,
    context,
    condition,
    context_condition,
    norm_gain,
    shift_weight,
    scale_weight,
    gate_weight,
    query_weight,
    key_weight,
    value_weight,
    query_gain,
    key_gain,
    output_weight,
):
    head_split = lax.axis_size("tp")
    seq_index = lax.axis_index("sp")
    head_index = lax.axis_index("tp")
    row_slab = shift_weight.shape[0]
    columns = shift_weight.shape[1]
    conditions = jnp.stack([condition, context_condition])
    activated = jax.nn.silu(
        lax.dynamic_slice_in_dim(conditions, seq_index * row_slab, row_slab, 1)
    ).astype(jnp.bfloat16)
    part_shift = jnp.dot(activated, shift_weight, preferred_element_type=jnp.float32)
    part_scale = jnp.dot(activated, scale_weight, preferred_element_type=jnp.float32)
    part_gate = jnp.dot(activated, gate_weight, preferred_element_type=jnp.float32)

    def widen(member):
        blank = jnp.zeros((2, columns * head_split), jnp.float32)
        return lax.dynamic_update_slice_in_dim(blank, member, head_index * columns, 1)

    shifts, scales, gates = lax.psum(
        (widen(part_shift), widen(part_scale), widen(part_gate)), ("sp", "tp")
    )
    own_rows = latent.shape[0]
    tok_count = own_rows * head_split
    ctx_rows = context.shape[0]
    hidden = modulate(latent, norm_gain, shifts[0], scales[0])
    context_hidden = modulate(context, norm_gain, shifts[1], scales[1])
    q_heads = query_weight.shape[1] // CHANNEL_SPAN
    kv_heads = key_weight.shape[1] // CHANNEL_SPAN
    group_size = q_heads // kv_heads
    q_width = q_heads * CHANNEL_SPAN
    kv_width = kv_heads * CHANNEL_SPAN
    joined_weight = jnp.concatenate([query_weight, key_weight, value_weight], axis=1)
    projected = jnp.dot(
        lax.all_gather(hidden, "tp", axis=0, tiled=True),
        joined_weight,
        preferred_element_type=jnp.float32,
    )
    places = seq_index * tok_count + jnp.arange(tok_count, dtype=jnp.int32)
    probe_entries = rotate(headnorm(projected[:, :q_width], query_gain, q_heads), places).astype(
        jnp.bfloat16
    )
    probe_entries = probe_entries.reshape(tok_count, kv_heads, group_size, CHANNEL_SPAN)
    latent_keys = rotate(
        headnorm(projected[:, q_width : q_width + kv_width], key_gain, kv_heads), places
    ).astype(jnp.bfloat16)
    latent_values = projected[:, q_width + kv_width :].astype(jnp.bfloat16)
    own_pairs = jnp.concatenate([latent_keys.reshape(tok_count, kv_width), latent_values], axis=1)
    ctx_projected = jnp.dot(
        context_hidden, joined_weight[:, q_width:], preferred_element_type=jnp.float32
    )
    ctx_keys = (
        headnorm(ctx_projected[:, :kv_width], key_gain, kv_heads)
        .astype(jnp.bfloat16)
        .reshape(ctx_rows, kv_width)
    )
    ctx_pairs = jnp.concatenate(
        [ctx_keys, ctx_projected[:, kv_width:].astype(jnp.bfloat16)], axis=1
    )
    prefix_mapped = math.log(tok_count / (2.0 * ctx_rows))
    stat_shape = (tok_count, kv_heads, group_size)
    start_state = (
        jnp.full(stat_shape, -jnp.inf, jnp.float32),
        jnp.zeros(stat_shape, jnp.float32),
        jnp.zeros(stat_shape + (CHANNEL_SPAN,), jnp.float32),
    )
    ctx_whole = lax.all_gather(ctx_pairs, "sp", axis=0, tiled=True)
    ctx_state = group_walker(
        start_state,
        probe_entries,
        ctx_whole,
        jnp.full((ctx_whole.shape[0],), prefix_mapped, jnp.float32),
    )
    key_piece = lax.all_gather(own_pairs, "sp", axis=0, tiled=True)
    final_state = group_walker(
        ctx_state, probe_entries, key_piece, jnp.zeros((key_piece.shape[0],), jnp.float32)
    )
    _, row_total, weighted = final_state
    attended = (weighted / row_total[..., None]).astype(jnp.bfloat16).reshape(tok_count, q_width)
    branch = jnp.dot(
        lax.all_to_all(attended, "tp", split_axis=0, concat_axis=1, tiled=True),
        output_weight,
        preferred_element_type=jnp.float32,
    )
    return (latent.astype(jnp.float32) + gates[0] * branch).astype(jnp.bfloat16)


LOG2E = math.log2(math.e)


def whole_spec():
    return pl.BlockSpec(memory_space=pltpu.VMEM)


def kernel_call(body, out_shape, count, flops, scratch=()):
    return pl.pallas_call(
        body,
        out_shape=out_shape,
        in_specs=[whole_spec()] * count,
        out_specs=jax.tree.map(lambda unused: whole_spec(), out_shape),
        scratch_shapes=list(scratch),
        cost_estimate=pl.CostEstimate(flops=flops, transcendentals=0, bytes_accessed=0),
        compiler_params=pltpu.CompilerParams(vmem_limit_bytes=48 * 1024 * 1024),
    )


ROOMY = 60 * 1024 * 1024


def hbm_spec():
    return pl.BlockSpec(memory_space=pltpu.HBM)


def start_loads(pairs, sems):
    copies = []
    for i, (source, target) in enumerate(pairs):
        copies.append(pltpu.make_async_copy(source, target, sems.at[i]))
        copies[-1].start()
    return copies


def opening_body(first_hbm, second_hbm, shift_hbm, scale_hbm, gate_hbm, out_ref, *scratch):
    first, second, *targets, sems = scratch
    row_slab = shift_hbm.shape[0]
    cut = pl.ds(pl.multiple_of(lax.axis_index("sp") * row_slab, row_slab), row_slab)
    copies = start_loads(
        [(first_hbm.at[:, cut], first), (second_hbm.at[:, cut], second)]
        + list(zip((shift_hbm, scale_hbm, gate_hbm), targets)),
        sems,
    )
    copies[0].wait()
    copies[1].wait()
    rows = lax.broadcasted_iota(jnp.int32, (16, row_slab), 0)
    pair = jnp.where(rows == 0, first[...], second[...])
    activated = (pair / (1.0 + jnp.exp(-pair))).astype(jnp.bfloat16)
    out_ref[6:8, :] = jnp.zeros((2, out_ref.shape[1]), jnp.float32)
    for i in range(3):
        copies[2 + i].wait()
        part = jnp.dot(activated, targets[i][...], preferred_element_type=jnp.float32)
        out_ref[2 * i : 2 * i + 2, :] = part[0:2]


def combine_body(one_ref, other_ref, out_ref):
    out_ref[...] = one_ref[...] + other_ref[...]


def combine(one, other, flops):
    return kernel_call(combine_body, jax.ShapeDtypeStruct(one.shape, one.dtype), 2, flops)(
        one, other
    )


def opening(first, second, *weights):
    row_slab, columns = weights[0].shape
    return pl.pallas_call(
        opening_body,
        out_shape=jax.ShapeDtypeStruct((8, columns), jnp.float32),
        in_specs=[hbm_spec()] * 5,
        out_specs=whole_spec(),
        scratch_shapes=[pltpu.VMEM((1, row_slab), jnp.float32)] * 2
        + [pltpu.VMEM((row_slab, columns), jnp.bfloat16)] * 3
        + [pltpu.SemaphoreType.DMA((5,))],
        cost_estimate=pl.CostEstimate(flops=10**8, transcendentals=0, bytes_accessed=0),
        compiler_params=pltpu.CompilerParams(vmem_limit_bytes=ROOMY),
    )(first, second, *weights)


def turn(field, cosine, sine):
    quarter = field.shape[0] // 4
    pieces = [field[i * quarter : (i + 1) * quarter] for i in range(4)]
    swapped = jnp.concatenate([pieces[1], pieces[0], pieces[3], pieces[2]], axis=0)
    return field * cosine + swapped * sine


def projection_body(
    heads,
    kv_heads,
    own_ref,
    context_ref,
    query_ref,
    key_ref,
    value_ref,
    core_ref,
    far_ref,
    both_ref,
    mod_ref,
    gain_ref,
    query_gain_ref,
    key_gain_ref,
    cosine_ref,
    sine_ref,
    q_out,
    kv_out,
):
    span = CHANNEL_SPAN
    group = heads // kv_heads

    def vector(row):
        return jnp.concatenate([mod_ref[i, row : row + 1, :] for i in range(mod_ref.shape[0])], axis=1)

    gain = gain_ref[...]

    def hidden_of(ref, row):
        wide = ref[...].astype(jnp.float32)
        scaled = wide * lax.rsqrt(jnp.mean(wide * wide, axis=-1, keepdims=True) + epsilon)
        return (scaled * (gain * (1.0 + vector(2 + row))) + vector(row)).astype(jnp.bfloat16)

    def normed(raw, head_gain):
        return raw * lax.rsqrt(jnp.mean(raw * raw, axis=0, keepdims=True) + epsilon) * head_gain

    q_out[...] = jnp.zeros_like(q_out)

    def upright(ref):
        return jnp.broadcast_to(ref[...], (8, span)).T[:, 0:1]

    query_gain = upright(query_gain_ref)
    key_gain = upright(key_gain_ref)
    blocks = (own_ref, core_ref, far_ref, both_ref)
    own_rows = own_ref.shape[0]
    tok_count = own_rows * len(blocks)
    for j in (1, 2, 3, 0):
        hidden = hidden_of(blocks[j], 0)
        cosine = cosine_ref[j]
        sine = sine_ref[j]
        queries = jnp.dot(hidden, query_ref[...], preferred_element_type=jnp.float32).T
        for h in range(heads):
            turned = turn(normed(queries[h * span : (h + 1) * span], query_gain), cosine, sine)
            kv, g = h // group, h % group
            lane = g * tok_count + j * own_rows
            q_out[kv, kv * span : (kv + 1) * span, lane : lane + own_rows] = turned.astype(jnp.bfloat16)
        keys = jnp.dot(hidden, key_ref[...], preferred_element_type=jnp.float32).T
        made = [
            turn(normed(keys[h * span : (h + 1) * span], key_gain), cosine, sine)
            for h in range(kv_heads)
        ]
        kv_out[j] = jnp.concatenate(made, axis=0).T.astype(jnp.bfloat16)
        values = jnp.dot(hidden, value_ref[...], preferred_element_type=jnp.float32)
        kv_out[len(blocks) + j] = values.T.astype(jnp.bfloat16)
    hidden = hidden_of(context_ref, 1)
    ctx_rows = context_ref.shape[0]
    keys = jnp.dot(hidden, key_ref[...], preferred_element_type=jnp.float32).T
    made = [normed(keys[h * span : (h + 1) * span], key_gain) for h in range(kv_heads)]
    kv_out[2 * len(blocks), 0:ctx_rows, :] = jnp.concatenate(made, axis=0).T.astype(jnp.bfloat16)
    kv_out[2 * len(blocks), ctx_rows : 2 * ctx_rows, :] = jnp.dot(
        hidden, value_ref[...], preferred_element_type=jnp.float32
    ).astype(jnp.bfloat16)


def attention_body(blocks, first, last, offset, q_tile, *refs):
    q_ref = refs[0]
    kv_refs = refs[1 : 1 + blocks]
    refs = refs[1 + blocks :]
    if not first:
        peak_in, total_in, sum_in = refs[:3]
        refs = refs[3:]
    kv_heads, width, lanes = q_ref.shape
    span = width // kv_heads
    scale = span ** (-0.5) * LOG2E
    parts = (kv_refs[0].shape[0] - 1) // 2
    ctx_rows = kv_refs[0].shape[1] // 2
    chunks = []
    for ref in kv_refs:
        half = parts // 2
        chunks += [(ref, range(half), False), (ref, range(half, parts), True)]
    tiles = [
        (h, lane, chunk)
        for chunk in chunks
        for h in range(kv_heads)
        for lane in range(0, lanes, q_tile)
    ]
    states = {}

    def scores(tile):
        h, lane, (ref, places, context) = tile
        keys = [ref[j] for j in places]
        if context:
            keys.append(ref[2 * parts, 0:ctx_rows, :])
        query = q_ref[h, :, lane : lane + q_tile]
        found = jnp.dot(jnp.concatenate(keys, axis=0), query, preferred_element_type=jnp.float32)
        found = found * scale
        if context:
            rows = found.shape[0] - ctx_rows
            found = jnp.concatenate([found[:rows], found[rows:] + offset * LOG2E], axis=0)
        return found

    def soften(tile, found):
        h, lane, _ = tile
        peak = jnp.max(found, axis=0, keepdims=True)
        old = states.get((h, lane))
        if old is None and not first:
            cut = slice(lane, lane + q_tile)
            old = (peak_in[h, :, cut], total_in[h, :, cut], sum_in[h, :, cut])
        if old is not None:
            peak = jnp.maximum(peak, old[0])
        shares = jnp.exp2(found - peak)
        total = jnp.sum(shares, axis=0, keepdims=True)
        shrink = None
        if old is not None:
            shrink = jnp.exp2(old[0] - peak)
            total = total + old[1] * shrink
        states[(h, lane)] = (peak, total, old[2] if old is not None else None)
        return shares.astype(jnp.bfloat16), shrink

    def gather(tile, shares, shrink):
        h, lane, (ref, places, context) = tile
        rows = slice(h * span, (h + 1) * span)
        values = [ref[parts + j, rows, :] for j in places]
        if context:
            values.append(ref[2 * parts, ctx_rows : 2 * ctx_rows, :].T[rows])
        weighted = jnp.dot(
            jnp.concatenate(values, axis=1), shares, preferred_element_type=jnp.float32
        )
        peak, total, old = states[(h, lane)]
        if shrink is not None:
            weighted = weighted + old * shrink
        states[(h, lane)] = (peak, total, weighted)

    following = scores(tiles[0])
    waiting = None
    for i, tile in enumerate(tiles):
        found = following
        if i + 1 < len(tiles):
            following = scores(tiles[i + 1])
        shares, shrink = soften(tile, found)
        if waiting:
            gather(*waiting)
        waiting = (tile, shares, shrink)
    gather(*waiting)
    for (h, lane), (peak, total, weighted) in states.items():
        cut = slice(lane, lane + q_tile)
        if last:
            (out_ref,) = refs
            attended = (weighted / total).astype(jnp.bfloat16)
            own_rows = out_ref.shape[2]
            group_lanes = own_rows * out_ref.shape[0]
            for at in range(0, q_tile, own_rows):
                g, j = (lane + at) // group_lanes, (lane + at) % group_lanes // own_rows
                head = h * (lanes // group_lanes) + g
                out_ref[j, head * span : (head + 1) * span, :] = attended[:, at : at + own_rows]
        else:
            peak_out, total_out, sum_out = refs
            peak_out[h, :, cut] = peak
            total_out[h, :, cut] = total
            sum_out[h, :, cut] = weighted


def attend(state, probes, pairs, offset, last):
    kv_heads, width, lanes = probes.shape
    span = width // kv_heads
    keys = sum(p.shape[0] // 2 * p.shape[1] + p.shape[1] // 2 for p in pairs)
    inputs = [probes, *pairs] + list(state or ())
    if last:
        out = jax.ShapeDtypeStruct(last, jnp.bfloat16)
    else:
        stat = jax.ShapeDtypeStruct((kv_heads, 1, lanes), jnp.float32)
        out = [stat, stat, jax.ShapeDtypeStruct((kv_heads, span, lanes), jnp.float32)]

    def body(*refs):
        attention_body(len(pairs), state is None, bool(last), offset, 512, *refs)

    return kernel_call(body, out, len(inputs), 40 * kv_heads * lanes * keys * span)(*inputs)


def output_body(latent_ref, mod_ref, weight_ref, *refs):
    out_ref, lhs_ref = refs[-2:]
    parts = refs[:-2]
    head_index = lax.axis_index("tp")
    rows = parts[0].shape[0]
    for j, ref in enumerate(parts):
        at = pl.multiple_of(jnp.bitwise_xor(head_index, j) * rows, rows)
        lhs_ref[pl.ds(at, rows), :] = ref[...]
    lhs = lhs_ref[...].T
    columns = mod_ref.shape[2]
    for i in range(mod_ref.shape[0]):
        cut = slice(i * columns, (i + 1) * columns)
        branch = jnp.dot(lhs, weight_ref[:, cut], preferred_element_type=jnp.float32)
        gate = mod_ref[i, 4:5, :]
        out_ref[:, cut] = (latent_ref[:, cut].astype(jnp.float32) + gate * branch).astype(
            jnp.bfloat16
        )


def fast_device(*args):
    return inner_device(*args)


def xor_move(member, axis, mask):
    size = lax.axis_size(axis)
    return lax.ppermute(member, axis, [(i, i ^ mask) for i in range(size)])


def ring_move(member, step):
    size = lax.axis_size("sp")
    return lax.ppermute(member, "sp", [(i, (i + step) % size) for i in range(size)])


def tables(seq_index, head_index, own_rows, head_split):
    quarter = CHANNEL_SPAN // 4
    blocks = jnp.bitwise_xor(jnp.arange(head_split, dtype=jnp.int32), head_index)
    places = (
        seq_index * own_rows * head_split
        + blocks[:, None] * own_rows
        + jnp.arange(own_rows, dtype=jnp.int32)
    )
    inverse = rope_base ** (-jnp.arange(quarter, dtype=jnp.float32) / quarter)
    grid_row = (places // GRID_W).astype(jnp.float32)[:, None, :] * inverse[:, None]
    grid_col = (places % GRID_W).astype(jnp.float32)[:, None, :] * inverse[:, None]
    row_sine, col_sine = jnp.sin(grid_row), jnp.sin(grid_col)
    row_cosine, col_cosine = jnp.cos(grid_row), jnp.cos(grid_col)
    cosine = jnp.concatenate([row_cosine, row_cosine, col_cosine, col_cosine], axis=1)
    sine = jnp.concatenate([-row_sine, row_sine, -col_sine, col_sine], axis=1)
    return cosine, sine


def inner_device(
    latent,
    context,
    condition,
    context_condition,
    norm_gain,
    shift_weight,
    scale_weight,
    gate_weight,
    query_weight,
    key_weight,
    value_weight,
    query_gain,
    key_gain,
    output_weight,
):
    head_split = lax.axis_size("tp")
    seq_split = lax.axis_size("sp")
    seq_index = lax.axis_index("sp")
    head_index = lax.axis_index("tp")
    own_rows, depth = latent.shape
    ctx_rows = context.shape[0]
    tok_count = own_rows * head_split
    q_heads = query_weight.shape[1] // CHANNEL_SPAN
    kv_heads = key_weight.shape[1] // CHANNEL_SPAN

    part = opening(
        condition.reshape(1, depth),
        context_condition.reshape(1, depth),
        shift_weight,
        scale_weight,
        gate_weight,
    )
    far = xor_move(latent, "tp", 2)
    near = xor_move(latent, "tp", 1)
    mask = seq_split // 2
    while mask:
        other = xor_move(part, "sp", mask)
        part = combine(part, other, 10**11 if 2 * mask == seq_split else 10**6)
        mask //= 2
    both = xor_move(far, "tp", 1)
    modulation = lax.all_gather(part, "tp", axis=0, tiled=False)
    cosine, sine = tables(seq_index, head_index, own_rows, head_split)
    probes, own_pairs = pl.pallas_call(
        lambda *refs: projection_body(q_heads, kv_heads, *refs),
        out_shape=[
            jax.ShapeDtypeStruct(
                (kv_heads, kv_heads * CHANNEL_SPAN, q_heads // kv_heads * tok_count), jnp.bfloat16
            ),
            jax.ShapeDtypeStruct((2 * head_split + 1, own_rows, own_rows), jnp.bfloat16),
        ],
        in_specs=[whole_spec()] * 14,
        out_specs=[whole_spec()] * 2,
        cost_estimate=pl.CostEstimate(
            flops=4 * tok_count * depth * (q_heads + 2 * kv_heads) * CHANNEL_SPAN,
            transcendentals=0,
            bytes_accessed=0,
        ),
        compiler_params=pltpu.CompilerParams(vmem_limit_bytes=48 * 1024 * 1024),
    )(
        latent,
        context,
        query_weight,
        key_weight,
        value_weight,
        near,
        far,
        both,
        modulation,
        norm_gain.reshape(1, depth),
        query_gain.reshape(1, CHANNEL_SPAN),
        key_gain.reshape(1, CHANNEL_SPAN),
        cosine,
        sine,
    )
    offset = math.log(tok_count / (2.0 * ctx_rows))
    near_pairs = xor_move(own_pairs, "sp", 1)
    up = ring_move(own_pairs, 2)
    down = ring_move(own_pairs, -2)
    near_up = xor_move(up, "sp", 1)
    near_down = xor_move(down, "sp", 1)
    across = ring_move(up, 2)
    near_across = xor_move(across, "sp", 1)
    state = attend(None, probes, [own_pairs], offset, None)
    state = attend(state, probes, [near_pairs], offset, None)
    state = attend(state, probes, [up], offset, None)
    state = attend(state, probes, [down, near_up], offset, None)
    state = attend(state, probes, [across, near_down], offset, None)
    attended = attend(
        state, probes, [near_across], offset, (head_split, q_heads * CHANNEL_SPAN, own_rows)
    )
    parts = [attended[0]] + [xor_move(attended[j], "tp", j) for j in range(1, head_split)]
    width = q_heads * CHANNEL_SPAN
    return kernel_call(
        output_body,
        jax.ShapeDtypeStruct(latent.shape, jnp.bfloat16),
        3 + head_split,
        2 * own_rows * depth * width * head_split,
        [pltpu.VMEM((width * head_split, own_rows), jnp.bfloat16)],
    )(latent, modulation, output_weight, *parts)


def suits(mesh, latent, context, query_weight, key_weight):
    seq_split, head_split = mesh.shape["sp"], mesh.shape["tp"]
    own_rows = latent.shape[0] // (seq_split * head_split)
    ctx_rows = context.shape[0] // seq_split
    kv_heads = key_weight.shape[1] // CHANNEL_SPAN // head_split
    return (
        seq_split == 8
        and head_split == 4
        and own_rows == 2 * CHANNEL_SPAN
        and ctx_rows == CHANNEL_SPAN
        and kv_heads == 2
        and query_weight.shape[1] == 2 * key_weight.shape[1]
    )


def solution(mesh):
    in_specs = (
        P(("sp", "tp"), None),
        P("sp", None),
        P(),
        P(),
        P(),
        P("sp", "tp"),
        P("sp", "tp"),
        P("sp", "tp"),
        P(None, "tp"),
        P(None, "tp"),
        P(None, "tp"),
        P(),
        P(),
        P(),
    )
    out_specs = P(("sp", "tp"), None)

    def program(*args):
        fast = suits(mesh, args[0], args[1], args[8], args[9])
        step = jax.shard_map(
            fast_device if fast else general_device,
            mesh=mesh,
            in_specs=in_specs,
            out_specs=out_specs,
            check_vma=False,
        )
        return step(*args)

    return program
```

```python
import math

import jax
import jax.numpy as jnp
from jax import lax
from jax.experimental import pallas as pl
from jax.experimental.pallas import tpu as pltpu
from jax.sharding import PartitionSpec as P


CHANNEL_SPAN = 64
GRID_W = 64


epsilon = 1e-06
rope_base = 10000.0


def modulate(tok_rows, norm_gain, shift_row, scale_row):
    wide = tok_rows.astype(jnp.float32)
    normed = wide * lax.rsqrt(jnp.mean(wide * wide, axis=-1, keepdims=True) + epsilon)
    return (normed * norm_gain * (1.0 + scale_row) + shift_row).astype(jnp.bfloat16)


def headnorm(raw, gain, heads):
    field = raw.reshape(raw.shape[0], heads, -1)
    return field * lax.rsqrt(jnp.mean(field * field, axis=-1, keepdims=True) + epsilon) * gain


def rotate(field, places):
    count = field.shape[0]
    heads = field.shape[1]
    quarter = field.shape[2] // 4
    grid_row = (places // GRID_W).astype(jnp.float32)
    grid_col = (places % GRID_W).astype(jnp.float32)
    inverse = rope_base ** (-jnp.arange(quarter, dtype=jnp.float32) / quarter)
    angles = jnp.stack([grid_row[:, None] * inverse, grid_col[:, None] * inverse], axis=1)[:, None]
    cosine = jnp.cos(angles)
    sine = jnp.sin(angles)
    matcher_content_couples = field.reshape(count, heads, 2, 2, quarter)
    first = matcher_content_couples[:, :, :, 0]
    second = matcher_content_couples[:, :, :, 1]
    turned = jnp.stack([first * cosine - second * sine, second * cosine + first * sine], axis=3)
    return turned.reshape(count, heads, 4 * quarter)


def process_probe_group(
    accumulator_carry, probe_entries, matcher_content_couples, similarity_offset
):
    row_peak, row_total, weighted = accumulator_carry
    kv_heads = probe_entries.shape[1]
    head_size = probe_entries.shape[3]
    pair_width = kv_heads * head_size
    matcher_pieces = matcher_content_couples[:, :pair_width].reshape(
        matcher_content_couples.shape[0], kv_heads, head_size
    )
    value_rows = matcher_content_couples[:, pair_width:].reshape(
        matcher_content_couples.shape[0], kv_heads, head_size
    )
    similarity_matrix = (
        jnp.einsum(
            "dmvk,hmk->dmvh", probe_entries, matcher_pieces, preferred_element_type=jnp.float32
        )
        * head_size ** (-0.5)
        + similarity_offset
    )
    new_peak = jnp.maximum(row_peak, jnp.max(similarity_matrix, axis=-1))
    shares = jnp.exp(similarity_matrix - new_peak[..., None])
    shrink = jnp.exp(row_peak - new_peak)
    row_total = row_total * shrink + jnp.sum(shares, axis=-1)
    weighted = weighted * shrink[..., None] + jnp.einsum(
        "qkgn,nkd->qkgd",
        shares.astype(jnp.bfloat16),
        value_rows,
        preferred_element_type=jnp.float32,
    )
    return (new_peak, row_total, weighted)


def group_walker(accumulator_carry, probe_entries, matcher_content_couples, similarity_offset):
    pair_count = matcher_content_couples.shape[0]
    probe_group_total = -(-pair_count // 2048)
    while pair_count % probe_group_total:
        probe_group_total += 1
    if probe_group_total == 1:
        return process_probe_group(
            accumulator_carry, probe_entries, matcher_content_couples, similarity_offset
        )
    group_extent = pair_count // probe_group_total

    def scan_step(inner, slices):
        return (process_probe_group(inner, probe_entries, slices[0], slices[1]), None)

    result, _ = lax.scan(
        scan_step,
        accumulator_carry,
        (
            matcher_content_couples.reshape(
                probe_group_total, group_extent, matcher_content_couples.shape[1]
            ),
            similarity_offset.reshape(probe_group_total, group_extent),
        ),
    )
    return result


def general_device(
    latent,
    context,
    condition,
    context_condition,
    norm_gain,
    shift_weight,
    scale_weight,
    gate_weight,
    query_weight,
    key_weight,
    value_weight,
    query_gain,
    key_gain,
    output_weight,
):
    head_split = lax.axis_size("tp")
    seq_index = lax.axis_index("sp")
    head_index = lax.axis_index("tp")
    row_slab = shift_weight.shape[0]
    columns = shift_weight.shape[1]
    conditions = jnp.stack([condition, context_condition])
    activated = jax.nn.silu(
        lax.dynamic_slice_in_dim(conditions, seq_index * row_slab, row_slab, 1)
    ).astype(jnp.bfloat16)
    part_shift = jnp.dot(activated, shift_weight, preferred_element_type=jnp.float32)
    part_scale = jnp.dot(activated, scale_weight, preferred_element_type=jnp.float32)
    part_gate = jnp.dot(activated, gate_weight, preferred_element_type=jnp.float32)

    def widen(member):
        blank = jnp.zeros((2, columns * head_split), jnp.float32)
        return lax.dynamic_update_slice_in_dim(blank, member, head_index * columns, 1)

    shifts, scales, gates = lax.psum(
        (widen(part_shift), widen(part_scale), widen(part_gate)), ("sp", "tp")
    )
    own_rows = latent.shape[0]
    tok_count = own_rows * head_split
    ctx_rows = context.shape[0]
    hidden = modulate(latent, norm_gain, shifts[0], scales[0])
    context_hidden = modulate(context, norm_gain, shifts[1], scales[1])
    q_heads = query_weight.shape[1] // CHANNEL_SPAN
    kv_heads = key_weight.shape[1] // CHANNEL_SPAN
    group_size = q_heads // kv_heads
    q_width = q_heads * CHANNEL_SPAN
    kv_width = kv_heads * CHANNEL_SPAN
    joined_weight = jnp.concatenate([query_weight, key_weight, value_weight], axis=1)
    projected = jnp.dot(
        lax.all_gather(hidden, "tp", axis=0, tiled=True),
        joined_weight,
        preferred_element_type=jnp.float32,
    )
    places = seq_index * tok_count + jnp.arange(tok_count, dtype=jnp.int32)
    probe_entries = rotate(headnorm(projected[:, :q_width], query_gain, q_heads), places).astype(
        jnp.bfloat16
    )
    probe_entries = probe_entries.reshape(tok_count, kv_heads, group_size, CHANNEL_SPAN)
    latent_keys = rotate(
        headnorm(projected[:, q_width : q_width + kv_width], key_gain, kv_heads), places
    ).astype(jnp.bfloat16)
    latent_values = projected[:, q_width + kv_width :].astype(jnp.bfloat16)
    own_pairs = jnp.concatenate([latent_keys.reshape(tok_count, kv_width), latent_values], axis=1)
    ctx_projected = jnp.dot(
        context_hidden, joined_weight[:, q_width:], preferred_element_type=jnp.float32
    )
    ctx_keys = (
        headnorm(ctx_projected[:, :kv_width], key_gain, kv_heads)
        .astype(jnp.bfloat16)
        .reshape(ctx_rows, kv_width)
    )
    ctx_pairs = jnp.concatenate(
        [ctx_keys, ctx_projected[:, kv_width:].astype(jnp.bfloat16)], axis=1
    )
    prefix_mapped = math.log(tok_count / (2.0 * ctx_rows))
    stat_shape = (tok_count, kv_heads, group_size)
    start_state = (
        jnp.full(stat_shape, -jnp.inf, jnp.float32),
        jnp.zeros(stat_shape, jnp.float32),
        jnp.zeros(stat_shape + (CHANNEL_SPAN,), jnp.float32),
    )
    ctx_whole = lax.all_gather(ctx_pairs, "sp", axis=0, tiled=True)
    ctx_state = group_walker(
        start_state,
        probe_entries,
        ctx_whole,
        jnp.full((ctx_whole.shape[0],), prefix_mapped, jnp.float32),
    )
    key_piece = lax.all_gather(own_pairs, "sp", axis=0, tiled=True)
    final_state = group_walker(
        ctx_state, probe_entries, key_piece, jnp.zeros((key_piece.shape[0],), jnp.float32)
    )
    _, row_total, weighted = final_state
    attended = (weighted / row_total[..., None]).astype(jnp.bfloat16).reshape(tok_count, q_width)
    branch = jnp.dot(
        lax.all_to_all(attended, "tp", split_axis=0, concat_axis=1, tiled=True),
        output_weight,
        preferred_element_type=jnp.float32,
    )
    return (latent.astype(jnp.float32) + gates[0] * branch).astype(jnp.bfloat16)


LOG2E = math.log2(math.e)


def whole_spec():
    return pl.BlockSpec(memory_space=pltpu.VMEM)


def kernel_call(body, out_shape, count, flops, scratch=()):
    return pl.pallas_call(
        body,
        out_shape=out_shape,
        in_specs=[whole_spec()] * count,
        out_specs=jax.tree.map(lambda unused: whole_spec(), out_shape),
        scratch_shapes=list(scratch),
        cost_estimate=pl.CostEstimate(flops=flops, transcendentals=0, bytes_accessed=0),
        compiler_params=pltpu.CompilerParams(vmem_limit_bytes=48 * 1024 * 1024),
    )


ROOMY = 60 * 1024 * 1024


def hbm_spec():
    return pl.BlockSpec(memory_space=pltpu.HBM)


def start_loads(pairs, sems):
    copies = []
    for i, (source, target) in enumerate(pairs):
        copies.append(pltpu.make_async_copy(source, target, sems.at[i]))
        copies[-1].start()
    return copies


def opening_body(first_hbm, second_hbm, shift_hbm, scale_hbm, gate_hbm, out_ref, *scratch):
    first, second, *targets, sems = scratch
    row_slab = shift_hbm.shape[0]
    cut = pl.ds(pl.multiple_of(lax.axis_index("sp") * row_slab, row_slab), row_slab)
    copies = start_loads(
        [(first_hbm.at[:, cut], first), (second_hbm.at[:, cut], second)]
        + list(zip((shift_hbm, scale_hbm, gate_hbm), targets)),
        sems,
    )
    copies[0].wait()
    copies[1].wait()
    rows = lax.broadcasted_iota(jnp.int32, (16, row_slab), 0)
    pair = jnp.where(rows == 0, first[...], second[...])
    activated = (pair / (1.0 + jnp.exp(-pair))).astype(jnp.bfloat16)
    out_ref[6:8, :] = jnp.zeros((2, out_ref.shape[1]), jnp.float32)
    for i in range(3):
        copies[2 + i].wait()
        part = jnp.dot(activated, targets[i][...], preferred_element_type=jnp.float32)
        out_ref[2 * i : 2 * i + 2, :] = part[0:2]


def combine_body(one_ref, other_ref, out_ref):
    out_ref[...] = one_ref[...] + other_ref[...]


def combine(one, other, flops):
    return kernel_call(combine_body, jax.ShapeDtypeStruct(one.shape, one.dtype), 2, flops)(
        one, other
    )


def opening(first, second, *weights):
    row_slab, columns = weights[0].shape
    return pl.pallas_call(
        opening_body,
        out_shape=jax.ShapeDtypeStruct((8, columns), jnp.float32),
        in_specs=[hbm_spec()] * 5,
        out_specs=whole_spec(),
        scratch_shapes=[pltpu.VMEM((1, row_slab), jnp.float32)] * 2
        + [pltpu.VMEM((row_slab, columns), jnp.bfloat16)] * 3
        + [pltpu.SemaphoreType.DMA((5,))],
        cost_estimate=pl.CostEstimate(flops=10**8, transcendentals=0, bytes_accessed=0),
        compiler_params=pltpu.CompilerParams(vmem_limit_bytes=ROOMY),
    )(first, second, *weights)


def turn(field, cosine, sine):
    quarter = field.shape[0] // 4
    pieces = [field[i * quarter : (i + 1) * quarter] for i in range(4)]
    swapped = jnp.concatenate([pieces[1], pieces[0], pieces[3], pieces[2]], axis=0)
    return field * cosine + swapped * sine


def projection_body(
    heads,
    kv_heads,
    own_ref,
    context_ref,
    query_ref,
    key_ref,
    value_ref,
    core_ref,
    far_ref,
    both_ref,
    mod_ref,
    gain_ref,
    query_gain_ref,
    key_gain_ref,
    cosine_ref,
    sine_ref,
    keep_q,
    keep_kv,
    give,
    made,
):
    span = CHANNEL_SPAN
    group = heads // kv_heads

    def vector(row):
        return jnp.concatenate([mod_ref[i, row : row + 1, :] for i in range(mod_ref.shape[0])], axis=1)

    gain = gain_ref[...]

    def hidden_of(ref, row):
        wide = ref[...].astype(jnp.float32)
        scaled = wide * lax.rsqrt(jnp.mean(wide * wide, axis=-1, keepdims=True) + epsilon)
        return (scaled * (gain * (1.0 + vector(2 + row))) + vector(row)).astype(jnp.bfloat16)

    def normed(raw, head_gain):
        return raw * lax.rsqrt(jnp.mean(raw * raw, axis=0, keepdims=True) + epsilon) * head_gain

    def upright(ref):
        return jnp.broadcast_to(ref[...], (8, span)).T[:, 0:1]

    query_gain = upright(query_gain_ref)
    key_gain = upright(key_gain_ref)
    blocks = (own_ref, core_ref, far_ref, both_ref)
    q_tiles = group * len(blocks) // 2
    waiting = {}
    for j, ref in enumerate(blocks):
        hidden = hidden_of(ref, 0)
        cosine = cosine_ref[j]
        sine = sine_ref[j]
        rows = slice(j % 2 * span, (j % 2 + 1) * span)
        queries = jnp.dot(hidden, query_ref[...], preferred_element_type=jnp.float32).T
        for h in range(heads):
            turned = turn(normed(queries[h * span : (h + 1) * span], query_gain), cosine, sine)
            kv, g = h // group, h % group
            made[kv, g * len(blocks) // 2 + j // 2, rows, :] = turned.astype(jnp.bfloat16)
        keys = jnp.dot(hidden, key_ref[...], preferred_element_type=jnp.float32).T
        values = jnp.dot(hidden, value_ref[...], preferred_element_type=jnp.float32).T
        for h in range(kv_heads):
            cut = slice(h * span, (h + 1) * span)
            turned = turn(normed(keys[cut], key_gain), cosine, sine)
            if j % 2:
                pair = jnp.concatenate([waiting[h], turned], axis=0)
                made[h, q_tiles + j // 2] = pair.T.astype(jnp.bfloat16)
            waiting[h] = turned
            made[h, q_tiles + len(blocks) // 2 + j // 2, rows, :] = values[cut].astype(jnp.bfloat16)
    hidden = hidden_of(context_ref, 1)
    keys = jnp.dot(hidden, key_ref[...], preferred_element_type=jnp.float32).T
    values = jnp.dot(hidden, value_ref[...], preferred_element_type=jnp.float32).T
    for h in range(kv_heads):
        cut = slice(h * span, (h + 1) * span)
        both = jnp.concatenate([normed(keys[cut], key_gain).T, values[cut]], axis=0)
        made[h, q_tiles + len(blocks)] = jnp.concatenate([both, jnp.zeros_like(both)], axis=1).astype(
            jnp.bfloat16
        )
    side = lax.rem(lax.axis_index("sp"), kv_heads)
    for i in range(q_tiles):
        keep_q[i] = made[side, i]
    for i in range(keep_kv.shape[0]):
        keep_kv[i] = made[side, q_tiles + i]
    for i in range(give.shape[0]):
        give[i] = made[1 - side, i]


def attention_body(bases, first, last, offset, *refs):
    q_ref = refs[0]
    kv_refs = refs[1 : 1 + len(bases)]
    refs = refs[1 + len(bases) :]
    if not first:
        peak_in, total_in, sum_in = refs[:3]
        refs = refs[3:]
    span = q_ref.shape[1] // 2
    scale = span ** (-0.5) * LOG2E
    groups = 2
    pairs = 2
    chunks = [(ref, base, part) for ref, base in zip(kv_refs, bases) for part in (0, 1)]
    tiles = [(g, chunk) for chunk in chunks for g in range(groups)]
    states = {}
    queries = {}
    for g in range(groups):
        found = jnp.concatenate(
            [
                q_ref[g * pairs + p, half * span : (half + 1) * span, :]
                for p in range(pairs)
                for half in (0, 1)
            ],
            axis=1,
        )
        blank = jnp.zeros_like(found)
        queries[g, 0] = jnp.concatenate([found, blank], axis=0)
        queries[g, 1] = jnp.concatenate([blank, found], axis=0)

    def scores(tile):
        g, (ref, base, part) = tile
        keys = [ref[base + p] for p in range(pairs)]
        if part == 0:
            keys.append(ref[base + 2 * pairs, 0:span, :])
        found = jnp.dot(
            jnp.concatenate(keys, axis=0), queries[g, part], preferred_element_type=jnp.float32
        )
        found = found * scale
        if part == 0:
            rows = found.shape[0] - span
            found = jnp.concatenate([found[:rows], found[rows:] + offset * LOG2E], axis=0)
        return found

    def soften(tile, found):
        g = tile[0]
        peak = jnp.max(found, axis=0, keepdims=True)
        old = states.get(g)
        if old is None and not first:
            old = (peak_in[g], total_in[g], sum_in[g])
        if old is not None:
            peak = jnp.maximum(peak, old[0])
        shares = jnp.exp2(found - peak)
        total = jnp.sum(shares, axis=0, keepdims=True)
        shrink = None
        if old is not None:
            shrink = jnp.exp2(old[0] - peak)
            total = total + old[1] * shrink
        states[g] = (peak, total, old[2] if old is not None else None)
        return shares.astype(jnp.bfloat16), shrink

    def gather(tile, shares, shrink):
        g, (ref, base, part) = tile
        rows = slice(part * span, (part + 1) * span)
        values = [ref[base + pairs + p, rows, :] for p in range(pairs)]
        if part == 0:
            values.append(ref[base + 2 * pairs, span : 2 * span, 0:span])
        weighted = jnp.dot(
            jnp.concatenate(values, axis=1), shares, preferred_element_type=jnp.float32
        )
        peak, total, old = states[g]
        if shrink is not None:
            weighted = weighted + old * shrink
        states[g] = (peak, total, weighted)

    following = scores(tiles[0])
    waiting = None
    for i, tile in enumerate(tiles):
        found = following
        if i + 1 < len(tiles):
            following = scores(tiles[i + 1])
        shares, shrink = soften(tile, found)
        if waiting:
            gather(*waiting)
        waiting = (tile, shares, shrink)
    gather(*waiting)
    for g, (peak, total, weighted) in states.items():
        if last:
            (out_ref,) = refs
            attended = (weighted / total).astype(jnp.bfloat16)
            own_rows = out_ref.shape[2]
            for j in range(out_ref.shape[0]):
                out_ref[j, g * span : (g + 1) * span, :] = attended[
                    :, j * own_rows : (j + 1) * own_rows
                ]
        else:
            peak_out, total_out, sum_out = refs
            peak_out[g] = peak
            total_out[g] = total
            sum_out[g] = weighted


def attend(state, probes, pairs, offset, last=False):
    lanes = 2 * 2 * probes.shape[2]
    span = probes.shape[1] // 2
    keys = sum(lanes + span for unused in pairs)
    inputs = [probes, *(ref for ref, unused in pairs)] + list(state or ())
    if last:
        out = jax.ShapeDtypeStruct((4, 2 * span, probes.shape[2]), jnp.bfloat16)
    else:
        stat = jax.ShapeDtypeStruct((2, 1, lanes), jnp.float32)
        out = [stat, stat, jax.ShapeDtypeStruct((2, span, lanes), jnp.float32)]

    def body(*refs):
        attention_body([base for unused, base in pairs], state is None, last, offset, *refs)

    return kernel_call(body, out, len(inputs), 40 * 2 * lanes * keys * span)(*inputs)


def output_body(latent_ref, mod_ref, weight_ref, *refs):
    out_ref, lhs_ref = refs[-2:]
    parts = refs[:-2]
    head_index = lax.axis_index("tp")
    side = lax.rem(lax.axis_index("sp"), 2)
    rows = parts[0].shape[0]
    for i, ref in enumerate(parts):
        j, flip = i % (len(parts) // 2), i // (len(parts) // 2)
        place = jnp.bitwise_xor(head_index, j) * 2 + jnp.bitwise_xor(side, flip)
        lhs_ref[pl.ds(pl.multiple_of(place * rows, rows), rows), :] = ref[...]
    lhs = lhs_ref[...].T
    columns = mod_ref.shape[2]
    for i in range(mod_ref.shape[0]):
        cut = slice(i * columns, (i + 1) * columns)
        branch = jnp.dot(lhs, weight_ref[:, cut], preferred_element_type=jnp.float32)
        gate = mod_ref[i, 4:5, :]
        out_ref[:, cut] = (latent_ref[:, cut].astype(jnp.float32) + gate * branch).astype(
            jnp.bfloat16
        )


def fast_device(*args):
    return inner_device(*args)


def xor_move(member, axis, mask):
    size = lax.axis_size(axis)
    return lax.ppermute(member, axis, [(i, i ^ mask) for i in range(size)])


def cross_move(member, mask):
    seq_split, head_split = lax.axis_size("sp"), lax.axis_size("tp")
    pairs = [
        (i * head_split + j, (i ^ 1) * head_split + (j ^ mask))
        for i in range(seq_split)
        for j in range(head_split)
    ]
    return lax.ppermute(member, ("sp", "tp"), pairs)


def ring_move(member, step):
    size = lax.axis_size("sp")
    return lax.ppermute(member, "sp", [(i, (i + step) % size) for i in range(size)])


def tables(seq_index, head_index, own_rows, head_split):
    quarter = CHANNEL_SPAN // 4
    blocks = jnp.bitwise_xor(jnp.arange(head_split, dtype=jnp.int32), head_index)
    places = (
        seq_index * own_rows * head_split
        + blocks[:, None] * own_rows
        + jnp.arange(own_rows, dtype=jnp.int32)
    )
    inverse = rope_base ** (-jnp.arange(quarter, dtype=jnp.float32) / quarter)
    grid_row = (places // GRID_W).astype(jnp.float32)[:, None, :] * inverse[:, None]
    grid_col = (places % GRID_W).astype(jnp.float32)[:, None, :] * inverse[:, None]
    row_sine, col_sine = jnp.sin(grid_row), jnp.sin(grid_col)
    row_cosine, col_cosine = jnp.cos(grid_row), jnp.cos(grid_col)
    cosine = jnp.concatenate([row_cosine, row_cosine, col_cosine, col_cosine], axis=1)
    sine = jnp.concatenate([-row_sine, row_sine, -col_sine, col_sine], axis=1)
    return cosine, sine


def inner_device(
    latent,
    context,
    condition,
    context_condition,
    norm_gain,
    shift_weight,
    scale_weight,
    gate_weight,
    query_weight,
    key_weight,
    value_weight,
    query_gain,
    key_gain,
    output_weight,
):
    head_split = lax.axis_size("tp")
    seq_split = lax.axis_size("sp")
    seq_index = lax.axis_index("sp")
    head_index = lax.axis_index("tp")
    own_rows, depth = latent.shape
    ctx_rows = context.shape[0]
    tok_count = own_rows * head_split
    q_heads = query_weight.shape[1] // CHANNEL_SPAN
    kv_heads = key_weight.shape[1] // CHANNEL_SPAN

    part = opening(
        condition.reshape(1, depth),
        context_condition.reshape(1, depth),
        shift_weight,
        scale_weight,
        gate_weight,
    )
    far = xor_move(latent, "tp", 2)
    near = xor_move(latent, "tp", 1)
    mask = seq_split // 2
    while mask:
        other = xor_move(part, "sp", mask)
        part = combine(part, other, 10**11 if 2 * mask == seq_split else 10**6)
        mask //= 2
    both = xor_move(far, "tp", 1)
    modulation = lax.all_gather(part, "tp", axis=0, tiled=False)
    cosine, sine = tables(seq_index, head_index, own_rows, head_split)
    q_tiles = q_heads // kv_heads * head_split // 2
    kv_tiles = head_split + 1
    tile = (own_rows, own_rows)
    keep_q, keep_kv, give = pl.pallas_call(
        lambda *refs: projection_body(q_heads, kv_heads, *refs),
        out_shape=[
            jax.ShapeDtypeStruct((count, *tile), jnp.bfloat16)
            for count in (q_tiles, kv_tiles, q_tiles + kv_tiles)
        ],
        in_specs=[whole_spec()] * 14,
        out_specs=[whole_spec()] * 3,
        scratch_shapes=[pltpu.VMEM((kv_heads, q_tiles + kv_tiles, *tile), jnp.bfloat16)],
        cost_estimate=pl.CostEstimate(
            flops=4 * tok_count * depth * (q_heads + 2 * kv_heads) * CHANNEL_SPAN,
            transcendentals=0,
            bytes_accessed=0,
        ),
        compiler_params=pltpu.CompilerParams(vmem_limit_bytes=48 * 1024 * 1024),
    )(
        latent,
        context,
        query_weight,
        key_weight,
        value_weight,
        near,
        far,
        both,
        modulation,
        norm_gain.reshape(1, depth),
        query_gain.reshape(1, CHANNEL_SPAN),
        key_gain.reshape(1, CHANNEL_SPAN),
        cosine,
        sine,
    )
    offset = math.log(tok_count / (2.0 * ctx_rows))
    near = xor_move(give, "sp", 1)
    up = ring_move(keep_kv, 2)
    down = ring_move(keep_kv, -2)
    near_kv = near[q_tiles:]
    near_up = ring_move(near_kv, 2)
    near_down = ring_move(near_kv, -2)
    across = ring_move(up, 2)
    near_across = ring_move(near_up, 2)
    own = attend(None, keep_q, [(keep_kv, 0)], offset)
    other = attend(None, near, [(keep_kv, 0), (near, q_tiles)], offset)
    own = attend(own, keep_q, [(near, q_tiles)], offset)
    for group in ([up, down], [across, near_up], [near_down]):
        pieces = [(piece, 0) for piece in group]
        other = attend(other, near, pieces, offset)
        own = attend(own, keep_q, pieces, offset)
    other = attend(other, near, [(near_across, 0)], offset, True)
    own = attend(own, keep_q, [(near_across, 0)], offset, True)
    sent = [cross_move(other[j], j) for j in range(head_split)]
    parts = [own[0]] + [xor_move(own[j], "tp", j) for j in range(1, head_split)] + sent
    width = q_heads * CHANNEL_SPAN
    return kernel_call(
        output_body,
        jax.ShapeDtypeStruct(latent.shape, jnp.bfloat16),
        3 + len(parts),
        2 * own_rows * depth * width * head_split,
        [pltpu.VMEM((width * head_split, own_rows), jnp.bfloat16)],
    )(latent, modulation, output_weight, *parts)


def suits(mesh, latent, context, query_weight, key_weight):
    seq_split, head_split = mesh.shape["sp"], mesh.shape["tp"]
    own_rows = latent.shape[0] // (seq_split * head_split)
    ctx_rows = context.shape[0] // seq_split
    kv_heads = key_weight.shape[1] // CHANNEL_SPAN // head_split
    return (
        seq_split == 8
        and head_split == 4
        and own_rows == 2 * CHANNEL_SPAN
        and ctx_rows == CHANNEL_SPAN
        and kv_heads == 2
        and query_weight.shape[1] == 2 * key_weight.shape[1]
    )


def solution(mesh):
    in_specs = (
        P(("sp", "tp"), None),
        P("sp", None),
        P(),
        P(),
        P(),
        P("sp", "tp"),
        P("sp", "tp"),
        P("sp", "tp"),
        P(None, "tp"),
        P(None, "tp"),
        P(None, "tp"),
        P(),
        P(),
        P(),
    )
    out_specs = P(("sp", "tp"), None)

    def program(*args):
        fast = suits(mesh, args[0], args[1], args[8], args[9])
        step = jax.shard_map(
            fast_device if fast else general_device,
            mesh=mesh,
            in_specs=in_specs,
            out_specs=out_specs,
            check_vma=False,
        )
        return step(*args)

    return program
```

```python
import math

import jax
import jax.numpy as jnp
from jax import lax
from jax.experimental import pallas as pl
from jax.experimental.pallas import tpu as pltpu
from jax.sharding import PartitionSpec as P


CHANNEL_SPAN = 64
GRID_W = 64


epsilon = 1e-06
rope_base = 10000.0


def modulate(tok_rows, norm_gain, shift_row, scale_row):
    wide = tok_rows.astype(jnp.float32)
    normed = wide * lax.rsqrt(jnp.mean(wide * wide, axis=-1, keepdims=True) + epsilon)
    return (normed * norm_gain * (1.0 + scale_row) + shift_row).astype(jnp.bfloat16)


def headnorm(raw, gain, heads):
    field = raw.reshape(raw.shape[0], heads, -1)
    return field * lax.rsqrt(jnp.mean(field * field, axis=-1, keepdims=True) + epsilon) * gain


def rotate(field, places):
    count = field.shape[0]
    heads = field.shape[1]
    quarter = field.shape[2] // 4
    grid_row = (places // GRID_W).astype(jnp.float32)
    grid_col = (places % GRID_W).astype(jnp.float32)
    inverse = rope_base ** (-jnp.arange(quarter, dtype=jnp.float32) / quarter)
    angles = jnp.stack([grid_row[:, None] * inverse, grid_col[:, None] * inverse], axis=1)[:, None]
    cosine = jnp.cos(angles)
    sine = jnp.sin(angles)
    matcher_content_couples = field.reshape(count, heads, 2, 2, quarter)
    first = matcher_content_couples[:, :, :, 0]
    second = matcher_content_couples[:, :, :, 1]
    turned = jnp.stack([first * cosine - second * sine, second * cosine + first * sine], axis=3)
    return turned.reshape(count, heads, 4 * quarter)


def process_probe_group(
    accumulator_carry, probe_entries, matcher_content_couples, similarity_offset
):
    row_peak, row_total, weighted = accumulator_carry
    kv_heads = probe_entries.shape[1]
    head_size = probe_entries.shape[3]
    pair_width = kv_heads * head_size
    matcher_pieces = matcher_content_couples[:, :pair_width].reshape(
        matcher_content_couples.shape[0], kv_heads, head_size
    )
    value_rows = matcher_content_couples[:, pair_width:].reshape(
        matcher_content_couples.shape[0], kv_heads, head_size
    )
    similarity_matrix = (
        jnp.einsum(
            "dmvk,hmk->dmvh", probe_entries, matcher_pieces, preferred_element_type=jnp.float32
        )
        * head_size ** (-0.5)
        + similarity_offset
    )
    new_peak = jnp.maximum(row_peak, jnp.max(similarity_matrix, axis=-1))
    shares = jnp.exp(similarity_matrix - new_peak[..., None])
    shrink = jnp.exp(row_peak - new_peak)
    row_total = row_total * shrink + jnp.sum(shares, axis=-1)
    weighted = weighted * shrink[..., None] + jnp.einsum(
        "qkgn,nkd->qkgd",
        shares.astype(jnp.bfloat16),
        value_rows,
        preferred_element_type=jnp.float32,
    )
    return (new_peak, row_total, weighted)


def group_walker(accumulator_carry, probe_entries, matcher_content_couples, similarity_offset):
    pair_count = matcher_content_couples.shape[0]
    probe_group_total = -(-pair_count // 2048)
    while pair_count % probe_group_total:
        probe_group_total += 1
    if probe_group_total == 1:
        return process_probe_group(
            accumulator_carry, probe_entries, matcher_content_couples, similarity_offset
        )
    group_extent = pair_count // probe_group_total

    def scan_step(inner, slices):
        return (process_probe_group(inner, probe_entries, slices[0], slices[1]), None)

    result, _ = lax.scan(
        scan_step,
        accumulator_carry,
        (
            matcher_content_couples.reshape(
                probe_group_total, group_extent, matcher_content_couples.shape[1]
            ),
            similarity_offset.reshape(probe_group_total, group_extent),
        ),
    )
    return result


def general_device(
    latent,
    context,
    condition,
    context_condition,
    norm_gain,
    shift_weight,
    scale_weight,
    gate_weight,
    query_weight,
    key_weight,
    value_weight,
    query_gain,
    key_gain,
    output_weight,
):
    head_split = lax.axis_size("tp")
    seq_index = lax.axis_index("sp")
    head_index = lax.axis_index("tp")
    row_slab = shift_weight.shape[0]
    columns = shift_weight.shape[1]
    conditions = jnp.stack([condition, context_condition])
    activated = jax.nn.silu(
        lax.dynamic_slice_in_dim(conditions, seq_index * row_slab, row_slab, 1)
    ).astype(jnp.bfloat16)
    part_shift = jnp.dot(activated, shift_weight, preferred_element_type=jnp.float32)
    part_scale = jnp.dot(activated, scale_weight, preferred_element_type=jnp.float32)
    part_gate = jnp.dot(activated, gate_weight, preferred_element_type=jnp.float32)

    def widen(member):
        blank = jnp.zeros((2, columns * head_split), jnp.float32)
        return lax.dynamic_update_slice_in_dim(blank, member, head_index * columns, 1)

    shifts, scales, gates = lax.psum(
        (widen(part_shift), widen(part_scale), widen(part_gate)), ("sp", "tp")
    )
    own_rows = latent.shape[0]
    tok_count = own_rows * head_split
    ctx_rows = context.shape[0]
    hidden = modulate(latent, norm_gain, shifts[0], scales[0])
    context_hidden = modulate(context, norm_gain, shifts[1], scales[1])
    q_heads = query_weight.shape[1] // CHANNEL_SPAN
    kv_heads = key_weight.shape[1] // CHANNEL_SPAN
    group_size = q_heads // kv_heads
    q_width = q_heads * CHANNEL_SPAN
    kv_width = kv_heads * CHANNEL_SPAN
    joined_weight = jnp.concatenate([query_weight, key_weight, value_weight], axis=1)
    projected = jnp.dot(
        lax.all_gather(hidden, "tp", axis=0, tiled=True),
        joined_weight,
        preferred_element_type=jnp.float32,
    )
    places = seq_index * tok_count + jnp.arange(tok_count, dtype=jnp.int32)
    probe_entries = rotate(headnorm(projected[:, :q_width], query_gain, q_heads), places).astype(
        jnp.bfloat16
    )
    probe_entries = probe_entries.reshape(tok_count, kv_heads, group_size, CHANNEL_SPAN)
    latent_keys = rotate(
        headnorm(projected[:, q_width : q_width + kv_width], key_gain, kv_heads), places
    ).astype(jnp.bfloat16)
    latent_values = projected[:, q_width + kv_width :].astype(jnp.bfloat16)
    own_pairs = jnp.concatenate([latent_keys.reshape(tok_count, kv_width), latent_values], axis=1)
    ctx_projected = jnp.dot(
        context_hidden, joined_weight[:, q_width:], preferred_element_type=jnp.float32
    )
    ctx_keys = (
        headnorm(ctx_projected[:, :kv_width], key_gain, kv_heads)
        .astype(jnp.bfloat16)
        .reshape(ctx_rows, kv_width)
    )
    ctx_pairs = jnp.concatenate(
        [ctx_keys, ctx_projected[:, kv_width:].astype(jnp.bfloat16)], axis=1
    )
    prefix_mapped = math.log(tok_count / (2.0 * ctx_rows))
    stat_shape = (tok_count, kv_heads, group_size)
    start_state = (
        jnp.full(stat_shape, -jnp.inf, jnp.float32),
        jnp.zeros(stat_shape, jnp.float32),
        jnp.zeros(stat_shape + (CHANNEL_SPAN,), jnp.float32),
    )
    ctx_whole = lax.all_gather(ctx_pairs, "sp", axis=0, tiled=True)
    ctx_state = group_walker(
        start_state,
        probe_entries,
        ctx_whole,
        jnp.full((ctx_whole.shape[0],), prefix_mapped, jnp.float32),
    )
    key_piece = lax.all_gather(own_pairs, "sp", axis=0, tiled=True)
    final_state = group_walker(
        ctx_state, probe_entries, key_piece, jnp.zeros((key_piece.shape[0],), jnp.float32)
    )
    _, row_total, weighted = final_state
    attended = (weighted / row_total[..., None]).astype(jnp.bfloat16).reshape(tok_count, q_width)
    branch = jnp.dot(
        lax.all_to_all(attended, "tp", split_axis=0, concat_axis=1, tiled=True),
        output_weight,
        preferred_element_type=jnp.float32,
    )
    return (latent.astype(jnp.float32) + gates[0] * branch).astype(jnp.bfloat16)


LOG2E = math.log2(math.e)


def whole_spec():
    return pl.BlockSpec(memory_space=pltpu.VMEM)


def kernel_call(body, out_shape, count, flops, scratch=()):
    return pl.pallas_call(
        body,
        out_shape=out_shape,
        in_specs=[whole_spec()] * count,
        out_specs=jax.tree.map(lambda unused: whole_spec(), out_shape),
        scratch_shapes=list(scratch),
        cost_estimate=pl.CostEstimate(flops=flops, transcendentals=0, bytes_accessed=0),
        compiler_params=pltpu.CompilerParams(vmem_limit_bytes=48 * 1024 * 1024),
    )


ROOMY = 60 * 1024 * 1024


def hbm_spec():
    return pl.BlockSpec(memory_space=pltpu.HBM)


def start_loads(pairs, sems):
    copies = []
    for i, (source, target) in enumerate(pairs):
        copies.append(pltpu.make_async_copy(source, target, sems.at[i]))
        copies[-1].start()
    return copies


def opening_body(first_hbm, second_hbm, shift_hbm, scale_hbm, gate_hbm, out_ref, *scratch):
    first, second, *targets, sems = scratch
    row_slab = shift_hbm.shape[0]
    cut = pl.ds(pl.multiple_of(lax.axis_index("sp") * row_slab, row_slab), row_slab)
    copies = start_loads(
        [(first_hbm.at[:, cut], first), (second_hbm.at[:, cut], second)]
        + list(zip((shift_hbm, scale_hbm, gate_hbm), targets)),
        sems,
    )
    copies[0].wait()
    copies[1].wait()
    rows = lax.broadcasted_iota(jnp.int32, (16, row_slab), 0)
    pair = jnp.where(rows == 0, first[...], second[...])
    activated = (pair / (1.0 + jnp.exp(-pair))).astype(jnp.bfloat16)
    out_ref[6:8, :] = jnp.zeros((2, out_ref.shape[1]), jnp.float32)
    for i in range(3):
        copies[2 + i].wait()
        part = jnp.dot(activated, targets[i][...], preferred_element_type=jnp.float32)
        out_ref[2 * i : 2 * i + 2, :] = part[0:2]


def combine_body(one_ref, other_ref, out_ref):
    out_ref[...] = one_ref[...] + other_ref[...]


def combine(one, other, flops):
    return kernel_call(combine_body, jax.ShapeDtypeStruct(one.shape, one.dtype), 2, flops)(
        one, other
    )


def opening(first, second, *weights):
    row_slab, columns = weights[0].shape
    return pl.pallas_call(
        opening_body,
        out_shape=jax.ShapeDtypeStruct((8, columns), jnp.float32),
        in_specs=[hbm_spec()] * 5,
        out_specs=whole_spec(),
        scratch_shapes=[pltpu.VMEM((1, row_slab), jnp.float32)] * 2
        + [pltpu.VMEM((row_slab, columns), jnp.bfloat16)] * 3
        + [pltpu.SemaphoreType.DMA((5,))],
        cost_estimate=pl.CostEstimate(flops=10**8, transcendentals=0, bytes_accessed=0),
        compiler_params=pltpu.CompilerParams(vmem_limit_bytes=ROOMY),
    )(first, second, *weights)


def turn(field, cosine, sine):
    quarter = field.shape[0] // 4
    pieces = [field[i * quarter : (i + 1) * quarter] for i in range(4)]
    swapped = jnp.concatenate([pieces[1], pieces[0], pieces[3], pieces[2]], axis=0)
    return field * cosine + swapped * sine


def projection_body(
    heads,
    kv_heads,
    own_ref,
    context_ref,
    query_ref,
    key_ref,
    value_ref,
    core_ref,
    far_ref,
    both_ref,
    mod_ref,
    gain_ref,
    query_gain_ref,
    key_gain_ref,
    cosine_ref,
    sine_ref,
    keep_q,
    keep_kv,
    keep_ctx,
    give_q,
    give_kv,
    made,
):
    span = CHANNEL_SPAN
    group = heads // kv_heads

    def vector(row):
        return jnp.concatenate([mod_ref[i, row : row + 1, :] for i in range(mod_ref.shape[0])], axis=1)

    gain = gain_ref[...]

    def hidden_of(ref, row):
        wide = ref[...].astype(jnp.float32)
        scaled = wide * lax.rsqrt(jnp.mean(wide * wide, axis=-1, keepdims=True) + epsilon)
        return (scaled * (gain * (1.0 + vector(2 + row))) + vector(row)).astype(jnp.bfloat16)

    def normed(raw, head_gain):
        return raw * lax.rsqrt(jnp.mean(raw * raw, axis=0, keepdims=True) + epsilon) * head_gain

    def upright(ref):
        return jnp.broadcast_to(ref[...], (8, span)).T[:, 0:1]

    query_gain = upright(query_gain_ref)
    key_gain = upright(key_gain_ref)
    blocks = (own_ref, core_ref, far_ref, both_ref)
    q_tiles = group * len(blocks) // 2
    waiting = {}
    for j, ref in enumerate(blocks):
        hidden = hidden_of(ref, 0)
        cosine = cosine_ref[j]
        sine = sine_ref[j]
        rows = slice(j % 2 * span, (j % 2 + 1) * span)
        queries = jnp.dot(hidden, query_ref[...], preferred_element_type=jnp.float32).T
        for h in range(heads):
            turned = turn(normed(queries[h * span : (h + 1) * span], query_gain), cosine, sine)
            kv, g = h // group, h % group
            made[kv, g * len(blocks) // 2 + j // 2, rows, :] = turned.astype(jnp.bfloat16)
        keys = jnp.dot(hidden, key_ref[...], preferred_element_type=jnp.float32).T
        values = jnp.dot(hidden, value_ref[...], preferred_element_type=jnp.float32).T
        for h in range(kv_heads):
            cut = slice(h * span, (h + 1) * span)
            turned = turn(normed(keys[cut], key_gain), cosine, sine)
            if j % 2:
                pair = jnp.concatenate([waiting[h], turned], axis=0)
                made[h, q_tiles + j // 2] = pair.T.astype(jnp.bfloat16)
            waiting[h] = turned
            made[h, q_tiles + len(blocks) // 2 + j // 2, rows, :] = values[cut].astype(jnp.bfloat16)
    hidden = hidden_of(context_ref, 1)
    keys = jnp.dot(hidden, key_ref[...], preferred_element_type=jnp.float32).T
    values = jnp.dot(hidden, value_ref[...], preferred_element_type=jnp.float32).T
    for h in range(kv_heads):
        cut = slice(h * span, (h + 1) * span)
        both = jnp.concatenate([normed(keys[cut], key_gain).T, values[cut]], axis=0)
        made[h, q_tiles + len(blocks)] = jnp.concatenate([both, jnp.zeros_like(both)], axis=1).astype(
            jnp.bfloat16
        )
    side = lax.rem(lax.axis_index("sp"), kv_heads)
    for head, q_ref, kv_ref in ((1 - side, give_q, give_kv), (side, keep_q, keep_kv)):
        for i in range(q_tiles):
            q_ref[i] = made[head, i]
        for i in range(kv_ref.shape[0]):
            kv_ref[i] = made[head, q_tiles + i]
    keep_ctx[...] = made[side, q_tiles + len(blocks)]


def merge_body(near_ref, ctx_ref, out_ref):
    last = near_ref.shape[0] - 1
    span = ctx_ref.shape[1] // 2
    for i in range(last):
        out_ref[i] = near_ref[i]
    out_ref[last] = jnp.concatenate([near_ref[last, :, 0:span], ctx_ref[:, 0:span]], axis=1)


def merge(near, ctx):
    return kernel_call(merge_body, jax.ShapeDtypeStruct(near.shape, near.dtype), 2, 10**6)(near, ctx)


def attention_body(count, first, last, offset, *refs):
    q_ref = refs[0]
    kv_refs = refs[1 : 1 + count]
    refs = refs[1 + count :]
    if not first:
        peak_in, total_in, sum_in = refs[:3]
        refs = refs[3:]
    span = q_ref.shape[1] // 2
    scale = span ** (-0.5) * LOG2E
    groups = 2
    pairs = 2
    chunks = [(ref, part, ref.shape[0] > 2 * pairs) for ref in kv_refs for part in (0, 1)]
    tiles = [(g, chunk) for chunk in chunks for g in range(groups)]
    states = {}
    queries = {}
    for g in range(groups):
        found = jnp.concatenate(
            [
                q_ref[g * pairs + p, half * span : (half + 1) * span, :]
                for p in range(pairs)
                for half in (0, 1)
            ],
            axis=1,
        )
        blank = jnp.zeros_like(found)
        queries[g, 0] = jnp.concatenate([found, blank], axis=0)
        queries[g, 1] = jnp.concatenate([blank, found], axis=0)

    def scores(tile):
        g, (ref, part, context) = tile
        keys = [ref[p] for p in range(pairs)]
        if context:
            keys.append(ref[2 * pairs, 0:span, :])
        found = jnp.dot(
            jnp.concatenate(keys, axis=0), queries[g, part], preferred_element_type=jnp.float32
        )
        found = found * scale
        if context:
            rows = found.shape[0] - span
            found = jnp.concatenate([found[:rows], found[rows:] + offset * LOG2E], axis=0)
        return found

    def soften(tile, found):
        g = tile[0]
        peak = jnp.max(found, axis=0, keepdims=True)
        old = states.get(g)
        if old is None and not first:
            old = (peak_in[g], total_in[g], sum_in[g])
        if old is not None:
            peak = jnp.maximum(peak, old[0])
        shares = jnp.exp2(found - peak)
        total = jnp.sum(shares, axis=0, keepdims=True)
        shrink = None
        if old is not None:
            shrink = jnp.exp2(old[0] - peak)
            total = total + old[1] * shrink
        states[g] = (peak, total, old[2] if old is not None else None)
        return shares.astype(jnp.bfloat16), shrink

    def gather(tile, shares, shrink):
        g, (ref, part, context) = tile
        rows = slice(part * span, (part + 1) * span)
        values = [ref[pairs + p, rows, :] for p in range(pairs)]
        if context:
            values.append(ref[2 * pairs, span : 2 * span, rows])
        weighted = jnp.dot(
            jnp.concatenate(values, axis=1), shares, preferred_element_type=jnp.float32
        )
        peak, total, old = states[g]
        if shrink is not None:
            weighted = weighted + old * shrink
        states[g] = (peak, total, weighted)

    following = scores(tiles[0])
    waiting = None
    for i, tile in enumerate(tiles):
        found = following
        if i + 1 < len(tiles):
            following = scores(tiles[i + 1])
        shares, shrink = soften(tile, found)
        if waiting:
            gather(*waiting)
        waiting = (tile, shares, shrink)
    gather(*waiting)
    for g, (peak, total, weighted) in states.items():
        if last:
            (out_ref,) = refs
            attended = (weighted / total).astype(jnp.bfloat16)
            own_rows = out_ref.shape[2]
            for j in range(out_ref.shape[0]):
                out_ref[j, g * span : (g + 1) * span, :] = attended[
                    :, j * own_rows : (j + 1) * own_rows
                ]
        else:
            peak_out, total_out, sum_out = refs
            peak_out[g] = peak
            total_out[g] = total
            sum_out[g] = weighted


def attend(state, probes, pairs, offset, last=False):
    lanes = 2 * 2 * probes.shape[2]
    span = probes.shape[1] // 2
    keys = sum(p.shape[0] * p.shape[1] // 2 for p in pairs)
    inputs = [probes, *pairs] + list(state or ())
    if last:
        out = jax.ShapeDtypeStruct((4, 2 * span, probes.shape[2]), jnp.bfloat16)
    else:
        stat = jax.ShapeDtypeStruct((2, 1, lanes), jnp.float32)
        out = [stat, stat, jax.ShapeDtypeStruct((2, span, lanes), jnp.float32)]

    def body(*refs):
        attention_body(len(pairs), state is None, last, offset, *refs)

    return kernel_call(body, out, len(inputs), 40 * 2 * lanes * keys * span)(*inputs)


def output_body(latent_ref, mod_ref, weight_ref, *refs):
    out_ref, lhs_ref = refs[-2:]
    parts = refs[:-2]
    head_index = lax.axis_index("tp")
    side = lax.rem(lax.axis_index("sp"), 2)
    rows = parts[0].shape[0]
    for i, ref in enumerate(parts):
        j, flip = i % (len(parts) // 2), i // (len(parts) // 2)
        place = jnp.bitwise_xor(head_index, j) * 2 + jnp.bitwise_xor(side, flip)
        lhs_ref[pl.ds(pl.multiple_of(place * rows, rows), rows), :] = ref[...]
    lhs = lhs_ref[...].T
    columns = mod_ref.shape[2]
    for i in range(mod_ref.shape[0]):
        cut = slice(i * columns, (i + 1) * columns)
        branch = jnp.dot(lhs, weight_ref[:, cut], preferred_element_type=jnp.float32)
        gate = mod_ref[i, 4:5, :]
        out_ref[:, cut] = (latent_ref[:, cut].astype(jnp.float32) + gate * branch).astype(
            jnp.bfloat16
        )


def fast_device(*args):
    return inner_device(*args)


def xor_move(member, axis, mask):
    size = lax.axis_size(axis)
    return lax.ppermute(member, axis, [(i, i ^ mask) for i in range(size)])


def cross_move(member, mask):
    seq_split, head_split = lax.axis_size("sp"), lax.axis_size("tp")
    pairs = [
        (i * head_split + j, (i ^ 1) * head_split + (j ^ mask))
        for i in range(seq_split)
        for j in range(head_split)
    ]
    return lax.ppermute(member, ("sp", "tp"), pairs)


def ring_move(member, step):
    size = lax.axis_size("sp")
    return lax.ppermute(member, "sp", [(i, (i + step) % size) for i in range(size)])


def tables(seq_index, head_index, own_rows, head_split):
    quarter = CHANNEL_SPAN // 4
    blocks = jnp.bitwise_xor(jnp.arange(head_split, dtype=jnp.int32), head_index)
    places = (
        seq_index * own_rows * head_split
        + blocks[:, None] * own_rows
        + jnp.arange(own_rows, dtype=jnp.int32)
    )
    inverse = rope_base ** (-jnp.arange(quarter, dtype=jnp.float32) / quarter)
    grid_row = (places // GRID_W).astype(jnp.float32)[:, None, :] * inverse[:, None]
    grid_col = (places % GRID_W).astype(jnp.float32)[:, None, :] * inverse[:, None]
    row_sine, col_sine = jnp.sin(grid_row), jnp.sin(grid_col)
    row_cosine, col_cosine = jnp.cos(grid_row), jnp.cos(grid_col)
    cosine = jnp.concatenate([row_cosine, row_cosine, col_cosine, col_cosine], axis=1)
    sine = jnp.concatenate([-row_sine, row_sine, -col_sine, col_sine], axis=1)
    return cosine, sine


def inner_device(
    latent,
    context,
    condition,
    context_condition,
    norm_gain,
    shift_weight,
    scale_weight,
    gate_weight,
    query_weight,
    key_weight,
    value_weight,
    query_gain,
    key_gain,
    output_weight,
):
    head_split = lax.axis_size("tp")
    seq_split = lax.axis_size("sp")
    seq_index = lax.axis_index("sp")
    head_index = lax.axis_index("tp")
    own_rows, depth = latent.shape
    ctx_rows = context.shape[0]
    tok_count = own_rows * head_split
    q_heads = query_weight.shape[1] // CHANNEL_SPAN
    kv_heads = key_weight.shape[1] // CHANNEL_SPAN

    part = opening(
        condition.reshape(1, depth),
        context_condition.reshape(1, depth),
        shift_weight,
        scale_weight,
        gate_weight,
    )
    far = xor_move(latent, "tp", 2)
    near = xor_move(latent, "tp", 1)
    mask = seq_split // 2
    while mask:
        other = xor_move(part, "sp", mask)
        part = combine(part, other, 10**11 if 2 * mask == seq_split else 10**6)
        mask //= 2
    both = xor_move(far, "tp", 1)
    modulation = lax.all_gather(part, "tp", axis=0, tiled=False)
    cosine, sine = tables(seq_index, head_index, own_rows, head_split)
    q_tiles = q_heads // kv_heads * head_split // 2
    kv_tiles = head_split
    tile = (own_rows, own_rows)
    keep_q, keep_kv, keep_ctx, give_q, give_kv = pl.pallas_call(
        lambda *refs: projection_body(q_heads, kv_heads, *refs),
        out_shape=[
            jax.ShapeDtypeStruct((*count, *tile), jnp.bfloat16)
            for count in ((q_tiles,), (kv_tiles,), (), (q_tiles,), (kv_tiles + 1,))
        ],
        in_specs=[whole_spec()] * 14,
        out_specs=[whole_spec()] * 5,
        scratch_shapes=[pltpu.VMEM((kv_heads, q_tiles + kv_tiles + 1, *tile), jnp.bfloat16)],
        cost_estimate=pl.CostEstimate(
            flops=4 * tok_count * depth * (q_heads + 2 * kv_heads) * CHANNEL_SPAN,
            transcendentals=0,
            bytes_accessed=0,
        ),
        compiler_params=pltpu.CompilerParams(vmem_limit_bytes=48 * 1024 * 1024),
    )(
        latent,
        context,
        query_weight,
        key_weight,
        value_weight,
        near,
        far,
        both,
        modulation,
        norm_gain.reshape(1, depth),
        query_gain.reshape(1, CHANNEL_SPAN),
        key_gain.reshape(1, CHANNEL_SPAN),
        cosine,
        sine,
    )
    offset = math.log(tok_count / (2.0 * ctx_rows))
    near = xor_move(give_kv, "sp", 1)
    up = ring_move(keep_kv, 2)
    down = ring_move(keep_kv, -2)
    near_q = xor_move(give_q, "sp", 1)
    near = merge(near, keep_ctx)
    near_up = ring_move(near, 2)
    near_down = ring_move(near, -2)
    across = ring_move(up, 2)
    near_across = ring_move(near_up, 2)
    own = attend(None, keep_q, [keep_kv], offset)
    own = attend(own, keep_q, [near], offset)
    other = attend(None, near_q, [keep_kv, near], offset)
    for pieces in ([up, down], [near_up, across], [near_down]):
        other = attend(other, near_q, pieces, offset)
        own = attend(own, keep_q, pieces, offset)
    other = attend(other, near_q, [near_across], offset, True)
    own = attend(own, keep_q, [near_across], offset, True)
    sent = [cross_move(other[j], j) for j in range(head_split)]
    parts = [own[0]] + [xor_move(own[j], "tp", j) for j in range(1, head_split)] + sent
    width = q_heads * CHANNEL_SPAN
    return kernel_call(
        output_body,
        jax.ShapeDtypeStruct(latent.shape, jnp.bfloat16),
        3 + len(parts),
        2 * own_rows * depth * width * head_split,
        [pltpu.VMEM((width * head_split, own_rows), jnp.bfloat16)],
    )(latent, modulation, output_weight, *parts)


def suits(mesh, latent, context, query_weight, key_weight):
    seq_split, head_split = mesh.shape["sp"], mesh.shape["tp"]
    own_rows = latent.shape[0] // (seq_split * head_split)
    ctx_rows = context.shape[0] // seq_split
    kv_heads = key_weight.shape[1] // CHANNEL_SPAN // head_split
    return (
        seq_split == 8
        and head_split == 4
        and own_rows == 2 * CHANNEL_SPAN
        and ctx_rows == CHANNEL_SPAN
        and kv_heads == 2
        and query_weight.shape[1] == 2 * key_weight.shape[1]
    )


def solution(mesh):
    in_specs = (
        P(("sp", "tp"), None),
        P("sp", None),
        P(),
        P(),
        P(),
        P("sp", "tp"),
        P("sp", "tp"),
        P("sp", "tp"),
        P(None, "tp"),
        P(None, "tp"),
        P(None, "tp"),
        P(),
        P(),
        P(),
    )
    out_specs = P(("sp", "tp"), None)

    def program(*args):
        fast = suits(mesh, args[0], args[1], args[8], args[9])
        step = jax.shard_map(
            fast_device if fast else general_device,
            mesh=mesh,
            in_specs=in_specs,
            out_specs=out_specs,
            check_vma=False,
        )
        return step(*args)

    return program
```

```python
import math

import jax
import jax.numpy as jnp
from jax import lax
from jax.experimental import pallas as pl
from jax.experimental.pallas import tpu as pltpu
from jax.sharding import PartitionSpec as P


CHANNEL_SPAN = 64
GRID_W = 64


epsilon = 1e-06
rope_base = 10000.0


def modulate(tok_rows, norm_gain, shift_row, scale_row):
    wide = tok_rows.astype(jnp.float32)
    normed = wide * lax.rsqrt(jnp.mean(wide * wide, axis=-1, keepdims=True) + epsilon)
    return (normed * norm_gain * (1.0 + scale_row) + shift_row).astype(jnp.bfloat16)


def headnorm(raw, gain, heads):
    field = raw.reshape(raw.shape[0], heads, -1)
    return field * lax.rsqrt(jnp.mean(field * field, axis=-1, keepdims=True) + epsilon) * gain


def rotate(field, places):
    count = field.shape[0]
    heads = field.shape[1]
    quarter = field.shape[2] // 4
    grid_row = (places // GRID_W).astype(jnp.float32)
    grid_col = (places % GRID_W).astype(jnp.float32)
    inverse = rope_base ** (-jnp.arange(quarter, dtype=jnp.float32) / quarter)
    angles = jnp.stack([grid_row[:, None] * inverse, grid_col[:, None] * inverse], axis=1)[:, None]
    cosine = jnp.cos(angles)
    sine = jnp.sin(angles)
    matcher_content_couples = field.reshape(count, heads, 2, 2, quarter)
    first = matcher_content_couples[:, :, :, 0]
    second = matcher_content_couples[:, :, :, 1]
    turned = jnp.stack([first * cosine - second * sine, second * cosine + first * sine], axis=3)
    return turned.reshape(count, heads, 4 * quarter)


def process_probe_group(
    accumulator_carry, probe_entries, matcher_content_couples, similarity_offset
):
    row_peak, row_total, weighted = accumulator_carry
    kv_heads = probe_entries.shape[1]
    head_size = probe_entries.shape[3]
    pair_width = kv_heads * head_size
    matcher_pieces = matcher_content_couples[:, :pair_width].reshape(
        matcher_content_couples.shape[0], kv_heads, head_size
    )
    value_rows = matcher_content_couples[:, pair_width:].reshape(
        matcher_content_couples.shape[0], kv_heads, head_size
    )
    similarity_matrix = (
        jnp.einsum(
            "dmvk,hmk->dmvh", probe_entries, matcher_pieces, preferred_element_type=jnp.float32
        )
        * head_size ** (-0.5)
        + similarity_offset
    )
    new_peak = jnp.maximum(row_peak, jnp.max(similarity_matrix, axis=-1))
    shares = jnp.exp(similarity_matrix - new_peak[..., None])
    shrink = jnp.exp(row_peak - new_peak)
    row_total = row_total * shrink + jnp.sum(shares, axis=-1)
    weighted = weighted * shrink[..., None] + jnp.einsum(
        "qkgn,nkd->qkgd",
        shares.astype(jnp.bfloat16),
        value_rows,
        preferred_element_type=jnp.float32,
    )
    return (new_peak, row_total, weighted)


def group_walker(accumulator_carry, probe_entries, matcher_content_couples, similarity_offset):
    pair_count = matcher_content_couples.shape[0]
    probe_group_total = -(-pair_count // 2048)
    while pair_count % probe_group_total:
        probe_group_total += 1
    if probe_group_total == 1:
        return process_probe_group(
            accumulator_carry, probe_entries, matcher_content_couples, similarity_offset
        )
    group_extent = pair_count // probe_group_total

    def scan_step(inner, slices):
        return (process_probe_group(inner, probe_entries, slices[0], slices[1]), None)

    result, _ = lax.scan(
        scan_step,
        accumulator_carry,
        (
            matcher_content_couples.reshape(
                probe_group_total, group_extent, matcher_content_couples.shape[1]
            ),
            similarity_offset.reshape(probe_group_total, group_extent),
        ),
    )
    return result


def general_device(
    latent,
    context,
    condition,
    context_condition,
    norm_gain,
    shift_weight,
    scale_weight,
    gate_weight,
    query_weight,
    key_weight,
    value_weight,
    query_gain,
    key_gain,
    output_weight,
):
    head_split = lax.axis_size("tp")
    seq_index = lax.axis_index("sp")
    head_index = lax.axis_index("tp")
    row_slab = shift_weight.shape[0]
    columns = shift_weight.shape[1]
    conditions = jnp.stack([condition, context_condition])
    activated = jax.nn.silu(
        lax.dynamic_slice_in_dim(conditions, seq_index * row_slab, row_slab, 1)
    ).astype(jnp.bfloat16)
    part_shift = jnp.dot(activated, shift_weight, preferred_element_type=jnp.float32)
    part_scale = jnp.dot(activated, scale_weight, preferred_element_type=jnp.float32)
    part_gate = jnp.dot(activated, gate_weight, preferred_element_type=jnp.float32)

    def widen(member):
        blank = jnp.zeros((2, columns * head_split), jnp.float32)
        return lax.dynamic_update_slice_in_dim(blank, member, head_index * columns, 1)

    shifts, scales, gates = lax.psum(
        (widen(part_shift), widen(part_scale), widen(part_gate)), ("sp", "tp")
    )
    own_rows = latent.shape[0]
    tok_count = own_rows * head_split
    ctx_rows = context.shape[0]
    hidden = modulate(latent, norm_gain, shifts[0], scales[0])
    context_hidden = modulate(context, norm_gain, shifts[1], scales[1])
    q_heads = query_weight.shape[1] // CHANNEL_SPAN
    kv_heads = key_weight.shape[1] // CHANNEL_SPAN
    group_size = q_heads // kv_heads
    q_width = q_heads * CHANNEL_SPAN
    kv_width = kv_heads * CHANNEL_SPAN
    joined_weight = jnp.concatenate([query_weight, key_weight, value_weight], axis=1)
    projected = jnp.dot(
        lax.all_gather(hidden, "tp", axis=0, tiled=True),
        joined_weight,
        preferred_element_type=jnp.float32,
    )
    places = seq_index * tok_count + jnp.arange(tok_count, dtype=jnp.int32)
    probe_entries = rotate(headnorm(projected[:, :q_width], query_gain, q_heads), places).astype(
        jnp.bfloat16
    )
    probe_entries = probe_entries.reshape(tok_count, kv_heads, group_size, CHANNEL_SPAN)
    latent_keys = rotate(
        headnorm(projected[:, q_width : q_width + kv_width], key_gain, kv_heads), places
    ).astype(jnp.bfloat16)
    latent_values = projected[:, q_width + kv_width :].astype(jnp.bfloat16)
    own_pairs = jnp.concatenate([latent_keys.reshape(tok_count, kv_width), latent_values], axis=1)
    ctx_projected = jnp.dot(
        context_hidden, joined_weight[:, q_width:], preferred_element_type=jnp.float32
    )
    ctx_keys = (
        headnorm(ctx_projected[:, :kv_width], key_gain, kv_heads)
        .astype(jnp.bfloat16)
        .reshape(ctx_rows, kv_width)
    )
    ctx_pairs = jnp.concatenate(
        [ctx_keys, ctx_projected[:, kv_width:].astype(jnp.bfloat16)], axis=1
    )
    prefix_mapped = math.log(tok_count / (2.0 * ctx_rows))
    stat_shape = (tok_count, kv_heads, group_size)
    start_state = (
        jnp.full(stat_shape, -jnp.inf, jnp.float32),
        jnp.zeros(stat_shape, jnp.float32),
        jnp.zeros(stat_shape + (CHANNEL_SPAN,), jnp.float32),
    )
    ctx_whole = lax.all_gather(ctx_pairs, "sp", axis=0, tiled=True)
    ctx_state = group_walker(
        start_state,
        probe_entries,
        ctx_whole,
        jnp.full((ctx_whole.shape[0],), prefix_mapped, jnp.float32),
    )
    key_piece = lax.all_gather(own_pairs, "sp", axis=0, tiled=True)
    final_state = group_walker(
        ctx_state, probe_entries, key_piece, jnp.zeros((key_piece.shape[0],), jnp.float32)
    )
    _, row_total, weighted = final_state
    attended = (weighted / row_total[..., None]).astype(jnp.bfloat16).reshape(tok_count, q_width)
    branch = jnp.dot(
        lax.all_to_all(attended, "tp", split_axis=0, concat_axis=1, tiled=True),
        output_weight,
        preferred_element_type=jnp.float32,
    )
    return (latent.astype(jnp.float32) + gates[0] * branch).astype(jnp.bfloat16)


LOG2E = math.log2(math.e)


def whole_spec():
    return pl.BlockSpec(memory_space=pltpu.VMEM)


def kernel_call(body, out_shape, count, flops, scratch=()):
    return pl.pallas_call(
        body,
        out_shape=out_shape,
        in_specs=[whole_spec()] * count,
        out_specs=jax.tree.map(lambda unused: whole_spec(), out_shape),
        scratch_shapes=list(scratch),
        cost_estimate=pl.CostEstimate(flops=flops, transcendentals=0, bytes_accessed=0),
        compiler_params=pltpu.CompilerParams(vmem_limit_bytes=48 * 1024 * 1024),
    )


ROOMY = 60 * 1024 * 1024


def hbm_spec():
    return pl.BlockSpec(memory_space=pltpu.HBM)


def start_loads(pairs, sems):
    copies = []
    for i, (source, target) in enumerate(pairs):
        copies.append(pltpu.make_async_copy(source, target, sems.at[i]))
        copies[-1].start()
    return copies


def opening_body(first_hbm, second_hbm, shift_hbm, scale_hbm, gate_hbm, out_ref, *scratch):
    first, second, *targets, sems = scratch
    row_slab = shift_hbm.shape[0]
    cut = pl.ds(pl.multiple_of(lax.axis_index("sp") * row_slab, row_slab), row_slab)
    copies = start_loads(
        [(first_hbm.at[:, cut], first), (second_hbm.at[:, cut], second)]
        + list(zip((shift_hbm, scale_hbm, gate_hbm), targets)),
        sems,
    )
    copies[0].wait()
    copies[1].wait()
    rows = lax.broadcasted_iota(jnp.int32, (16, row_slab), 0)
    pair = jnp.where(rows == 0, first[...], second[...])
    activated = (pair / (1.0 + jnp.exp(-pair))).astype(jnp.bfloat16)
    out_ref[6:8, :] = jnp.zeros((2, out_ref.shape[1]), jnp.float32)
    for i in range(3):
        copies[2 + i].wait()
        part = jnp.dot(activated, targets[i][...], preferred_element_type=jnp.float32)
        out_ref[2 * i : 2 * i + 2, :] = part[0:2]


def combine_body(one_ref, other_ref, out_ref):
    out_ref[...] = one_ref[...] + other_ref[...]


def combine(one, other, flops):
    return kernel_call(combine_body, jax.ShapeDtypeStruct(one.shape, one.dtype), 2, flops)(
        one, other
    )


def opening(first, second, *weights):
    row_slab, columns = weights[0].shape
    return pl.pallas_call(
        opening_body,
        out_shape=jax.ShapeDtypeStruct((8, columns), jnp.float32),
        in_specs=[hbm_spec()] * 5,
        out_specs=whole_spec(),
        scratch_shapes=[pltpu.VMEM((1, row_slab), jnp.float32)] * 2
        + [pltpu.VMEM((row_slab, columns), jnp.bfloat16)] * 3
        + [pltpu.SemaphoreType.DMA((5,))],
        cost_estimate=pl.CostEstimate(flops=10**8, transcendentals=0, bytes_accessed=0),
        compiler_params=pltpu.CompilerParams(vmem_limit_bytes=ROOMY),
    )(first, second, *weights)


def turn(field, cosine, sine):
    quarter = field.shape[0] // 4
    pieces = [field[i * quarter : (i + 1) * quarter] for i in range(4)]
    swapped = jnp.concatenate([pieces[1], pieces[0], pieces[3], pieces[2]], axis=0)
    return field * cosine + swapped * sine


def projection_body(
    heads,
    kv_heads,
    own_ref,
    context_ref,
    query_ref,
    key_ref,
    value_ref,
    core_ref,
    far_ref,
    both_ref,
    mod_ref,
    gain_ref,
    query_gain_ref,
    key_gain_ref,
    cosine_ref,
    sine_ref,
    keep_q,
    keep_kv,
    keep_ctx,
    give_q,
    give_kv,
    made,
):
    span = CHANNEL_SPAN
    group = heads // kv_heads

    def vector(row):
        return jnp.concatenate([mod_ref[i, row : row + 1, :] for i in range(mod_ref.shape[0])], axis=1)

    gain = gain_ref[...]

    def hidden_of(ref, row):
        wide = ref[...].astype(jnp.float32)
        scaled = wide * lax.rsqrt(jnp.mean(wide * wide, axis=-1, keepdims=True) + epsilon)
        return (scaled * (gain * (1.0 + vector(2 + row))) + vector(row)).astype(jnp.bfloat16)

    def normed(raw, head_gain):
        return raw * lax.rsqrt(jnp.mean(raw * raw, axis=0, keepdims=True) + epsilon) * head_gain

    def upright(ref):
        return jnp.broadcast_to(ref[...], (8, span)).T[:, 0:1]

    query_gain = upright(query_gain_ref)
    key_gain = upright(key_gain_ref)
    blocks = (own_ref, core_ref, far_ref, both_ref)
    q_tiles = group * len(blocks) // 2
    waiting = {}
    for j, ref in enumerate(blocks):
        hidden = hidden_of(ref, 0)
        cosine = cosine_ref[j]
        sine = sine_ref[j]
        rows = slice(j % 2 * span, (j % 2 + 1) * span)
        queries = jnp.dot(hidden, query_ref[...], preferred_element_type=jnp.float32).T
        for h in range(heads):
            turned = turn(normed(queries[h * span : (h + 1) * span], query_gain), cosine, sine)
            kv, g = h // group, h % group
            made[kv, g * len(blocks) // 2 + j // 2, rows, :] = turned.astype(jnp.bfloat16)
        keys = jnp.dot(hidden, key_ref[...], preferred_element_type=jnp.float32).T
        values = jnp.dot(hidden, value_ref[...], preferred_element_type=jnp.float32).T
        for h in range(kv_heads):
            cut = slice(h * span, (h + 1) * span)
            turned = turn(normed(keys[cut], key_gain), cosine, sine)
            if j % 2:
                pair = jnp.concatenate([waiting[h], turned], axis=0)
                made[h, q_tiles + j // 2] = pair.T.astype(jnp.bfloat16)
            waiting[h] = turned
            made[h, q_tiles + len(blocks) // 2 + j // 2, rows, :] = values[cut].astype(jnp.bfloat16)
    hidden = hidden_of(context_ref, 1)
    keys = jnp.dot(hidden, key_ref[...], preferred_element_type=jnp.float32).T
    values = jnp.dot(hidden, value_ref[...], preferred_element_type=jnp.float32).T
    for h in range(kv_heads):
        cut = slice(h * span, (h + 1) * span)
        both = jnp.concatenate([normed(keys[cut], key_gain).T, values[cut]], axis=0)
        made[h, q_tiles + len(blocks)] = jnp.concatenate([both, jnp.zeros_like(both)], axis=1).astype(
            jnp.bfloat16
        )
    side = lax.rem(lax.axis_index("sp"), kv_heads)
    for head, q_ref, kv_ref in ((1 - side, give_q, give_kv), (side, keep_q, keep_kv)):
        for i in range(q_tiles):
            q_ref[i] = made[head, i]
        for i in range(kv_ref.shape[0]):
            kv_ref[i] = made[head, q_tiles + i]
    keep_ctx[...] = made[side, q_tiles + len(blocks)]


def merge_body(near_ref, ctx_ref, out_ref):
    last = near_ref.shape[0] - 1
    span = ctx_ref.shape[1] // 2
    for i in range(last):
        out_ref[i] = near_ref[i]
    out_ref[last] = jnp.concatenate([near_ref[last, :, 0:span], ctx_ref[:, 0:span]], axis=1)


def merge(near, ctx):
    return kernel_call(merge_body, jax.ShapeDtypeStruct(near.shape, near.dtype), 2, 10**6)(near, ctx)


def attention_body(plan, pieces, last, offset, *refs):
    q_refs, refs = refs[: len(plan)], refs[len(plan) :]
    kv_refs, refs = refs[:pieces], refs[pieces:]
    pairs = 2
    groups = 2
    span = q_refs[0].shape[1] // 2
    scale = span ** (-0.5) * LOG2E
    halves = (0, 1)
    states = {}
    queries = {}
    tiles = []
    for i, (q_ref, (started, wanted)) in enumerate(zip(q_refs, plan)):
        if started:
            old, refs = refs[:3], refs[3:]
        for g in range(groups):
            found = jnp.concatenate(
                [
                    q_ref[g * pairs + p, half * span : (half + 1) * span, :]
                    for p in range(pairs)
                    for half in halves
                ],
                axis=1,
            )
            blank = jnp.zeros_like(found)
            queries[i, g, 0] = jnp.concatenate([found, blank], axis=0)
            queries[i, g, 1] = jnp.concatenate([blank, found], axis=0)
            if started:
                states[i, g] = tuple(ref[g] for ref in old)
            tiles += [(i, g, place) for place in wanted]
    tiles.sort(key=lambda tile: tile[2])

    def scores(tile):
        i, g, place = tile
        ref = kv_refs[place]
        context = ref.shape[0] > 2 * pairs
        keys = [ref[p] for p in range(pairs)]
        if context:
            keys.append(ref[2 * pairs, 0:span, :])
        keys = jnp.concatenate(keys, axis=0)
        made = []
        for half in halves:
            found = jnp.dot(keys, queries[i, g, half], preferred_element_type=jnp.float32) * scale
            if context:
                rows = found.shape[0] - span
                made += [found[:rows], found[rows:] + offset * LOG2E]
            else:
                made.append(found)
        return jnp.concatenate(made, axis=0)

    def soften(tile, found):
        place = tile[:2]
        peak = jnp.max(found, axis=0, keepdims=True)
        old = states.get(place)
        if old is not None:
            peak = jnp.maximum(peak, old[0])
        shares = jnp.exp2(found - peak)
        total = jnp.sum(shares, axis=0, keepdims=True)
        shrink = None
        if old is not None:
            shrink = jnp.exp2(old[0] - peak)
            total = total + old[1] * shrink
        states[place] = (peak, total, old[2] if old is not None else None)
        return shares.astype(jnp.bfloat16), shrink

    def gather(tile, shares, shrink):
        ref = kv_refs[tile[2]]
        values = []
        for half in halves:
            rows = slice(half * span, (half + 1) * span)
            values += [ref[pairs + p, rows, :] for p in range(pairs)]
            if ref.shape[0] > 2 * pairs:
                values.append(ref[2 * pairs, span : 2 * span, rows])
        weighted = jnp.dot(
            jnp.concatenate(values, axis=1), shares, preferred_element_type=jnp.float32
        )
        peak, total, old = states[tile[:2]]
        if shrink is not None:
            weighted = weighted + old * shrink
        states[tile[:2]] = (peak, total, weighted)

    following = scores(tiles[0])
    waiting = None
    for i, tile in enumerate(tiles):
        found = following
        if i + 1 < len(tiles):
            following = scores(tiles[i + 1])
        shares, shrink = soften(tile, found)
        if waiting:
            gather(*waiting)
        waiting = (tile, shares, shrink)
    gather(*waiting)
    for (i, g), (peak, total, weighted) in states.items():
        if last:
            out_ref = refs[i]
            attended = (weighted / total).astype(jnp.bfloat16)
            own_rows = out_ref.shape[2]
            for j in range(out_ref.shape[0]):
                out_ref[j, g * span : (g + 1) * span, :] = attended[
                    :, j * own_rows : (j + 1) * own_rows
                ]
        else:
            for ref, value in zip(refs[3 * i : 3 * i + 3], (peak, total, weighted)):
                ref[g] = value


def attend(sources, pieces, offset, last=False):
    probes = [source[0] for source in sources]
    lanes = 2 * 2 * probes[0].shape[2]
    span = probes[0].shape[1] // 2
    plan = [(source[1] is not None, source[2]) for source in sources]
    keys = sum(pieces[i].shape[0] * pieces[i].shape[1] // 2 for source in sources for i in source[2])
    inputs = probes + pieces
    for source in sources:
        inputs += list(source[1] or ())
    if last:
        out = [jax.ShapeDtypeStruct((4, 2 * span, probes[0].shape[2]), jnp.bfloat16)]
    else:
        stat = jax.ShapeDtypeStruct((2, 1, lanes), jnp.float32)
        out = [stat, stat, jax.ShapeDtypeStruct((2, span, lanes), jnp.float32)]

    def body(*refs):
        attention_body(plan, len(pieces), last, offset, *refs)

    found = kernel_call(
        body, out * len(sources), len(inputs), 40 * 2 * lanes * keys * span
    )(*inputs)
    size = len(out)
    return [found[size * i : size * (i + 1)] for i in range(len(sources))]


def output_body(latent_ref, mod_ref, weight_ref, *refs):
    out_ref, lhs_ref = refs[-2:]
    parts = refs[:-2]
    head_index = lax.axis_index("tp")
    side = lax.rem(lax.axis_index("sp"), 2)
    rows = parts[0].shape[0]
    for i, ref in enumerate(parts):
        j, flip = i % (len(parts) // 2), i // (len(parts) // 2)
        place = jnp.bitwise_xor(head_index, j) * 2 + jnp.bitwise_xor(side, flip)
        lhs_ref[pl.ds(pl.multiple_of(place * rows, rows), rows), :] = ref[...]
    lhs = lhs_ref[...].T
    columns = mod_ref.shape[2]
    for i in range(mod_ref.shape[0]):
        cut = slice(i * columns, (i + 1) * columns)
        branch = jnp.dot(lhs, weight_ref[:, cut], preferred_element_type=jnp.float32)
        gate = mod_ref[i, 4:5, :]
        out_ref[:, cut] = (latent_ref[:, cut].astype(jnp.float32) + gate * branch).astype(
            jnp.bfloat16
        )


def fast_device(*args):
    return inner_device(*args)


def xor_move(member, axis, mask):
    size = lax.axis_size(axis)
    return lax.ppermute(member, axis, [(i, i ^ mask) for i in range(size)])


def cross_move(member, mask):
    seq_split, head_split = lax.axis_size("sp"), lax.axis_size("tp")
    pairs = [
        (i * head_split + j, (i ^ 1) * head_split + (j ^ mask))
        for i in range(seq_split)
        for j in range(head_split)
    ]
    return lax.ppermute(member, ("sp", "tp"), pairs)


def tables(seq_index, head_index, own_rows, head_split):
    quarter = CHANNEL_SPAN // 4
    blocks = jnp.bitwise_xor(jnp.arange(head_split, dtype=jnp.int32), head_index)
    places = (
        seq_index * own_rows * head_split
        + blocks[:, None] * own_rows
        + jnp.arange(own_rows, dtype=jnp.int32)
    )
    inverse = rope_base ** (-jnp.arange(quarter, dtype=jnp.float32) / quarter)
    grid_row = (places // GRID_W).astype(jnp.float32)[:, None, :] * inverse[:, None]
    grid_col = (places % GRID_W).astype(jnp.float32)[:, None, :] * inverse[:, None]
    row_sine, col_sine = jnp.sin(grid_row), jnp.sin(grid_col)
    row_cosine, col_cosine = jnp.cos(grid_row), jnp.cos(grid_col)
    cosine = jnp.concatenate([row_cosine, row_cosine, col_cosine, col_cosine], axis=1)
    sine = jnp.concatenate([-row_sine, row_sine, -col_sine, col_sine], axis=1)
    return cosine, sine


def inner_device(
    latent,
    context,
    condition,
    context_condition,
    norm_gain,
    shift_weight,
    scale_weight,
    gate_weight,
    query_weight,
    key_weight,
    value_weight,
    query_gain,
    key_gain,
    output_weight,
):
    head_split = lax.axis_size("tp")
    seq_split = lax.axis_size("sp")
    seq_index = lax.axis_index("sp")
    head_index = lax.axis_index("tp")
    own_rows, depth = latent.shape
    ctx_rows = context.shape[0]
    tok_count = own_rows * head_split
    q_heads = query_weight.shape[1] // CHANNEL_SPAN
    kv_heads = key_weight.shape[1] // CHANNEL_SPAN

    part = opening(
        condition.reshape(1, depth),
        context_condition.reshape(1, depth),
        shift_weight,
        scale_weight,
        gate_weight,
    )
    far = xor_move(latent, "tp", 2)
    near = xor_move(latent, "tp", 1)
    mask = seq_split // 2
    while mask:
        other = xor_move(part, "sp", mask)
        part = combine(part, other, 10**11 if 2 * mask == seq_split else 10**6)
        mask //= 2
    both = xor_move(far, "tp", 1)
    modulation = lax.all_gather(part, "tp", axis=0, tiled=False)
    cosine, sine = tables(seq_index, head_index, own_rows, head_split)
    q_tiles = q_heads // kv_heads * head_split // 2
    kv_tiles = head_split
    tile = (own_rows, own_rows)
    keep_q, keep_kv, keep_ctx, give_q, give_kv = pl.pallas_call(
        lambda *refs: projection_body(q_heads, kv_heads, *refs),
        out_shape=[
            jax.ShapeDtypeStruct((*count, *tile), jnp.bfloat16)
            for count in ((q_tiles,), (kv_tiles,), (), (q_tiles,), (kv_tiles + 1,))
        ],
        in_specs=[whole_spec()] * 14,
        out_specs=[whole_spec()] * 5,
        scratch_shapes=[pltpu.VMEM((kv_heads, q_tiles + kv_tiles + 1, *tile), jnp.bfloat16)],
        cost_estimate=pl.CostEstimate(
            flops=4 * tok_count * depth * (q_heads + 2 * kv_heads) * CHANNEL_SPAN,
            transcendentals=0,
            bytes_accessed=0,
        ),
        compiler_params=pltpu.CompilerParams(vmem_limit_bytes=48 * 1024 * 1024),
    )(
        latent,
        context,
        query_weight,
        key_weight,
        value_weight,
        near,
        far,
        both,
        modulation,
        norm_gain.reshape(1, depth),
        query_gain.reshape(1, CHANNEL_SPAN),
        key_gain.reshape(1, CHANNEL_SPAN),
        cosine,
        sine,
    )
    offset = math.log(tok_count / (2.0 * ctx_rows))
    near = xor_move(give_kv, "sp", 1)
    up = xor_move(keep_kv, "sp", 2)
    down = xor_move(keep_kv, "sp", 6)
    near_q = xor_move(give_q, "sp", 1)
    near = merge(near, keep_ctx)
    near_down = xor_move(near, "sp", 6)
    near_up = xor_move(near, "sp", 2)
    across = xor_move(down, "sp", 2)
    near_across = xor_move(near_down, "sp", 2)
    (own,) = attend([(keep_q, None, [0])], [keep_kv], offset)
    own, other = attend([(keep_q, own, [1]), (near_q, None, [0, 1])], [keep_kv, near], offset)
    for piece in (up, down, near_up, across, near_down):
        own, other = attend([(keep_q, own, [0]), (near_q, other, [0])], [piece], offset)
    (own,), (other,) = attend(
        [(keep_q, own, [0]), (near_q, other, [0])], [near_across], offset, True
    )
    sent = [cross_move(other[j], j) for j in range(head_split)]
    parts = [own[0]] + [xor_move(own[j], "tp", j) for j in range(1, head_split)] + sent
    width = q_heads * CHANNEL_SPAN
    return kernel_call(
        output_body,
        jax.ShapeDtypeStruct(latent.shape, jnp.bfloat16),
        3 + len(parts),
        2 * own_rows * depth * width * head_split,
        [pltpu.VMEM((width * head_split, own_rows), jnp.bfloat16)],
    )(latent, modulation, output_weight, *parts)


def suits(mesh, latent, context, query_weight, key_weight):
    seq_split, head_split = mesh.shape["sp"], mesh.shape["tp"]
    own_rows = latent.shape[0] // (seq_split * head_split)
    ctx_rows = context.shape[0] // seq_split
    kv_heads = key_weight.shape[1] // CHANNEL_SPAN // head_split
    return (
        seq_split == 8
        and head_split == 4
        and own_rows == 2 * CHANNEL_SPAN
        and ctx_rows == CHANNEL_SPAN
        and kv_heads == 2
        and query_weight.shape[1] == 2 * key_weight.shape[1]
    )


def solution(mesh):
    in_specs = (
        P(("sp", "tp"), None),
        P("sp", None),
        P(),
        P(),
        P(),
        P("sp", "tp"),
        P("sp", "tp"),
        P("sp", "tp"),
        P(None, "tp"),
        P(None, "tp"),
        P(None, "tp"),
        P(),
        P(),
        P(),
    )
    out_specs = P(("sp", "tp"), None)

    def program(*args):
        fast = suits(mesh, args[0], args[1], args[8], args[9])
        step = jax.shard_map(
            fast_device if fast else general_device,
            mesh=mesh,
            in_specs=in_specs,
            out_specs=out_specs,
            check_vma=False,
        )
        return step(*args)

    return program
```

```python
import math

import jax
import jax.numpy as jnp
from jax import lax
from jax.experimental import pallas as pl
from jax.experimental.pallas import tpu as pltpu
from jax.sharding import PartitionSpec as P


CHANNEL_SPAN = 64
GRID_W = 64


epsilon = 1e-06
rope_base = 10000.0


def modulate(tok_rows, norm_gain, shift_row, scale_row):
    wide = tok_rows.astype(jnp.float32)
    normed = wide * lax.rsqrt(jnp.mean(wide * wide, axis=-1, keepdims=True) + epsilon)
    return (normed * norm_gain * (1.0 + scale_row) + shift_row).astype(jnp.bfloat16)


def headnorm(raw, gain, heads):
    field = raw.reshape(raw.shape[0], heads, -1)
    return field * lax.rsqrt(jnp.mean(field * field, axis=-1, keepdims=True) + epsilon) * gain


def rotate(field, places):
    count = field.shape[0]
    heads = field.shape[1]
    quarter = field.shape[2] // 4
    grid_row = (places // GRID_W).astype(jnp.float32)
    grid_col = (places % GRID_W).astype(jnp.float32)
    inverse = rope_base ** (-jnp.arange(quarter, dtype=jnp.float32) / quarter)
    angles = jnp.stack([grid_row[:, None] * inverse, grid_col[:, None] * inverse], axis=1)[:, None]
    cosine = jnp.cos(angles)
    sine = jnp.sin(angles)
    matcher_content_couples = field.reshape(count, heads, 2, 2, quarter)
    first = matcher_content_couples[:, :, :, 0]
    second = matcher_content_couples[:, :, :, 1]
    turned = jnp.stack([first * cosine - second * sine, second * cosine + first * sine], axis=3)
    return turned.reshape(count, heads, 4 * quarter)


def process_probe_group(
    accumulator_carry, probe_entries, matcher_content_couples, similarity_offset
):
    row_peak, row_total, weighted = accumulator_carry
    kv_heads = probe_entries.shape[1]
    head_size = probe_entries.shape[3]
    pair_width = kv_heads * head_size
    matcher_pieces = matcher_content_couples[:, :pair_width].reshape(
        matcher_content_couples.shape[0], kv_heads, head_size
    )
    value_rows = matcher_content_couples[:, pair_width:].reshape(
        matcher_content_couples.shape[0], kv_heads, head_size
    )
    similarity_matrix = (
        jnp.einsum(
            "dmvk,hmk->dmvh", probe_entries, matcher_pieces, preferred_element_type=jnp.float32
        )
        * head_size ** (-0.5)
        + similarity_offset
    )
    new_peak = jnp.maximum(row_peak, jnp.max(similarity_matrix, axis=-1))
    shares = jnp.exp(similarity_matrix - new_peak[..., None])
    shrink = jnp.exp(row_peak - new_peak)
    row_total = row_total * shrink + jnp.sum(shares, axis=-1)
    weighted = weighted * shrink[..., None] + jnp.einsum(
        "qkgn,nkd->qkgd",
        shares.astype(jnp.bfloat16),
        value_rows,
        preferred_element_type=jnp.float32,
    )
    return (new_peak, row_total, weighted)


def group_walker(accumulator_carry, probe_entries, matcher_content_couples, similarity_offset):
    pair_count = matcher_content_couples.shape[0]
    probe_group_total = -(-pair_count // 2048)
    while pair_count % probe_group_total:
        probe_group_total += 1
    if probe_group_total == 1:
        return process_probe_group(
            accumulator_carry, probe_entries, matcher_content_couples, similarity_offset
        )
    group_extent = pair_count // probe_group_total

    def scan_step(inner, slices):
        return (process_probe_group(inner, probe_entries, slices[0], slices[1]), None)

    result, _ = lax.scan(
        scan_step,
        accumulator_carry,
        (
            matcher_content_couples.reshape(
                probe_group_total, group_extent, matcher_content_couples.shape[1]
            ),
            similarity_offset.reshape(probe_group_total, group_extent),
        ),
    )
    return result


def general_device(
    latent,
    context,
    condition,
    context_condition,
    norm_gain,
    shift_weight,
    scale_weight,
    gate_weight,
    query_weight,
    key_weight,
    value_weight,
    query_gain,
    key_gain,
    output_weight,
):
    head_split = lax.axis_size("tp")
    seq_index = lax.axis_index("sp")
    head_index = lax.axis_index("tp")
    row_slab = shift_weight.shape[0]
    columns = shift_weight.shape[1]
    conditions = jnp.stack([condition, context_condition])
    activated = jax.nn.silu(
        lax.dynamic_slice_in_dim(conditions, seq_index * row_slab, row_slab, 1)
    ).astype(jnp.bfloat16)
    part_shift = jnp.dot(activated, shift_weight, preferred_element_type=jnp.float32)
    part_scale = jnp.dot(activated, scale_weight, preferred_element_type=jnp.float32)
    part_gate = jnp.dot(activated, gate_weight, preferred_element_type=jnp.float32)

    def widen(member):
        blank = jnp.zeros((2, columns * head_split), jnp.float32)
        return lax.dynamic_update_slice_in_dim(blank, member, head_index * columns, 1)

    shifts, scales, gates = lax.psum(
        (widen(part_shift), widen(part_scale), widen(part_gate)), ("sp", "tp")
    )
    own_rows = latent.shape[0]
    tok_count = own_rows * head_split
    ctx_rows = context.shape[0]
    hidden = modulate(latent, norm_gain, shifts[0], scales[0])
    context_hidden = modulate(context, norm_gain, shifts[1], scales[1])
    q_heads = query_weight.shape[1] // CHANNEL_SPAN
    kv_heads = key_weight.shape[1] // CHANNEL_SPAN
    group_size = q_heads // kv_heads
    q_width = q_heads * CHANNEL_SPAN
    kv_width = kv_heads * CHANNEL_SPAN
    joined_weight = jnp.concatenate([query_weight, key_weight, value_weight], axis=1)
    projected = jnp.dot(
        lax.all_gather(hidden, "tp", axis=0, tiled=True),
        joined_weight,
        preferred_element_type=jnp.float32,
    )
    places = seq_index * tok_count + jnp.arange(tok_count, dtype=jnp.int32)
    probe_entries = rotate(headnorm(projected[:, :q_width], query_gain, q_heads), places).astype(
        jnp.bfloat16
    )
    probe_entries = probe_entries.reshape(tok_count, kv_heads, group_size, CHANNEL_SPAN)
    latent_keys = rotate(
        headnorm(projected[:, q_width : q_width + kv_width], key_gain, kv_heads), places
    ).astype(jnp.bfloat16)
    latent_values = projected[:, q_width + kv_width :].astype(jnp.bfloat16)
    own_pairs = jnp.concatenate([latent_keys.reshape(tok_count, kv_width), latent_values], axis=1)
    ctx_projected = jnp.dot(
        context_hidden, joined_weight[:, q_width:], preferred_element_type=jnp.float32
    )
    ctx_keys = (
        headnorm(ctx_projected[:, :kv_width], key_gain, kv_heads)
        .astype(jnp.bfloat16)
        .reshape(ctx_rows, kv_width)
    )
    ctx_pairs = jnp.concatenate(
        [ctx_keys, ctx_projected[:, kv_width:].astype(jnp.bfloat16)], axis=1
    )
    prefix_mapped = math.log(tok_count / (2.0 * ctx_rows))
    stat_shape = (tok_count, kv_heads, group_size)
    start_state = (
        jnp.full(stat_shape, -jnp.inf, jnp.float32),
        jnp.zeros(stat_shape, jnp.float32),
        jnp.zeros(stat_shape + (CHANNEL_SPAN,), jnp.float32),
    )
    ctx_whole = lax.all_gather(ctx_pairs, "sp", axis=0, tiled=True)
    ctx_state = group_walker(
        start_state,
        probe_entries,
        ctx_whole,
        jnp.full((ctx_whole.shape[0],), prefix_mapped, jnp.float32),
    )
    key_piece = lax.all_gather(own_pairs, "sp", axis=0, tiled=True)
    final_state = group_walker(
        ctx_state, probe_entries, key_piece, jnp.zeros((key_piece.shape[0],), jnp.float32)
    )
    _, row_total, weighted = final_state
    attended = (weighted / row_total[..., None]).astype(jnp.bfloat16).reshape(tok_count, q_width)
    branch = jnp.dot(
        lax.all_to_all(attended, "tp", split_axis=0, concat_axis=1, tiled=True),
        output_weight,
        preferred_element_type=jnp.float32,
    )
    return (latent.astype(jnp.float32) + gates[0] * branch).astype(jnp.bfloat16)


LOG2E = math.log2(math.e)


def whole_spec():
    return pl.BlockSpec(memory_space=pltpu.VMEM)


def kernel_call(body, out_shape, count, flops, scratch=()):
    return pl.pallas_call(
        body,
        out_shape=out_shape,
        in_specs=[whole_spec()] * count,
        out_specs=jax.tree.map(lambda unused: whole_spec(), out_shape),
        scratch_shapes=list(scratch),
        cost_estimate=pl.CostEstimate(flops=flops, transcendentals=0, bytes_accessed=0),
        compiler_params=pltpu.CompilerParams(vmem_limit_bytes=MODEST),
    )


ROOMY = 60 * 1024 * 1024
MODEST = 32 * 1024 * 1024


def hbm_spec():
    return pl.BlockSpec(memory_space=pltpu.HBM)


def start_loads(pairs, sems):
    copies = []
    for i, (source, target) in enumerate(pairs):
        copies.append(pltpu.make_async_copy(source, target, sems.at[i]))
        copies[-1].start()
    return copies


def opening_body(first_hbm, second_hbm, shift_hbm, scale_hbm, gate_hbm, out_ref, *scratch):
    first, second, *targets, sems = scratch
    row_slab = shift_hbm.shape[0]
    cut = pl.ds(pl.multiple_of(lax.axis_index("sp") * row_slab, row_slab), row_slab)
    copies = start_loads(
        [(first_hbm.at[:, cut], first), (second_hbm.at[:, cut], second)]
        + list(zip((shift_hbm, scale_hbm, gate_hbm), targets)),
        sems,
    )
    copies[0].wait()
    copies[1].wait()
    rows = lax.broadcasted_iota(jnp.int32, (16, row_slab), 0)
    pair = jnp.where(rows == 0, first[...], second[...])
    activated = (pair / (1.0 + jnp.exp(-pair))).astype(jnp.bfloat16)
    out_ref[6:8, :] = jnp.zeros((2, out_ref.shape[1]), jnp.float32)
    for i in range(3):
        copies[2 + i].wait()
        part = jnp.dot(activated, targets[i][...], preferred_element_type=jnp.float32)
        out_ref[2 * i : 2 * i + 2, :] = part[0:2]


def combine_body(one_ref, other_ref, out_ref):
    out_ref[...] = one_ref[...] + other_ref[...]


def combine(one, other, flops):
    return kernel_call(combine_body, jax.ShapeDtypeStruct(one.shape, one.dtype), 2, flops)(
        one, other
    )


def opening(first, second, *weights):
    row_slab, columns = weights[0].shape
    return pl.pallas_call(
        opening_body,
        out_shape=jax.ShapeDtypeStruct((8, columns), jnp.float32),
        in_specs=[hbm_spec()] * 5,
        out_specs=whole_spec(),
        scratch_shapes=[pltpu.VMEM((1, row_slab), jnp.float32)] * 2
        + [pltpu.VMEM((row_slab, columns), jnp.bfloat16)] * 3
        + [pltpu.SemaphoreType.DMA((5,))],
        cost_estimate=pl.CostEstimate(flops=10**8, transcendentals=0, bytes_accessed=0),
        compiler_params=pltpu.CompilerParams(vmem_limit_bytes=ROOMY),
    )(first, second, *weights)


def turn(field, cosine, sine):
    quarter = field.shape[0] // 4
    pieces = [field[i * quarter : (i + 1) * quarter] for i in range(4)]
    swapped = jnp.concatenate([pieces[1], pieces[0], pieces[3], pieces[2]], axis=0)
    return field * cosine + swapped * sine


def projection_body(
    heads,
    kv_heads,
    own_ref,
    context_ref,
    query_ref,
    key_ref,
    value_ref,
    core_ref,
    far_ref,
    both_ref,
    mod_ref,
    gain_ref,
    query_gain_ref,
    key_gain_ref,
    cosine_ref,
    sine_ref,
    keep_q,
    keep_kv,
    keep_ctx,
    give_q,
    give_kv,
    made,
):
    span = CHANNEL_SPAN
    group = heads // kv_heads

    def vector(row):
        return jnp.concatenate([mod_ref[i, row : row + 1, :] for i in range(mod_ref.shape[0])], axis=1)

    gain = gain_ref[...]

    def hidden_of(ref, row):
        wide = ref[...].astype(jnp.float32)
        scaled = wide * lax.rsqrt(jnp.mean(wide * wide, axis=-1, keepdims=True) + epsilon)
        return (scaled * (gain * (1.0 + vector(2 + row))) + vector(row)).astype(jnp.bfloat16)

    def normed(raw, head_gain):
        return raw * lax.rsqrt(jnp.mean(raw * raw, axis=0, keepdims=True) + epsilon) * head_gain

    def upright(ref):
        return jnp.broadcast_to(ref[...], (8, span)).T[:, 0:1]

    query_gain = upright(query_gain_ref)
    key_gain = upright(key_gain_ref)
    blocks = (own_ref, core_ref, far_ref, both_ref)
    q_tiles = group * len(blocks) // 2
    waiting = {}
    for j, ref in enumerate(blocks):
        hidden = hidden_of(ref, 0)
        cosine = cosine_ref[j]
        sine = sine_ref[j]
        rows = slice(j % 2 * span, (j % 2 + 1) * span)
        queries = jnp.dot(hidden, query_ref[...], preferred_element_type=jnp.float32).T
        for h in range(heads):
            turned = turn(normed(queries[h * span : (h + 1) * span], query_gain), cosine, sine)
            kv, g = h // group, h % group
            made[kv, g * len(blocks) // 2 + j // 2, rows, :] = turned.astype(jnp.bfloat16)
        keys = jnp.dot(hidden, key_ref[...], preferred_element_type=jnp.float32).T
        values = jnp.dot(hidden, value_ref[...], preferred_element_type=jnp.float32).T
        for h in range(kv_heads):
            cut = slice(h * span, (h + 1) * span)
            turned = turn(normed(keys[cut], key_gain), cosine, sine)
            if j % 2:
                pair = jnp.concatenate([waiting[h], turned], axis=0)
                made[h, q_tiles + j // 2] = pair.T.astype(jnp.bfloat16)
            waiting[h] = turned
            made[h, q_tiles + len(blocks) // 2 + j // 2, rows, :] = values[cut].astype(jnp.bfloat16)
    hidden = hidden_of(context_ref, 1)
    keys = jnp.dot(hidden, key_ref[...], preferred_element_type=jnp.float32).T
    values = jnp.dot(hidden, value_ref[...], preferred_element_type=jnp.float32).T
    for h in range(kv_heads):
        cut = slice(h * span, (h + 1) * span)
        both = jnp.concatenate([normed(keys[cut], key_gain).T, values[cut]], axis=0)
        made[h, q_tiles + len(blocks)] = jnp.concatenate([both, jnp.zeros_like(both)], axis=1).astype(
            jnp.bfloat16
        )
    side = lax.rem(lax.axis_index("sp"), kv_heads)
    for head, q_ref, kv_ref in ((1 - side, give_q, give_kv), (side, keep_q, keep_kv)):
        for i in range(q_tiles):
            if q_ref is keep_q:
                q_ref[i], q_ref[q_tiles + i] = scaled_halves(made[head, i])
            else:
                q_ref[i] = made[head, i]
        for i in range(kv_ref.shape[0]):
            kv_ref[i] = made[head, q_tiles + i]
    keep_ctx[...] = made[side, q_tiles + len(blocks)]


def merge_body(near_ref, ctx_ref, out_ref):
    last = near_ref.shape[0] - 1
    span = ctx_ref.shape[1] // 2
    for i in range(last):
        out_ref[i] = near_ref[i]
    out_ref[last] = jnp.concatenate([near_ref[last, :, 0:span], ctx_ref[:, 0:span]], axis=1)


def merge(near, ctx):
    return kernel_call(merge_body, jax.ShapeDtypeStruct(near.shape, near.dtype), 2, 10**6)(near, ctx)


def scaled_halves(tile):
    scale = (tile.shape[-2] // 2) ** (-0.5) * LOG2E
    wide = tile.astype(jnp.float32) * scale
    high = wide.astype(jnp.bfloat16)
    return high, (wide - high.astype(jnp.float32)).astype(jnp.bfloat16)


def ready_body(q_ref, out_ref):
    count = q_ref.shape[0]
    for i in range(count):
        out_ref[i], out_ref[count + i] = scaled_halves(q_ref[i])


def ready(probes):
    shape = jax.ShapeDtypeStruct((2 * probes.shape[0], *probes.shape[1:]), probes.dtype)
    return kernel_call(ready_body, shape, 1, 10**6)(probes)


def attention_body(plan, pieces, last, offset, *refs):
    q_refs, refs = refs[: len(plan)], refs[len(plan) :]
    kv_refs, refs = refs[:pieces], refs[pieces:]
    pairs = 2
    groups = 2
    span = q_refs[0].shape[1] // 2
    halves = (0, 1)
    states = {}
    queries = {}
    tiles = []
    for i, (q_ref, (started, wanted)) in enumerate(zip(q_refs, plan)):
        if started:
            old, refs = refs[:3], refs[3:]
        for g in range(groups):
            high, low = [
                jnp.concatenate(
                    [
                        q_ref[(level * groups + g) * pairs + p, half * span : (half + 1) * span, :]
                        for p in range(pairs)
                        for half in halves
                    ],
                    axis=1,
                )
                for level in halves
            ]
            blank = jnp.zeros_like(high)
            queries[i, g, 0] = jnp.concatenate([high, blank, low, blank], axis=0)
            queries[i, g, 1] = jnp.concatenate([blank, high, blank, low], axis=0)
            if started:
                states[i, g] = tuple(ref[g] for ref in old)
            tiles += [(i, g, place) for place in wanted]
    tiles.sort(key=lambda tile: tile[2])

    def scores(tile):
        i, g, place = tile
        ref = kv_refs[place]
        context = ref.shape[0] > 2 * pairs
        keys = [ref[p] for p in range(pairs)]
        if context:
            keys.append(ref[2 * pairs, 0:span, :])
        keys = jnp.concatenate(keys, axis=0)
        keys = jnp.concatenate([keys, keys], axis=1)
        made = []
        for half in halves:
            found = jnp.dot(keys, queries[i, g, half], preferred_element_type=jnp.float32)
            if context:
                rows = found.shape[0] - span
                made += [found[:rows], found[rows:] + offset * LOG2E]
            else:
                made.append(found)
        return jnp.concatenate(made, axis=0)

    def soften(tile, found):
        place = tile[:2]
        peak = jnp.max(found, axis=0, keepdims=True)
        old = states.get(place)
        if old is not None:
            peak = jnp.maximum(peak, old[0])
        shares = jnp.exp2(found - peak)
        total = jnp.sum(shares, axis=0, keepdims=True)
        shrink = None
        if old is not None:
            shrink = jnp.exp2(old[0] - peak)
            total = total + old[1] * shrink
        states[place] = (peak, total, old[2] if old is not None else None)
        return shares.astype(jnp.bfloat16), shrink

    def gather(tile, shares, shrink):
        ref = kv_refs[tile[2]]
        values = []
        for half in halves:
            rows = slice(half * span, (half + 1) * span)
            values += [ref[pairs + p, rows, :] for p in range(pairs)]
            if ref.shape[0] > 2 * pairs:
                values.append(ref[2 * pairs, span : 2 * span, rows])
        weighted = jnp.dot(
            jnp.concatenate(values, axis=1), shares, preferred_element_type=jnp.float32
        )
        peak, total, old = states[tile[:2]]
        if shrink is not None:
            weighted = weighted + old * shrink
        states[tile[:2]] = (peak, total, weighted)

    following = scores(tiles[0])
    waiting = None
    for i, tile in enumerate(tiles):
        found = following
        if i + 1 < len(tiles):
            following = scores(tiles[i + 1])
        shares, shrink = soften(tile, found)
        if waiting:
            gather(*waiting)
        waiting = (tile, shares, shrink)
    gather(*waiting)
    for (i, g), (peak, total, weighted) in states.items():
        if last:
            out_ref = refs[i]
            attended = (weighted / total).astype(jnp.bfloat16)
            own_rows = out_ref.shape[2]
            for j in range(out_ref.shape[0]):
                out_ref[j, g * span : (g + 1) * span, :] = attended[
                    :, j * own_rows : (j + 1) * own_rows
                ]
        else:
            for ref, value in zip(refs[3 * i : 3 * i + 3], (peak, total, weighted)):
                ref[g] = value


def attend(sources, pieces, offset, last=False):
    probes = [source[0] for source in sources]
    lanes = 2 * 2 * probes[0].shape[2]
    span = probes[0].shape[1] // 2
    plan = [(source[1] is not None, source[2]) for source in sources]
    keys = sum(pieces[i].shape[0] * pieces[i].shape[1] // 2 for source in sources for i in source[2])
    inputs = probes + pieces
    for source in sources:
        inputs += list(source[1] or ())
    if last:
        out = [jax.ShapeDtypeStruct((4, 2 * span, probes[0].shape[2]), jnp.bfloat16)]
    else:
        stat = jax.ShapeDtypeStruct((2, 1, lanes), jnp.float32)
        out = [stat, stat, jax.ShapeDtypeStruct((2, span, lanes), jnp.float32)]

    def body(*refs):
        attention_body(plan, len(pieces), last, offset, *refs)

    found = kernel_call(
        body, out * len(sources), len(inputs), 40 * 2 * lanes * keys * span
    )(*inputs)
    size = len(out)
    return [found[size * i : size * (i + 1)] for i in range(len(sources))]


def output_body(latent_ref, mod_ref, weight_ref, *refs):
    out_ref, lhs_ref = refs[-2:]
    parts = refs[:-2]
    head_index = lax.axis_index("tp")
    side = lax.rem(lax.axis_index("sp"), 2)
    rows = parts[0].shape[0]
    for i, ref in enumerate(parts):
        j, flip = i % (len(parts) // 2), i // (len(parts) // 2)
        place = jnp.bitwise_xor(head_index, j) * 2 + jnp.bitwise_xor(side, flip)
        lhs_ref[pl.ds(pl.multiple_of(place * rows, rows), rows), :] = ref[...]
    lhs = lhs_ref[...].T
    columns = mod_ref.shape[2]
    for i in range(mod_ref.shape[0]):
        cut = slice(i * columns, (i + 1) * columns)
        branch = jnp.dot(lhs, weight_ref[:, cut], preferred_element_type=jnp.float32)
        gate = mod_ref[i, 4:5, :]
        out_ref[:, cut] = (latent_ref[:, cut].astype(jnp.float32) + gate * branch).astype(
            jnp.bfloat16
        )


def fast_device(*args):
    return inner_device(*args)


def xor_move(member, axis, mask):
    size = lax.axis_size(axis)
    return lax.ppermute(member, axis, [(i, i ^ mask) for i in range(size)])


def cross_move(member, mask):
    seq_split, head_split = lax.axis_size("sp"), lax.axis_size("tp")
    pairs = [
        (i * head_split + j, (i ^ 1) * head_split + (j ^ mask))
        for i in range(seq_split)
        for j in range(head_split)
    ]
    return lax.ppermute(member, ("sp", "tp"), pairs)


def tables(seq_index, head_index, own_rows, head_split):
    quarter = CHANNEL_SPAN // 4
    blocks = jnp.bitwise_xor(jnp.arange(head_split, dtype=jnp.int32), head_index)
    places = (
        seq_index * own_rows * head_split
        + blocks[:, None] * own_rows
        + jnp.arange(own_rows, dtype=jnp.int32)
    )
    inverse = rope_base ** (-jnp.arange(quarter, dtype=jnp.float32) / quarter)
    grid_row = (places // GRID_W).astype(jnp.float32)[:, None, :] * inverse[:, None]
    grid_col = (places % GRID_W).astype(jnp.float32)[:, None, :] * inverse[:, None]
    row_sine, col_sine = jnp.sin(grid_row), jnp.sin(grid_col)
    row_cosine, col_cosine = jnp.cos(grid_row), jnp.cos(grid_col)
    cosine = jnp.concatenate([row_cosine, row_cosine, col_cosine, col_cosine], axis=1)
    sine = jnp.concatenate([-row_sine, row_sine, -col_sine, col_sine], axis=1)
    return cosine, sine


def inner_device(
    latent,
    context,
    condition,
    context_condition,
    norm_gain,
    shift_weight,
    scale_weight,
    gate_weight,
    query_weight,
    key_weight,
    value_weight,
    query_gain,
    key_gain,
    output_weight,
):
    head_split = lax.axis_size("tp")
    seq_split = lax.axis_size("sp")
    seq_index = lax.axis_index("sp")
    head_index = lax.axis_index("tp")
    own_rows, depth = latent.shape
    ctx_rows = context.shape[0]
    tok_count = own_rows * head_split
    q_heads = query_weight.shape[1] // CHANNEL_SPAN
    kv_heads = key_weight.shape[1] // CHANNEL_SPAN

    part = opening(
        condition.reshape(1, depth),
        context_condition.reshape(1, depth),
        shift_weight,
        scale_weight,
        gate_weight,
    )
    far = xor_move(latent, "tp", 2)
    near = xor_move(latent, "tp", 1)
    mask = seq_split // 2
    while mask:
        other = xor_move(part, "sp", mask)
        part = combine(part, other, 10**11 if 2 * mask == seq_split else 10**6)
        mask //= 2
    both = xor_move(far, "tp", 1)
    modulation = lax.all_gather(part, "tp", axis=0, tiled=False)
    cosine, sine = tables(seq_index, head_index, own_rows, head_split)
    q_tiles = q_heads // kv_heads * head_split // 2
    kv_tiles = head_split
    tile = (own_rows, own_rows)
    keep_q, keep_kv, keep_ctx, give_q, give_kv = pl.pallas_call(
        lambda *refs: projection_body(q_heads, kv_heads, *refs),
        out_shape=[
            jax.ShapeDtypeStruct((*count, *tile), jnp.bfloat16)
            for count in ((2 * q_tiles,), (kv_tiles,), (), (q_tiles,), (kv_tiles + 1,))
        ],
        in_specs=[whole_spec()] * 14,
        out_specs=[whole_spec()] * 5,
        scratch_shapes=[pltpu.VMEM((kv_heads, q_tiles + kv_tiles + 1, *tile), jnp.bfloat16)],
        cost_estimate=pl.CostEstimate(
            flops=4 * tok_count * depth * (q_heads + 2 * kv_heads) * CHANNEL_SPAN,
            transcendentals=0,
            bytes_accessed=0,
        ),
        compiler_params=pltpu.CompilerParams(vmem_limit_bytes=MODEST),
    )(
        latent,
        context,
        query_weight,
        key_weight,
        value_weight,
        near,
        far,
        both,
        modulation,
        norm_gain.reshape(1, depth),
        query_gain.reshape(1, CHANNEL_SPAN),
        key_gain.reshape(1, CHANNEL_SPAN),
        cosine,
        sine,
    )
    offset = math.log(tok_count / (2.0 * ctx_rows))
    near = xor_move(give_kv, "sp", 1)
    near_q = xor_move(give_q, "sp", 1)
    up = xor_move(keep_kv, "sp", 2)
    down = xor_move(keep_kv, "sp", 6)
    near = merge(near, keep_ctx)
    near_down = xor_move(near, "sp", 6)
    near_up = xor_move(near, "sp", 2)
    across = xor_move(down, "sp", 2)
    near_across = xor_move(near_down, "sp", 2)
    (own,) = attend([(keep_q, None, [0])], [keep_kv], offset)
    near_q = ready(near_q)
    own, other = attend([(keep_q, own, [1]), (near_q, None, [0, 1])], [keep_kv, near], offset)
    for piece in (up, down, near_up, across):
        own, other = attend([(keep_q, own, [0]), (near_q, other, [0])], [piece], offset)
    (other,) = attend([(near_q, other, [0])], [near_down], offset)
    ((other,),) = attend([(near_q, other, [0])], [near_across], offset, True)
    ((own,),) = attend([(keep_q, own, [0, 1])], [near_down, near_across], offset, True)
    sent = [cross_move(other[j], j) for j in range(head_split)]
    parts = [own[0]] + [xor_move(own[j], "tp", j) for j in range(1, head_split)] + sent
    width = q_heads * CHANNEL_SPAN
    return kernel_call(
        output_body,
        jax.ShapeDtypeStruct(latent.shape, jnp.bfloat16),
        3 + len(parts),
        2 * own_rows * depth * width * head_split,
        [pltpu.VMEM((width * head_split, own_rows), jnp.bfloat16)],
    )(latent, modulation, output_weight, *parts)


def suits(mesh, latent, context, query_weight, key_weight):
    seq_split, head_split = mesh.shape["sp"], mesh.shape["tp"]
    own_rows = latent.shape[0] // (seq_split * head_split)
    ctx_rows = context.shape[0] // seq_split
    kv_heads = key_weight.shape[1] // CHANNEL_SPAN // head_split
    return (
        seq_split == 8
        and head_split == 4
        and own_rows == 2 * CHANNEL_SPAN
        and ctx_rows == CHANNEL_SPAN
        and kv_heads == 2
        and query_weight.shape[1] == 2 * key_weight.shape[1]
    )


def solution(mesh):
    in_specs = (
        P(("sp", "tp"), None),
        P("sp", None),
        P(),
        P(),
        P(),
        P("sp", "tp"),
        P("sp", "tp"),
        P("sp", "tp"),
        P(None, "tp"),
        P(None, "tp"),
        P(None, "tp"),
        P(),
        P(),
        P(),
    )
    out_specs = P(("sp", "tp"), None)

    def program(*args):
        fast = suits(mesh, args[0], args[1], args[8], args[9])
        step = jax.shard_map(
            fast_device if fast else general_device,
            mesh=mesh,
            in_specs=in_specs,
            out_specs=out_specs,
            check_vma=False,
        )
        return step(*args)

    return program
```

```python
import math

import jax
import jax.numpy as jnp
from jax import lax
from jax.experimental import pallas as pl
from jax.experimental.pallas import tpu as pltpu
from jax.sharding import PartitionSpec as P


CHANNEL_SPAN = 64
GRID_W = 64


epsilon = 1e-06
rope_base = 10000.0


def modulate(tok_rows, norm_gain, shift_row, scale_row):
    wide = tok_rows.astype(jnp.float32)
    normed = wide * lax.rsqrt(jnp.mean(wide * wide, axis=-1, keepdims=True) + epsilon)
    return (normed * norm_gain * (1.0 + scale_row) + shift_row).astype(jnp.bfloat16)


def headnorm(raw, gain, heads):
    field = raw.reshape(raw.shape[0], heads, -1)
    return field * lax.rsqrt(jnp.mean(field * field, axis=-1, keepdims=True) + epsilon) * gain


def rotate(field, places):
    count = field.shape[0]
    heads = field.shape[1]
    quarter = field.shape[2] // 4
    grid_row = (places // GRID_W).astype(jnp.float32)
    grid_col = (places % GRID_W).astype(jnp.float32)
    inverse = rope_base ** (-jnp.arange(quarter, dtype=jnp.float32) / quarter)
    angles = jnp.stack([grid_row[:, None] * inverse, grid_col[:, None] * inverse], axis=1)[:, None]
    cosine = jnp.cos(angles)
    sine = jnp.sin(angles)
    matcher_content_couples = field.reshape(count, heads, 2, 2, quarter)
    first = matcher_content_couples[:, :, :, 0]
    second = matcher_content_couples[:, :, :, 1]
    turned = jnp.stack([first * cosine - second * sine, second * cosine + first * sine], axis=3)
    return turned.reshape(count, heads, 4 * quarter)


def process_probe_group(
    accumulator_carry, probe_entries, matcher_content_couples, similarity_offset
):
    row_peak, row_total, weighted = accumulator_carry
    kv_heads = probe_entries.shape[1]
    head_size = probe_entries.shape[3]
    pair_width = kv_heads * head_size
    matcher_pieces = matcher_content_couples[:, :pair_width].reshape(
        matcher_content_couples.shape[0], kv_heads, head_size
    )
    value_rows = matcher_content_couples[:, pair_width:].reshape(
        matcher_content_couples.shape[0], kv_heads, head_size
    )
    similarity_matrix = (
        jnp.einsum(
            "dmvk,hmk->dmvh", probe_entries, matcher_pieces, preferred_element_type=jnp.float32
        )
        * head_size ** (-0.5)
        + similarity_offset
    )
    new_peak = jnp.maximum(row_peak, jnp.max(similarity_matrix, axis=-1))
    shares = jnp.exp(similarity_matrix - new_peak[..., None])
    shrink = jnp.exp(row_peak - new_peak)
    row_total = row_total * shrink + jnp.sum(shares, axis=-1)
    weighted = weighted * shrink[..., None] + jnp.einsum(
        "qkgn,nkd->qkgd",
        shares.astype(jnp.bfloat16),
        value_rows,
        preferred_element_type=jnp.float32,
    )
    return (new_peak, row_total, weighted)


def group_walker(accumulator_carry, probe_entries, matcher_content_couples, similarity_offset):
    pair_count = matcher_content_couples.shape[0]
    probe_group_total = -(-pair_count // 2048)
    while pair_count % probe_group_total:
        probe_group_total += 1
    if probe_group_total == 1:
        return process_probe_group(
            accumulator_carry, probe_entries, matcher_content_couples, similarity_offset
        )
    group_extent = pair_count // probe_group_total

    def scan_step(inner, slices):
        return (process_probe_group(inner, probe_entries, slices[0], slices[1]), None)

    result, _ = lax.scan(
        scan_step,
        accumulator_carry,
        (
            matcher_content_couples.reshape(
                probe_group_total, group_extent, matcher_content_couples.shape[1]
            ),
            similarity_offset.reshape(probe_group_total, group_extent),
        ),
    )
    return result


def general_device(
    latent,
    context,
    condition,
    context_condition,
    norm_gain,
    shift_weight,
    scale_weight,
    gate_weight,
    query_weight,
    key_weight,
    value_weight,
    query_gain,
    key_gain,
    output_weight,
):
    head_split = lax.axis_size("tp")
    seq_index = lax.axis_index("sp")
    head_index = lax.axis_index("tp")
    row_slab = shift_weight.shape[0]
    columns = shift_weight.shape[1]
    conditions = jnp.stack([condition, context_condition])
    activated = jax.nn.silu(
        lax.dynamic_slice_in_dim(conditions, seq_index * row_slab, row_slab, 1)
    ).astype(jnp.bfloat16)
    part_shift = jnp.dot(activated, shift_weight, preferred_element_type=jnp.float32)
    part_scale = jnp.dot(activated, scale_weight, preferred_element_type=jnp.float32)
    part_gate = jnp.dot(activated, gate_weight, preferred_element_type=jnp.float32)

    def widen(member):
        blank = jnp.zeros((2, columns * head_split), jnp.float32)
        return lax.dynamic_update_slice_in_dim(blank, member, head_index * columns, 1)

    shifts, scales, gates = lax.psum(
        (widen(part_shift), widen(part_scale), widen(part_gate)), ("sp", "tp")
    )
    own_rows = latent.shape[0]
    tok_count = own_rows * head_split
    ctx_rows = context.shape[0]
    hidden = modulate(latent, norm_gain, shifts[0], scales[0])
    context_hidden = modulate(context, norm_gain, shifts[1], scales[1])
    q_heads = query_weight.shape[1] // CHANNEL_SPAN
    kv_heads = key_weight.shape[1] // CHANNEL_SPAN
    group_size = q_heads // kv_heads
    q_width = q_heads * CHANNEL_SPAN
    kv_width = kv_heads * CHANNEL_SPAN
    joined_weight = jnp.concatenate([query_weight, key_weight, value_weight], axis=1)
    projected = jnp.dot(
        lax.all_gather(hidden, "tp", axis=0, tiled=True),
        joined_weight,
        preferred_element_type=jnp.float32,
    )
    places = seq_index * tok_count + jnp.arange(tok_count, dtype=jnp.int32)
    probe_entries = rotate(headnorm(projected[:, :q_width], query_gain, q_heads), places).astype(
        jnp.bfloat16
    )
    probe_entries = probe_entries.reshape(tok_count, kv_heads, group_size, CHANNEL_SPAN)
    latent_keys = rotate(
        headnorm(projected[:, q_width : q_width + kv_width], key_gain, kv_heads), places
    ).astype(jnp.bfloat16)
    latent_values = projected[:, q_width + kv_width :].astype(jnp.bfloat16)
    own_pairs = jnp.concatenate([latent_keys.reshape(tok_count, kv_width), latent_values], axis=1)
    ctx_projected = jnp.dot(
        context_hidden, joined_weight[:, q_width:], preferred_element_type=jnp.float32
    )
    ctx_keys = (
        headnorm(ctx_projected[:, :kv_width], key_gain, kv_heads)
        .astype(jnp.bfloat16)
        .reshape(ctx_rows, kv_width)
    )
    ctx_pairs = jnp.concatenate(
        [ctx_keys, ctx_projected[:, kv_width:].astype(jnp.bfloat16)], axis=1
    )
    prefix_mapped = math.log(tok_count / (2.0 * ctx_rows))
    stat_shape = (tok_count, kv_heads, group_size)
    start_state = (
        jnp.full(stat_shape, -jnp.inf, jnp.float32),
        jnp.zeros(stat_shape, jnp.float32),
        jnp.zeros(stat_shape + (CHANNEL_SPAN,), jnp.float32),
    )
    ctx_whole = lax.all_gather(ctx_pairs, "sp", axis=0, tiled=True)
    ctx_state = group_walker(
        start_state,
        probe_entries,
        ctx_whole,
        jnp.full((ctx_whole.shape[0],), prefix_mapped, jnp.float32),
    )
    key_piece = lax.all_gather(own_pairs, "sp", axis=0, tiled=True)
    final_state = group_walker(
        ctx_state, probe_entries, key_piece, jnp.zeros((key_piece.shape[0],), jnp.float32)
    )
    _, row_total, weighted = final_state
    attended = (weighted / row_total[..., None]).astype(jnp.bfloat16).reshape(tok_count, q_width)
    branch = jnp.dot(
        lax.all_to_all(attended, "tp", split_axis=0, concat_axis=1, tiled=True),
        output_weight,
        preferred_element_type=jnp.float32,
    )
    return (latent.astype(jnp.float32) + gates[0] * branch).astype(jnp.bfloat16)


LOG2E = math.log2(math.e)


def whole_spec():
    return pl.BlockSpec(memory_space=pltpu.VMEM)


def kernel_call(body, out_shape, count, flops, scratch=()):
    return pl.pallas_call(
        body,
        out_shape=out_shape,
        in_specs=[whole_spec()] * count,
        out_specs=jax.tree.map(lambda unused: whole_spec(), out_shape),
        scratch_shapes=list(scratch),
        cost_estimate=pl.CostEstimate(flops=flops, transcendentals=0, bytes_accessed=0),
        compiler_params=pltpu.CompilerParams(vmem_limit_bytes=MODEST),
    )


ROOMY = 60 * 1024 * 1024
MODEST = 32 * 1024 * 1024


def hbm_spec():
    return pl.BlockSpec(memory_space=pltpu.HBM)


def start_loads(pairs, sems):
    copies = []
    for i, (source, target) in enumerate(pairs):
        copies.append(pltpu.make_async_copy(source, target, sems.at[i]))
        copies[-1].start()
    return copies


def opening_body(first_hbm, second_hbm, shift_hbm, scale_hbm, gate_hbm, out_ref, *scratch):
    first, second, *targets, sems = scratch
    row_slab = shift_hbm.shape[0]
    cut = pl.ds(pl.multiple_of(lax.axis_index("sp") * row_slab, row_slab), row_slab)
    copies = start_loads(
        [(first_hbm.at[:, cut], first), (second_hbm.at[:, cut], second)]
        + list(zip((shift_hbm, scale_hbm, gate_hbm), targets)),
        sems,
    )
    copies[0].wait()
    copies[1].wait()
    rows = lax.broadcasted_iota(jnp.int32, (16, row_slab), 0)
    pair = jnp.where(rows == 0, first[...], second[...])
    activated = (pair / (1.0 + jnp.exp(-pair))).astype(jnp.bfloat16)
    out_ref[6:8, :] = jnp.zeros((2, out_ref.shape[1]), jnp.float32)
    for i in range(3):
        copies[2 + i].wait()
        part = jnp.dot(activated, targets[i][...], preferred_element_type=jnp.float32)
        out_ref[2 * i : 2 * i + 2, :] = part[0:2]


def combine_body(one_ref, other_ref, out_ref):
    out_ref[...] = one_ref[...] + other_ref[...]


def combine(one, other, flops):
    return kernel_call(combine_body, jax.ShapeDtypeStruct(one.shape, one.dtype), 2, flops)(
        one, other
    )


def opening(first, second, *weights):
    row_slab, columns = weights[0].shape
    return pl.pallas_call(
        opening_body,
        out_shape=jax.ShapeDtypeStruct((8, columns), jnp.float32),
        in_specs=[hbm_spec()] * 5,
        out_specs=whole_spec(),
        scratch_shapes=[pltpu.VMEM((1, row_slab), jnp.float32)] * 2
        + [pltpu.VMEM((row_slab, columns), jnp.bfloat16)] * 3
        + [pltpu.SemaphoreType.DMA((5,))],
        cost_estimate=pl.CostEstimate(flops=10**8, transcendentals=0, bytes_accessed=0),
        compiler_params=pltpu.CompilerParams(vmem_limit_bytes=ROOMY),
    )(first, second, *weights)


def turn(field, cosine, sine):
    quarter = field.shape[0] // 4
    pieces = [field[i * quarter : (i + 1) * quarter] for i in range(4)]
    swapped = jnp.concatenate([pieces[1], pieces[0], pieces[3], pieces[2]], axis=0)
    return field * cosine + swapped * sine


def projection_body(
    heads,
    kv_heads,
    own_ref,
    context_ref,
    query_ref,
    key_ref,
    value_ref,
    core_ref,
    far_ref,
    both_ref,
    mod_ref,
    gain_ref,
    query_gain_ref,
    key_gain_ref,
    cosine_ref,
    sine_ref,
    keep_q,
    keep_kv,
    keep_ctx,
    give_q,
    give_kv,
    made,
):
    span = CHANNEL_SPAN
    group = heads // kv_heads

    def vector(row):
        return jnp.concatenate([mod_ref[i, row : row + 1, :] for i in range(mod_ref.shape[0])], axis=1)

    gain = gain_ref[...]

    def hidden_of(ref, row):
        wide = ref[...].astype(jnp.float32)
        scaled = wide * lax.rsqrt(jnp.mean(wide * wide, axis=-1, keepdims=True) + epsilon)
        return (scaled * (gain * (1.0 + vector(2 + row))) + vector(row)).astype(jnp.bfloat16)

    def normed(raw, head_gain):
        return raw * lax.rsqrt(jnp.mean(raw * raw, axis=0, keepdims=True) + epsilon) * head_gain

    def upright(ref):
        return jnp.broadcast_to(ref[...], (8, span)).T[:, 0:1]

    query_gain = upright(query_gain_ref)
    key_gain = upright(key_gain_ref)
    blocks = (own_ref, core_ref, far_ref, both_ref)
    q_tiles = group * len(blocks) // 2
    waiting = {}
    for j, ref in enumerate(blocks):
        hidden = hidden_of(ref, 0)
        cosine = cosine_ref[j]
        sine = sine_ref[j]
        rows = slice(j % 2 * span, (j % 2 + 1) * span)
        queries = jnp.dot(hidden, query_ref[...], preferred_element_type=jnp.float32).T
        for h in range(heads):
            turned = turn(normed(queries[h * span : (h + 1) * span], query_gain), cosine, sine)
            kv, g = h // group, h % group
            made[kv, g * len(blocks) // 2 + j // 2, rows, :] = turned.astype(jnp.bfloat16)
        keys = jnp.dot(hidden, key_ref[...], preferred_element_type=jnp.float32).T
        values = jnp.dot(hidden, value_ref[...], preferred_element_type=jnp.float32).T
        for h in range(kv_heads):
            cut = slice(h * span, (h + 1) * span)
            turned = turn(normed(keys[cut], key_gain), cosine, sine)
            if j % 2:
                pair = jnp.concatenate([waiting[h], turned], axis=0)
                made[h, q_tiles + j // 2] = pair.T.astype(jnp.bfloat16)
            waiting[h] = turned
            made[h, q_tiles + len(blocks) // 2 + j // 2, rows, :] = values[cut].astype(jnp.bfloat16)
    hidden = hidden_of(context_ref, 1)
    keys = jnp.dot(hidden, key_ref[...], preferred_element_type=jnp.float32).T
    values = jnp.dot(hidden, value_ref[...], preferred_element_type=jnp.float32).T
    for h in range(kv_heads):
        cut = slice(h * span, (h + 1) * span)
        both = jnp.concatenate([normed(keys[cut], key_gain).T, values[cut]], axis=0)
        made[h, q_tiles + len(blocks)] = jnp.concatenate([both, jnp.zeros_like(both)], axis=1).astype(
            jnp.bfloat16
        )
    side = lax.rem(lax.axis_index("sp"), kv_heads)
    for head, q_ref, kv_ref in ((1 - side, give_q, give_kv), (side, keep_q, keep_kv)):
        for i in range(q_tiles):
            if q_ref is keep_q:
                q_ref[i], q_ref[q_tiles + i] = scaled_halves(made[head, i])
            else:
                q_ref[i] = made[head, i]
        for i in range(kv_ref.shape[0]):
            kv_ref[i] = made[head, q_tiles + i]
    keep_ctx[...] = made[side, q_tiles + len(blocks)]


def merge_body(near_ref, ctx_ref, out_ref):
    last = near_ref.shape[0] - 1
    span = ctx_ref.shape[1] // 2
    for i in range(last):
        out_ref[i] = near_ref[i]
    out_ref[last] = jnp.concatenate([near_ref[last, :, 0:span], ctx_ref[:, 0:span]], axis=1)


def merge(near, ctx):
    return kernel_call(merge_body, jax.ShapeDtypeStruct(near.shape, near.dtype), 2, 10**6)(near, ctx)


def scaled_halves(tile):
    scale = (tile.shape[-2] // 2) ** (-0.5) * LOG2E
    wide = tile.astype(jnp.float32) * scale
    high = wide.astype(jnp.bfloat16)
    return high, (wide - high.astype(jnp.float32)).astype(jnp.bfloat16)


def ready_body(q_ref, out_ref):
    count = q_ref.shape[0]
    for i in range(count):
        out_ref[i], out_ref[count + i] = scaled_halves(q_ref[i])


def ready(probes):
    shape = jax.ShapeDtypeStruct((2 * probes.shape[0], *probes.shape[1:]), probes.dtype)
    return kernel_call(ready_body, shape, 1, 10**6)(probes)


def attention_body(plan, pieces, last, offset, *refs):
    q_refs, refs = refs[: len(plan)], refs[len(plan) :]
    kv_refs, refs = refs[:pieces], refs[pieces:]
    pairs = 2
    groups = 2
    span = q_refs[0].shape[1] // 2
    halves = (0, 1)
    states = {}
    queries = {}
    tiles = []
    for i, (q_ref, (started, wanted)) in enumerate(zip(q_refs, plan)):
        if started:
            old, refs = refs[:3], refs[3:]
        for g in range(groups):
            high, low = [
                jnp.concatenate(
                    [
                        q_ref[(level * groups + g) * pairs + p, half * span : (half + 1) * span, :]
                        for p in range(pairs)
                        for half in halves
                    ],
                    axis=1,
                )
                for level in halves
            ]
            blank = jnp.zeros_like(high)
            queries[i, g, 0] = jnp.concatenate([high, blank, low, blank], axis=0)
            queries[i, g, 1] = jnp.concatenate([blank, high, blank, low], axis=0)
            if started:
                states[i, g] = tuple(ref[g] for ref in old)
            tiles += [(i, g, place, part) for place in wanted for part in halves]
    tiles.sort(key=lambda tile: tile[2:])

    def scores(tile):
        i, g, place, part = tile
        ref = kv_refs[place]
        context = ref.shape[0] > 2 * pairs
        keys = [ref[p] for p in range(pairs)]
        if context:
            keys.append(ref[2 * pairs, 0:span, :])
        keys = jnp.concatenate(keys, axis=0)
        keys = jnp.concatenate([keys, keys], axis=1)
        found = jnp.dot(keys, queries[i, g, part], preferred_element_type=jnp.float32)
        if context:
            rows = found.shape[0] - span
            found = jnp.concatenate([found[:rows], found[rows:] + offset * LOG2E], axis=0)
        return found

    def soften(tile, found):
        place = tile[:2]
        peak = jnp.max(found, axis=0, keepdims=True)
        old = states.get(place)
        if old is not None:
            peak = jnp.maximum(peak, old[0])
        shares = jnp.exp2(found - peak)
        total = jnp.sum(shares, axis=0, keepdims=True)
        shrink = None
        if old is not None:
            shrink = jnp.exp2(old[0] - peak)
            total = total + old[1] * shrink
        states[place] = (peak, total, old[2] if old is not None else None)
        return shares.astype(jnp.bfloat16), shrink

    def gather(tile, shares, shrink):
        ref = kv_refs[tile[2]]
        rows = slice(tile[3] * span, (tile[3] + 1) * span)
        values = [ref[pairs + p, rows, :] for p in range(pairs)]
        if ref.shape[0] > 2 * pairs:
            values.append(ref[2 * pairs, span : 2 * span, rows])
        weighted = jnp.dot(
            jnp.concatenate(values, axis=1), shares, preferred_element_type=jnp.float32
        )
        peak, total, old = states[tile[:2]]
        if shrink is not None:
            weighted = weighted + old * shrink
        states[tile[:2]] = (peak, total, weighted)

    following = scores(tiles[0])
    waiting = None
    for i, tile in enumerate(tiles):
        found = following
        if i + 1 < len(tiles):
            following = scores(tiles[i + 1])
        shares, shrink = soften(tile, found)
        if waiting:
            gather(*waiting)
        waiting = (tile, shares, shrink)
    gather(*waiting)
    for (i, g), (peak, total, weighted) in states.items():
        if last:
            out_ref = refs[i]
            attended = (weighted / total).astype(jnp.bfloat16)
            own_rows = out_ref.shape[2]
            for j in range(out_ref.shape[0]):
                out_ref[j, g * span : (g + 1) * span, :] = attended[
                    :, j * own_rows : (j + 1) * own_rows
                ]
        else:
            for ref, value in zip(refs[3 * i : 3 * i + 3], (peak, total, weighted)):
                ref[g] = value


def attend(sources, pieces, offset, last=False):
    probes = [source[0] for source in sources]
    lanes = 2 * 2 * probes[0].shape[2]
    span = probes[0].shape[1] // 2
    plan = [(source[1] is not None, source[2]) for source in sources]
    keys = sum(pieces[i].shape[0] * pieces[i].shape[1] // 2 for source in sources for i in source[2])
    inputs = probes + pieces
    for source in sources:
        inputs += list(source[1] or ())
    if last:
        out = [jax.ShapeDtypeStruct((4, 2 * span, probes[0].shape[2]), jnp.bfloat16)]
    else:
        stat = jax.ShapeDtypeStruct((2, 1, lanes), jnp.float32)
        out = [stat, stat, jax.ShapeDtypeStruct((2, span, lanes), jnp.float32)]

    def body(*refs):
        attention_body(plan, len(pieces), last, offset, *refs)

    found = kernel_call(
        body, out * len(sources), len(inputs), 40 * 2 * lanes * keys * span
    )(*inputs)
    size = len(out)
    return [found[size * i : size * (i + 1)] for i in range(len(sources))]


def output_body(latent_ref, mod_ref, weight_ref, *refs):
    out_ref, lhs_ref = refs[-2:]
    parts = refs[:-2]
    head_index = lax.axis_index("tp")
    side = lax.rem(lax.axis_index("sp"), 2)
    rows = parts[0].shape[0]
    for i, ref in enumerate(parts):
        j, flip = i % (len(parts) // 2), i // (len(parts) // 2)
        place = jnp.bitwise_xor(head_index, j) * 2 + jnp.bitwise_xor(side, flip)
        lhs_ref[pl.ds(pl.multiple_of(place * rows, rows), rows), :] = ref[...]
    lhs = lhs_ref[...].T
    columns = mod_ref.shape[2]
    for i in range(mod_ref.shape[0]):
        cut = slice(i * columns, (i + 1) * columns)
        branch = jnp.dot(lhs, weight_ref[:, cut], preferred_element_type=jnp.float32)
        gate = mod_ref[i, 4:5, :]
        out_ref[:, cut] = (latent_ref[:, cut].astype(jnp.float32) + gate * branch).astype(
            jnp.bfloat16
        )


def fast_device(*args):
    return inner_device(*args)


def xor_move(member, axis, mask):
    size = lax.axis_size(axis)
    return lax.ppermute(member, axis, [(i, i ^ mask) for i in range(size)])


def cross_move(member, mask):
    seq_split, head_split = lax.axis_size("sp"), lax.axis_size("tp")
    pairs = [
        (i * head_split + j, (i ^ 1) * head_split + (j ^ mask))
        for i in range(seq_split)
        for j in range(head_split)
    ]
    return lax.ppermute(member, ("sp", "tp"), pairs)


def tables(seq_index, head_index, own_rows, head_split):
    quarter = CHANNEL_SPAN // 4
    blocks = jnp.bitwise_xor(jnp.arange(head_split, dtype=jnp.int32), head_index)
    places = (
        seq_index * own_rows * head_split
        + blocks[:, None] * own_rows
        + jnp.arange(own_rows, dtype=jnp.int32)
    )
    inverse = rope_base ** (-jnp.arange(quarter, dtype=jnp.float32) / quarter)
    grid_row = (places // GRID_W).astype(jnp.float32)[:, None, :] * inverse[:, None]
    grid_col = (places % GRID_W).astype(jnp.float32)[:, None, :] * inverse[:, None]
    row_sine, col_sine = jnp.sin(grid_row), jnp.sin(grid_col)
    row_cosine, col_cosine = jnp.cos(grid_row), jnp.cos(grid_col)
    cosine = jnp.concatenate([row_cosine, row_cosine, col_cosine, col_cosine], axis=1)
    sine = jnp.concatenate([-row_sine, row_sine, -col_sine, col_sine], axis=1)
    return cosine, sine


def inner_device(
    latent,
    context,
    condition,
    context_condition,
    norm_gain,
    shift_weight,
    scale_weight,
    gate_weight,
    query_weight,
    key_weight,
    value_weight,
    query_gain,
    key_gain,
    output_weight,
):
    head_split = lax.axis_size("tp")
    seq_split = lax.axis_size("sp")
    seq_index = lax.axis_index("sp")
    head_index = lax.axis_index("tp")
    own_rows, depth = latent.shape
    ctx_rows = context.shape[0]
    tok_count = own_rows * head_split
    q_heads = query_weight.shape[1] // CHANNEL_SPAN
    kv_heads = key_weight.shape[1] // CHANNEL_SPAN

    part = opening(
        condition.reshape(1, depth),
        context_condition.reshape(1, depth),
        shift_weight,
        scale_weight,
        gate_weight,
    )
    far = xor_move(latent, "tp", 2)
    near = xor_move(latent, "tp", 1)
    mask = seq_split // 2
    while mask:
        other = xor_move(part, "sp", mask)
        part = combine(part, other, 10**11 if 2 * mask == seq_split else 10**6)
        mask //= 2
    both = xor_move(far, "tp", 1)
    modulation = lax.all_gather(part, "tp", axis=0, tiled=False)
    cosine, sine = tables(seq_index, head_index, own_rows, head_split)
    q_tiles = q_heads // kv_heads * head_split // 2
    kv_tiles = head_split
    tile = (own_rows, own_rows)
    keep_q, keep_kv, keep_ctx, give_q, give_kv = pl.pallas_call(
        lambda *refs: projection_body(q_heads, kv_heads, *refs),
        out_shape=[
            jax.ShapeDtypeStruct((*count, *tile), jnp.bfloat16)
            for count in ((2 * q_tiles,), (kv_tiles,), (), (q_tiles,), (kv_tiles + 1,))
        ],
        in_specs=[whole_spec()] * 14,
        out_specs=[whole_spec()] * 5,
        scratch_shapes=[pltpu.VMEM((kv_heads, q_tiles + kv_tiles + 1, *tile), jnp.bfloat16)],
        cost_estimate=pl.CostEstimate(
            flops=4 * tok_count * depth * (q_heads + 2 * kv_heads) * CHANNEL_SPAN,
            transcendentals=0,
            bytes_accessed=0,
        ),
        compiler_params=pltpu.CompilerParams(vmem_limit_bytes=MODEST),
    )(
        latent,
        context,
        query_weight,
        key_weight,
        value_weight,
        near,
        far,
        both,
        modulation,
        norm_gain.reshape(1, depth),
        query_gain.reshape(1, CHANNEL_SPAN),
        key_gain.reshape(1, CHANNEL_SPAN),
        cosine,
        sine,
    )
    offset = math.log(tok_count / (2.0 * ctx_rows))
    near = xor_move(give_kv, "sp", 1)
    near_q = xor_move(give_q, "sp", 1)
    up = xor_move(keep_kv, "sp", 2)
    down = xor_move(keep_kv, "sp", 4)
    near = merge(near, keep_ctx)
    near_down = xor_move(near, "sp", 4)
    near_up = xor_move(near, "sp", 2)
    across = xor_move(down, "sp", 2)
    near_across = xor_move(near_down, "sp", 2)
    (own,) = attend([(keep_q, None, [0])], [keep_kv], offset)
    (own,) = attend([(keep_q, own, [0])], [near], offset)
    near_q = ready(near_q)
    own, other = attend(
        [(keep_q, own, [2, 3]), (near_q, None, [0, 1, 2, 3])], [keep_kv, near, up, down], offset
    )
    own, other = attend(
        [(keep_q, own, [0]), (near_q, other, [0, 1])], [near_up, near_down], offset
    )
    own, other = attend([(keep_q, own, [0]), (near_q, other, [0])], [across], offset)
    ((other,),) = attend([(near_q, other, [0])], [near_across], offset, True)
    ((own,),) = attend([(keep_q, own, [0, 1])], [near_down, near_across], offset, True)
    sent = [cross_move(other[j], j) for j in range(head_split)]
    parts = [own[0]] + [xor_move(own[j], "tp", j) for j in range(1, head_split)] + sent
    width = q_heads * CHANNEL_SPAN
    return kernel_call(
        output_body,
        jax.ShapeDtypeStruct(latent.shape, jnp.bfloat16),
        3 + len(parts),
        2 * own_rows * depth * width * head_split,
        [pltpu.VMEM((width * head_split, own_rows), jnp.bfloat16)],
    )(latent, modulation, output_weight, *parts)


def suits(mesh, latent, context, query_weight, key_weight):
    seq_split, head_split = mesh.shape["sp"], mesh.shape["tp"]
    own_rows = latent.shape[0] // (seq_split * head_split)
    ctx_rows = context.shape[0] // seq_split
    kv_heads = key_weight.shape[1] // CHANNEL_SPAN // head_split
    return (
        seq_split == 8
        and head_split == 4
        and own_rows == 2 * CHANNEL_SPAN
        and ctx_rows == CHANNEL_SPAN
        and kv_heads == 2
        and query_weight.shape[1] == 2 * key_weight.shape[1]
    )


def solution(mesh):
    in_specs = (
        P(("sp", "tp"), None),
        P("sp", None),
        P(),
        P(),
        P(),
        P("sp", "tp"),
        P("sp", "tp"),
        P("sp", "tp"),
        P(None, "tp"),
        P(None, "tp"),
        P(None, "tp"),
        P(),
        P(),
        P(),
    )
    out_specs = P(("sp", "tp"), None)

    def program(*args):
        fast = suits(mesh, args[0], args[1], args[8], args[9])
        step = jax.shard_map(
            fast_device if fast else general_device,
            mesh=mesh,
            in_specs=in_specs,
            out_specs=out_specs,
            check_vma=False,
        )
        return step(*args)

    return program
```

```python
import math

import jax
import jax.numpy as jnp
from jax import lax
from jax.experimental import pallas as pl
from jax.experimental.pallas import tpu as pltpu
from jax.sharding import PartitionSpec as P


CHANNEL_SPAN = 64
GRID_W = 64


epsilon = 1e-06
rope_base = 10000.0


def modulate(tok_rows, norm_gain, shift_row, scale_row):
    wide = tok_rows.astype(jnp.float32)
    normed = wide * lax.rsqrt(jnp.mean(wide * wide, axis=-1, keepdims=True) + epsilon)
    return (normed * norm_gain * (1.0 + scale_row) + shift_row).astype(jnp.bfloat16)


def headnorm(raw, gain, heads):
    field = raw.reshape(raw.shape[0], heads, -1)
    return field * lax.rsqrt(jnp.mean(field * field, axis=-1, keepdims=True) + epsilon) * gain


def rotate(field, places):
    count = field.shape[0]
    heads = field.shape[1]
    quarter = field.shape[2] // 4
    grid_row = (places // GRID_W).astype(jnp.float32)
    grid_col = (places % GRID_W).astype(jnp.float32)
    inverse = rope_base ** (-jnp.arange(quarter, dtype=jnp.float32) / quarter)
    angles = jnp.stack([grid_row[:, None] * inverse, grid_col[:, None] * inverse], axis=1)[:, None]
    cosine = jnp.cos(angles)
    sine = jnp.sin(angles)
    matcher_content_couples = field.reshape(count, heads, 2, 2, quarter)
    first = matcher_content_couples[:, :, :, 0]
    second = matcher_content_couples[:, :, :, 1]
    turned = jnp.stack([first * cosine - second * sine, second * cosine + first * sine], axis=3)
    return turned.reshape(count, heads, 4 * quarter)


def process_probe_group(
    accumulator_carry, probe_entries, matcher_content_couples, similarity_offset
):
    row_peak, row_total, weighted = accumulator_carry
    kv_heads = probe_entries.shape[1]
    head_size = probe_entries.shape[3]
    pair_width = kv_heads * head_size
    matcher_pieces = matcher_content_couples[:, :pair_width].reshape(
        matcher_content_couples.shape[0], kv_heads, head_size
    )
    value_rows = matcher_content_couples[:, pair_width:].reshape(
        matcher_content_couples.shape[0], kv_heads, head_size
    )
    similarity_matrix = (
        jnp.einsum(
            "dmvk,hmk->dmvh", probe_entries, matcher_pieces, preferred_element_type=jnp.float32
        )
        * head_size ** (-0.5)
        + similarity_offset
    )
    new_peak = jnp.maximum(row_peak, jnp.max(similarity_matrix, axis=-1))
    shares = jnp.exp(similarity_matrix - new_peak[..., None])
    shrink = jnp.exp(row_peak - new_peak)
    row_total = row_total * shrink + jnp.sum(shares, axis=-1)
    weighted = weighted * shrink[..., None] + jnp.einsum(
        "qkgn,nkd->qkgd",
        shares.astype(jnp.bfloat16),
        value_rows,
        preferred_element_type=jnp.float32,
    )
    return (new_peak, row_total, weighted)


def group_walker(accumulator_carry, probe_entries, matcher_content_couples, similarity_offset):
    pair_count = matcher_content_couples.shape[0]
    probe_group_total = -(-pair_count // 2048)
    while pair_count % probe_group_total:
        probe_group_total += 1
    if probe_group_total == 1:
        return process_probe_group(
            accumulator_carry, probe_entries, matcher_content_couples, similarity_offset
        )
    group_extent = pair_count // probe_group_total

    def scan_step(inner, slices):
        return (process_probe_group(inner, probe_entries, slices[0], slices[1]), None)

    result, _ = lax.scan(
        scan_step,
        accumulator_carry,
        (
            matcher_content_couples.reshape(
                probe_group_total, group_extent, matcher_content_couples.shape[1]
            ),
            similarity_offset.reshape(probe_group_total, group_extent),
        ),
    )
    return result


def general_device(
    latent,
    context,
    condition,
    context_condition,
    norm_gain,
    shift_weight,
    scale_weight,
    gate_weight,
    query_weight,
    key_weight,
    value_weight,
    query_gain,
    key_gain,
    output_weight,
):
    head_split = lax.axis_size("tp")
    seq_index = lax.axis_index("sp")
    head_index = lax.axis_index("tp")
    row_slab = shift_weight.shape[0]
    columns = shift_weight.shape[1]
    conditions = jnp.stack([condition, context_condition])
    activated = jax.nn.silu(
        lax.dynamic_slice_in_dim(conditions, seq_index * row_slab, row_slab, 1)
    ).astype(jnp.bfloat16)
    part_shift = jnp.dot(activated, shift_weight, preferred_element_type=jnp.float32)
    part_scale = jnp.dot(activated, scale_weight, preferred_element_type=jnp.float32)
    part_gate = jnp.dot(activated, gate_weight, preferred_element_type=jnp.float32)

    def widen(member):
        blank = jnp.zeros((2, columns * head_split), jnp.float32)
        return lax.dynamic_update_slice_in_dim(blank, member, head_index * columns, 1)

    shifts, scales, gates = lax.psum(
        (widen(part_shift), widen(part_scale), widen(part_gate)), ("sp", "tp")
    )
    own_rows = latent.shape[0]
    tok_count = own_rows * head_split
    ctx_rows = context.shape[0]
    hidden = modulate(latent, norm_gain, shifts[0], scales[0])
    context_hidden = modulate(context, norm_gain, shifts[1], scales[1])
    q_heads = query_weight.shape[1] // CHANNEL_SPAN
    kv_heads = key_weight.shape[1] // CHANNEL_SPAN
    group_size = q_heads // kv_heads
    q_width = q_heads * CHANNEL_SPAN
    kv_width = kv_heads * CHANNEL_SPAN
    joined_weight = jnp.concatenate([query_weight, key_weight, value_weight], axis=1)
    projected = jnp.dot(
        lax.all_gather(hidden, "tp", axis=0, tiled=True),
        joined_weight,
        preferred_element_type=jnp.float32,
    )
    places = seq_index * tok_count + jnp.arange(tok_count, dtype=jnp.int32)
    probe_entries = rotate(headnorm(projected[:, :q_width], query_gain, q_heads), places).astype(
        jnp.bfloat16
    )
    probe_entries = probe_entries.reshape(tok_count, kv_heads, group_size, CHANNEL_SPAN)
    latent_keys = rotate(
        headnorm(projected[:, q_width : q_width + kv_width], key_gain, kv_heads), places
    ).astype(jnp.bfloat16)
    latent_values = projected[:, q_width + kv_width :].astype(jnp.bfloat16)
    own_pairs = jnp.concatenate([latent_keys.reshape(tok_count, kv_width), latent_values], axis=1)
    ctx_projected = jnp.dot(
        context_hidden, joined_weight[:, q_width:], preferred_element_type=jnp.float32
    )
    ctx_keys = (
        headnorm(ctx_projected[:, :kv_width], key_gain, kv_heads)
        .astype(jnp.bfloat16)
        .reshape(ctx_rows, kv_width)
    )
    ctx_pairs = jnp.concatenate(
        [ctx_keys, ctx_projected[:, kv_width:].astype(jnp.bfloat16)], axis=1
    )
    prefix_mapped = math.log(tok_count / (2.0 * ctx_rows))
    stat_shape = (tok_count, kv_heads, group_size)
    start_state = (
        jnp.full(stat_shape, -jnp.inf, jnp.float32),
        jnp.zeros(stat_shape, jnp.float32),
        jnp.zeros(stat_shape + (CHANNEL_SPAN,), jnp.float32),
    )
    ctx_whole = lax.all_gather(ctx_pairs, "sp", axis=0, tiled=True)
    ctx_state = group_walker(
        start_state,
        probe_entries,
        ctx_whole,
        jnp.full((ctx_whole.shape[0],), prefix_mapped, jnp.float32),
    )
    key_piece = lax.all_gather(own_pairs, "sp", axis=0, tiled=True)
    final_state = group_walker(
        ctx_state, probe_entries, key_piece, jnp.zeros((key_piece.shape[0],), jnp.float32)
    )
    _, row_total, weighted = final_state
    attended = (weighted / row_total[..., None]).astype(jnp.bfloat16).reshape(tok_count, q_width)
    branch = jnp.dot(
        lax.all_to_all(attended, "tp", split_axis=0, concat_axis=1, tiled=True),
        output_weight,
        preferred_element_type=jnp.float32,
    )
    return (latent.astype(jnp.float32) + gates[0] * branch).astype(jnp.bfloat16)


LOG2E = math.log2(math.e)


def whole_spec():
    return pl.BlockSpec(memory_space=pltpu.VMEM)


def kernel_call(body, out_shape, count, flops, scratch=()):
    return pl.pallas_call(
        body,
        out_shape=out_shape,
        in_specs=[whole_spec()] * count,
        out_specs=jax.tree.map(lambda unused: whole_spec(), out_shape),
        scratch_shapes=list(scratch),
        cost_estimate=pl.CostEstimate(flops=flops, transcendentals=0, bytes_accessed=0),
        compiler_params=pltpu.CompilerParams(vmem_limit_bytes=MODEST),
    )


ROOMY = 60 * 1024 * 1024
MODEST = 32 * 1024 * 1024


def hbm_spec():
    return pl.BlockSpec(memory_space=pltpu.HBM)


def start_loads(pairs, sems):
    copies = []
    for i, (source, target) in enumerate(pairs):
        copies.append(pltpu.make_async_copy(source, target, sems.at[i]))
        copies[-1].start()
    return copies


def opening_body(first_hbm, second_hbm, shift_hbm, scale_hbm, gate_hbm, out_ref, *scratch):
    first, second, *targets, sems = scratch
    row_slab = shift_hbm.shape[0]
    cut = pl.ds(pl.multiple_of(lax.axis_index("sp") * row_slab, row_slab), row_slab)
    copies = start_loads(
        [(first_hbm.at[:, cut], first), (second_hbm.at[:, cut], second)]
        + list(zip((shift_hbm, scale_hbm, gate_hbm), targets)),
        sems,
    )
    copies[0].wait()
    copies[1].wait()
    rows = lax.broadcasted_iota(jnp.int32, (16, row_slab), 0)
    pair = jnp.where(rows == 0, first[...], second[...])
    activated = (pair / (1.0 + jnp.exp(-pair))).astype(jnp.bfloat16)
    out_ref[6:8, :] = jnp.zeros((2, out_ref.shape[1]), jnp.float32)
    for i in range(3):
        copies[2 + i].wait()
        part = jnp.dot(activated, targets[i][...], preferred_element_type=jnp.float32)
        out_ref[2 * i : 2 * i + 2, :] = part[0:2]


def combine_body(one_ref, other_ref, out_ref):
    out_ref[...] = one_ref[...] + other_ref[...]


def combine(one, other, flops):
    return kernel_call(combine_body, jax.ShapeDtypeStruct(one.shape, one.dtype), 2, flops)(
        one, other
    )


def opening(first, second, *weights):
    row_slab, columns = weights[0].shape
    return pl.pallas_call(
        opening_body,
        out_shape=jax.ShapeDtypeStruct((8, columns), jnp.float32),
        in_specs=[hbm_spec()] * 5,
        out_specs=whole_spec(),
        scratch_shapes=[pltpu.VMEM((1, row_slab), jnp.float32)] * 2
        + [pltpu.VMEM((row_slab, columns), jnp.bfloat16)] * 3
        + [pltpu.SemaphoreType.DMA((5,))],
        cost_estimate=pl.CostEstimate(flops=10**8, transcendentals=0, bytes_accessed=0),
        compiler_params=pltpu.CompilerParams(vmem_limit_bytes=ROOMY),
    )(first, second, *weights)


def turn(field, cosine, sine):
    quarter = field.shape[0] // 4
    pieces = [field[i * quarter : (i + 1) * quarter] for i in range(4)]
    swapped = jnp.concatenate([pieces[1], pieces[0], pieces[3], pieces[2]], axis=0)
    return field * cosine + swapped * sine


def projection_body(
    heads,
    kv_heads,
    own_ref,
    context_ref,
    query_ref,
    key_ref,
    value_ref,
    core_ref,
    far_ref,
    both_ref,
    mod_ref,
    gain_ref,
    query_gain_ref,
    key_gain_ref,
    cosine_ref,
    sine_ref,
    keep_q,
    keep_kv,
    keep_ctx,
    give_q,
    give_kv,
    made,
):
    span = CHANNEL_SPAN
    group = heads // kv_heads

    def vector(row):
        return jnp.concatenate([mod_ref[i, row : row + 1, :] for i in range(mod_ref.shape[0])], axis=1)

    gain = gain_ref[...]

    def hidden_of(ref, row):
        wide = ref[...].astype(jnp.float32)
        scaled = wide * lax.rsqrt(jnp.mean(wide * wide, axis=-1, keepdims=True) + epsilon)
        return (scaled * (gain * (1.0 + vector(2 + row))) + vector(row)).astype(jnp.bfloat16)

    def normed(raw, head_gain):
        return raw * lax.rsqrt(jnp.mean(raw * raw, axis=0, keepdims=True) + epsilon) * head_gain

    def upright(ref):
        return jnp.broadcast_to(ref[...], (8, span)).T[:, 0:1]

    query_gain = upright(query_gain_ref)
    key_gain = upright(key_gain_ref)
    blocks = (own_ref, core_ref, far_ref, both_ref)
    q_tiles = group * len(blocks) // 2
    waiting = {}
    for j, ref in enumerate(blocks):
        hidden = hidden_of(ref, 0)
        cosine = cosine_ref[j]
        sine = sine_ref[j]
        rows = slice(j % 2 * span, (j % 2 + 1) * span)
        queries = jnp.dot(hidden, query_ref[...], preferred_element_type=jnp.float32).T
        for h in range(heads):
            turned = turn(normed(queries[h * span : (h + 1) * span], query_gain), cosine, sine)
            kv, g = h // group, h % group
            made[kv, g * len(blocks) // 2 + j // 2, rows, :] = turned.astype(jnp.bfloat16)
        keys = jnp.dot(hidden, key_ref[...], preferred_element_type=jnp.float32).T
        values = jnp.dot(hidden, value_ref[...], preferred_element_type=jnp.float32).T
        for h in range(kv_heads):
            cut = slice(h * span, (h + 1) * span)
            turned = turn(normed(keys[cut], key_gain), cosine, sine)
            if j % 2:
                pair = jnp.concatenate([waiting[h], turned], axis=0)
                made[h, q_tiles + j // 2] = pair.T.astype(jnp.bfloat16)
            waiting[h] = turned
            made[h, q_tiles + len(blocks) // 2 + j // 2, rows, :] = values[cut].astype(jnp.bfloat16)
    hidden = hidden_of(context_ref, 1)
    keys = jnp.dot(hidden, key_ref[...], preferred_element_type=jnp.float32).T
    values = jnp.dot(hidden, value_ref[...], preferred_element_type=jnp.float32).T
    for h in range(kv_heads):
        cut = slice(h * span, (h + 1) * span)
        both = jnp.concatenate([normed(keys[cut], key_gain).T, values[cut]], axis=0)
        made[h, q_tiles + len(blocks)] = jnp.concatenate([both, jnp.zeros_like(both)], axis=1).astype(
            jnp.bfloat16
        )
    side = lax.rem(lax.axis_index("sp"), kv_heads)
    for head, q_ref, kv_ref in ((1 - side, give_q, give_kv), (side, keep_q, keep_kv)):
        for i in range(q_tiles):
            if q_ref is keep_q:
                q_ref[i], q_ref[q_tiles + i] = scaled_halves(made[head, i])
            else:
                q_ref[i] = made[head, i]
        for i in range(kv_ref.shape[0]):
            kv_ref[i] = made[head, q_tiles + i]
    keep_ctx[...] = made[side, q_tiles + len(blocks)]


def merge_body(near_ref, ctx_ref, out_ref):
    last = near_ref.shape[0] - 1
    span = ctx_ref.shape[1] // 2
    for i in range(last):
        out_ref[i] = near_ref[i]
    out_ref[last] = jnp.concatenate([near_ref[last, :, 0:span], ctx_ref[:, 0:span]], axis=1)


def merge(near, ctx):
    return kernel_call(merge_body, jax.ShapeDtypeStruct(near.shape, near.dtype), 2, 10**6)(near, ctx)


def scaled_halves(tile):
    scale = (tile.shape[-2] // 2) ** (-0.5) * LOG2E
    wide = tile.astype(jnp.float32) * scale
    high = wide.astype(jnp.bfloat16)
    return high, (wide - high.astype(jnp.float32)).astype(jnp.bfloat16)


def ready_body(q_ref, out_ref):
    count = q_ref.shape[0]
    for i in range(count):
        out_ref[i], out_ref[count + i] = scaled_halves(q_ref[i])


def ready(probes):
    shape = jax.ShapeDtypeStruct((2 * probes.shape[0], *probes.shape[1:]), probes.dtype)
    return kernel_call(ready_body, shape, 1, 10**6)(probes)


def attention_body(plan, pieces, last, offset, *refs):
    q_refs, refs = refs[: len(plan)], refs[len(plan) :]
    kv_refs, refs = refs[:pieces], refs[pieces:]
    pairs = 2
    groups = 2
    span = q_refs[0].shape[1] // 2
    halves = (0, 1)
    states = {}
    queries = {}
    tiles = []
    for i, (q_ref, (started, wanted)) in enumerate(zip(q_refs, plan)):
        if started:
            old, refs = refs[:3], refs[3:]
        for g in range(groups):
            high, low = [
                jnp.concatenate(
                    [
                        q_ref[(level * groups + g) * pairs + p, half * span : (half + 1) * span, :]
                        for p in range(pairs)
                        for half in halves
                    ],
                    axis=1,
                )
                for level in halves
            ]
            blank = jnp.zeros_like(high)
            queries[i, g, 0] = jnp.concatenate([high, blank, low, blank], axis=0)
            queries[i, g, 1] = jnp.concatenate([blank, high, blank, low], axis=0)
            if started:
                states[i, g] = tuple(ref[g] for ref in old)
            tiles += [(i, g, place, part) for place in wanted for part in halves]
    tiles.sort(key=lambda tile: tile[2:])

    def scores(tile):
        i, g, place, part = tile
        ref = kv_refs[place]
        context = ref.shape[0] > 2 * pairs
        keys = [ref[p] for p in range(pairs)]
        if context:
            keys.append(ref[2 * pairs, 0:span, :])
        keys = jnp.concatenate(keys, axis=0)
        keys = jnp.concatenate([keys, keys], axis=1)
        found = jnp.dot(keys, queries[i, g, part], preferred_element_type=jnp.float32)
        if context:
            rows = found.shape[0] - span
            found = jnp.concatenate([found[:rows], found[rows:] + offset * LOG2E], axis=0)
        return found

    def soften(tile, found):
        place = tile[:2]
        peak = jnp.max(found, axis=0, keepdims=True)
        old = states.get(place)
        if old is not None:
            peak = jnp.maximum(peak, old[0])
        shares = jnp.exp2(found - peak)
        total = jnp.sum(shares, axis=0, keepdims=True)
        shrink = None
        if old is not None:
            shrink = jnp.exp2(old[0] - peak)
            total = total + old[1] * shrink
        states[place] = (peak, total, old[2] if old is not None else None)
        return shares.astype(jnp.bfloat16), shrink

    def gather(tile, shares, shrink):
        ref = kv_refs[tile[2]]
        rows = slice(tile[3] * span, (tile[3] + 1) * span)
        values = [ref[pairs + p, rows, :] for p in range(pairs)]
        if ref.shape[0] > 2 * pairs:
            values.append(ref[2 * pairs, span : 2 * span, rows])
        weighted = jnp.dot(
            jnp.concatenate(values, axis=1), shares, preferred_element_type=jnp.float32
        )
        peak, total, old = states[tile[:2]]
        if shrink is not None:
            weighted = weighted + old * shrink
        states[tile[:2]] = (peak, total, weighted)

    following = scores(tiles[0])
    waiting = None
    for i, tile in enumerate(tiles):
        found = following
        if i + 1 < len(tiles):
            following = scores(tiles[i + 1])
        shares, shrink = soften(tile, found)
        if waiting:
            gather(*waiting)
        waiting = (tile, shares, shrink)
    gather(*waiting)
    for (i, g), (peak, total, weighted) in states.items():
        if last:
            out_ref = refs[i]
            attended = (weighted / total).astype(jnp.bfloat16)
            own_rows = out_ref.shape[2]
            for j in range(out_ref.shape[0]):
                out_ref[j, g * span : (g + 1) * span, :] = attended[
                    :, j * own_rows : (j + 1) * own_rows
                ]
        else:
            for ref, value in zip(refs[3 * i : 3 * i + 3], (peak, total, weighted)):
                ref[g] = value


def attend(sources, pieces, offset, last=False):
    probes = [source[0] for source in sources]
    lanes = 2 * 2 * probes[0].shape[2]
    span = probes[0].shape[1] // 2
    plan = [(source[1] is not None, source[2]) for source in sources]
    keys = sum(pieces[i].shape[0] * pieces[i].shape[1] // 2 for source in sources for i in source[2])
    inputs = probes + pieces
    for source in sources:
        inputs += list(source[1] or ())
    if last:
        out = [jax.ShapeDtypeStruct((4, 2 * span, probes[0].shape[2]), jnp.bfloat16)]
    else:
        stat = jax.ShapeDtypeStruct((2, 1, lanes), jnp.float32)
        out = [stat, stat, jax.ShapeDtypeStruct((2, span, lanes), jnp.float32)]

    def body(*refs):
        attention_body(plan, len(pieces), last, offset, *refs)

    found = kernel_call(
        body, out * len(sources), len(inputs), 40 * 2 * lanes * keys * span
    )(*inputs)
    size = len(out)
    return [found[size * i : size * (i + 1)] for i in range(len(sources))]


def output_body(latent_ref, mod_ref, weight_ref, *refs):
    out_ref, lhs_ref = refs[-2:]
    parts = refs[:-2]
    head_index = lax.axis_index("tp")
    side = lax.rem(lax.axis_index("sp"), 2)
    rows = parts[0].shape[0]
    for i, ref in enumerate(parts):
        j, flip = i % (len(parts) // 2), i // (len(parts) // 2)
        place = jnp.bitwise_xor(head_index, j) * 2 + jnp.bitwise_xor(side, flip)
        lhs_ref[pl.ds(pl.multiple_of(place * rows, rows), rows), :] = ref[...]
    lhs = lhs_ref[...].T
    columns = mod_ref.shape[2]
    for i in range(mod_ref.shape[0]):
        cut = slice(i * columns, (i + 1) * columns)
        branch = jnp.dot(lhs, weight_ref[:, cut], preferred_element_type=jnp.float32)
        gate = mod_ref[i, 4:5, :]
        out_ref[:, cut] = (latent_ref[:, cut].astype(jnp.float32) + gate * branch).astype(
            jnp.bfloat16
        )


def fast_device(*args):
    return inner_device(*args)


def xor_move(member, axis, mask):
    size = lax.axis_size(axis)
    return lax.ppermute(member, axis, [(i, i ^ mask) for i in range(size)])


def cross_move(member, mask):
    seq_split, head_split = lax.axis_size("sp"), lax.axis_size("tp")
    pairs = [
        (i * head_split + j, (i ^ 1) * head_split + (j ^ mask))
        for i in range(seq_split)
        for j in range(head_split)
    ]
    return lax.ppermute(member, ("sp", "tp"), pairs)


def tables(seq_index, head_index, own_rows, head_split):
    quarter = CHANNEL_SPAN // 4
    blocks = jnp.bitwise_xor(jnp.arange(head_split, dtype=jnp.int32), head_index)
    places = (
        seq_index * own_rows * head_split
        + blocks[:, None] * own_rows
        + jnp.arange(own_rows, dtype=jnp.int32)
    )
    inverse = rope_base ** (-jnp.arange(quarter, dtype=jnp.float32) / quarter)
    grid_row = (places // GRID_W).astype(jnp.float32)[:, None, :] * inverse[:, None]
    grid_col = (places % GRID_W).astype(jnp.float32)[:, None, :] * inverse[:, None]
    row_sine, col_sine = jnp.sin(grid_row), jnp.sin(grid_col)
    row_cosine, col_cosine = jnp.cos(grid_row), jnp.cos(grid_col)
    cosine = jnp.concatenate([row_cosine, row_cosine, col_cosine, col_cosine], axis=1)
    sine = jnp.concatenate([-row_sine, row_sine, -col_sine, col_sine], axis=1)
    return cosine, sine


def inner_device(
    latent,
    context,
    condition,
    context_condition,
    norm_gain,
    shift_weight,
    scale_weight,
    gate_weight,
    query_weight,
    key_weight,
    value_weight,
    query_gain,
    key_gain,
    output_weight,
):
    head_split = lax.axis_size("tp")
    seq_split = lax.axis_size("sp")
    seq_index = lax.axis_index("sp")
    head_index = lax.axis_index("tp")
    own_rows, depth = latent.shape
    ctx_rows = context.shape[0]
    tok_count = own_rows * head_split
    q_heads = query_weight.shape[1] // CHANNEL_SPAN
    kv_heads = key_weight.shape[1] // CHANNEL_SPAN

    part = opening(
        condition.reshape(1, depth),
        context_condition.reshape(1, depth),
        shift_weight,
        scale_weight,
        gate_weight,
    )
    far = xor_move(latent, "tp", 2)
    near = xor_move(latent, "tp", 1)
    mask = seq_split // 2
    while mask:
        other = xor_move(part, "sp", mask)
        part = combine(part, other, 10**11 if 2 * mask == seq_split else 10**6)
        mask //= 2
    both = xor_move(far, "tp", 1)
    modulation = lax.all_gather(part, "tp", axis=0, tiled=False)
    cosine, sine = tables(seq_index, head_index, own_rows, head_split)
    q_tiles = q_heads // kv_heads * head_split // 2
    kv_tiles = head_split
    tile = (own_rows, own_rows)
    keep_q, keep_kv, keep_ctx, give_q, give_kv = pl.pallas_call(
        lambda *refs: projection_body(q_heads, kv_heads, *refs),
        out_shape=[
            jax.ShapeDtypeStruct((*count, *tile), jnp.bfloat16)
            for count in ((2 * q_tiles,), (kv_tiles,), (), (q_tiles,), (kv_tiles + 1,))
        ],
        in_specs=[whole_spec()] * 14,
        out_specs=[whole_spec()] * 5,
        scratch_shapes=[pltpu.VMEM((kv_heads, q_tiles + kv_tiles + 1, *tile), jnp.bfloat16)],
        cost_estimate=pl.CostEstimate(
            flops=4 * tok_count * depth * (q_heads + 2 * kv_heads) * CHANNEL_SPAN,
            transcendentals=0,
            bytes_accessed=0,
        ),
        compiler_params=pltpu.CompilerParams(vmem_limit_bytes=MODEST),
    )(
        latent,
        context,
        query_weight,
        key_weight,
        value_weight,
        near,
        far,
        both,
        modulation,
        norm_gain.reshape(1, depth),
        query_gain.reshape(1, CHANNEL_SPAN),
        key_gain.reshape(1, CHANNEL_SPAN),
        cosine,
        sine,
    )
    offset = math.log(tok_count / (2.0 * ctx_rows))
    near = xor_move(give_kv, "sp", 1)
    near_q = xor_move(give_q, "sp", 1)
    up = xor_move(keep_kv, "sp", 2)
    down = xor_move(keep_kv, "sp", 6)
    near = merge(near, keep_ctx)
    near_down = xor_move(near, "sp", 6)
    near_up = xor_move(near, "sp", 2)
    across = xor_move(down, "sp", 2)
    near_across = xor_move(near_down, "sp", 2)
    (own,) = attend([(keep_q, None, [0])], [keep_kv], offset)
    near_q = ready(near_q)
    own, other = attend([(keep_q, own, [1]), (near_q, None, [0, 1])], [keep_kv, near], offset)
    own, other = attend([(keep_q, own, [0, 1]), (near_q, other, [0, 1])], [up, down], offset)
    own, other = attend(
        [(keep_q, own, [0]), (near_q, other, [0, 1])], [near_up, near_down], offset
    )
    own, other = attend([(keep_q, own, [0]), (near_q, other, [0])], [across], offset)
    ((other,),) = attend([(near_q, other, [0])], [near_across], offset, True)
    ((own,),) = attend([(keep_q, own, [0, 1])], [near_down, near_across], offset, True)
    sent = [cross_move(other[j], j) for j in range(head_split)]
    parts = [own[0]] + [xor_move(own[j], "tp", j) for j in range(1, head_split)] + sent
    width = q_heads * CHANNEL_SPAN
    return kernel_call(
        output_body,
        jax.ShapeDtypeStruct(latent.shape, jnp.bfloat16),
        3 + len(parts),
        2 * own_rows * depth * width * head_split,
        [pltpu.VMEM((width * head_split, own_rows), jnp.bfloat16)],
    )(latent, modulation, output_weight, *parts)


def suits(mesh, latent, context, query_weight, key_weight):
    seq_split, head_split = mesh.shape["sp"], mesh.shape["tp"]
    own_rows = latent.shape[0] // (seq_split * head_split)
    ctx_rows = context.shape[0] // seq_split
    kv_heads = key_weight.shape[1] // CHANNEL_SPAN // head_split
    return (
        seq_split == 8
        and head_split == 4
        and own_rows == 2 * CHANNEL_SPAN
        and ctx_rows == CHANNEL_SPAN
        and kv_heads == 2
        and query_weight.shape[1] == 2 * key_weight.shape[1]
    )


def solution(mesh):
    in_specs = (
        P(("sp", "tp"), None),
        P("sp", None),
        P(),
        P(),
        P(),
        P("sp", "tp"),
        P("sp", "tp"),
        P("sp", "tp"),
        P(None, "tp"),
        P(None, "tp"),
        P(None, "tp"),
        P(),
        P(),
        P(),
    )
    out_specs = P(("sp", "tp"), None)

    def program(*args):
        fast = suits(mesh, args[0], args[1], args[8], args[9])
        step = jax.shard_map(
            fast_device if fast else general_device,
            mesh=mesh,
            in_specs=in_specs,
            out_specs=out_specs,
            check_vma=False,
        )
        return step(*args)

    return program
```

```python
import math

import jax
import jax.numpy as jnp
from jax import lax
from jax.experimental import pallas as pl
from jax.experimental.pallas import tpu as pltpu
from jax.sharding import PartitionSpec as P


CHANNEL_SPAN = 64
GRID_W = 64


epsilon = 1e-06
rope_base = 10000.0


def modulate(tok_rows, norm_gain, shift_row, scale_row):
    wide = tok_rows.astype(jnp.float32)
    normed = wide * lax.rsqrt(jnp.mean(wide * wide, axis=-1, keepdims=True) + epsilon)
    return (normed * norm_gain * (1.0 + scale_row) + shift_row).astype(jnp.bfloat16)


def headnorm(raw, gain, heads):
    field = raw.reshape(raw.shape[0], heads, -1)
    return field * lax.rsqrt(jnp.mean(field * field, axis=-1, keepdims=True) + epsilon) * gain


def rotate(field, places):
    count = field.shape[0]
    heads = field.shape[1]
    quarter = field.shape[2] // 4
    grid_row = (places // GRID_W).astype(jnp.float32)
    grid_col = (places % GRID_W).astype(jnp.float32)
    inverse = rope_base ** (-jnp.arange(quarter, dtype=jnp.float32) / quarter)
    angles = jnp.stack([grid_row[:, None] * inverse, grid_col[:, None] * inverse], axis=1)[:, None]
    cosine = jnp.cos(angles)
    sine = jnp.sin(angles)
    matcher_content_couples = field.reshape(count, heads, 2, 2, quarter)
    first = matcher_content_couples[:, :, :, 0]
    second = matcher_content_couples[:, :, :, 1]
    turned = jnp.stack([first * cosine - second * sine, second * cosine + first * sine], axis=3)
    return turned.reshape(count, heads, 4 * quarter)


def process_probe_group(
    accumulator_carry, probe_entries, matcher_content_couples, similarity_offset
):
    row_peak, row_total, weighted = accumulator_carry
    kv_heads = probe_entries.shape[1]
    head_size = probe_entries.shape[3]
    pair_width = kv_heads * head_size
    matcher_pieces = matcher_content_couples[:, :pair_width].reshape(
        matcher_content_couples.shape[0], kv_heads, head_size
    )
    value_rows = matcher_content_couples[:, pair_width:].reshape(
        matcher_content_couples.shape[0], kv_heads, head_size
    )
    similarity_matrix = (
        jnp.einsum(
            "dmvk,hmk->dmvh", probe_entries, matcher_pieces, preferred_element_type=jnp.float32
        )
        * head_size ** (-0.5)
        + similarity_offset
    )
    new_peak = jnp.maximum(row_peak, jnp.max(similarity_matrix, axis=-1))
    shares = jnp.exp(similarity_matrix - new_peak[..., None])
    shrink = jnp.exp(row_peak - new_peak)
    row_total = row_total * shrink + jnp.sum(shares, axis=-1)
    weighted = weighted * shrink[..., None] + jnp.einsum(
        "qkgn,nkd->qkgd",
        shares.astype(jnp.bfloat16),
        value_rows,
        preferred_element_type=jnp.float32,
    )
    return (new_peak, row_total, weighted)


def group_walker(accumulator_carry, probe_entries, matcher_content_couples, similarity_offset):
    pair_count = matcher_content_couples.shape[0]
    probe_group_total = -(-pair_count // 2048)
    while pair_count % probe_group_total:
        probe_group_total += 1
    if probe_group_total == 1:
        return process_probe_group(
            accumulator_carry, probe_entries, matcher_content_couples, similarity_offset
        )
    group_extent = pair_count // probe_group_total

    def scan_step(inner, slices):
        return (process_probe_group(inner, probe_entries, slices[0], slices[1]), None)

    result, _ = lax.scan(
        scan_step,
        accumulator_carry,
        (
            matcher_content_couples.reshape(
                probe_group_total, group_extent, matcher_content_couples.shape[1]
            ),
            similarity_offset.reshape(probe_group_total, group_extent),
        ),
    )
    return result


def general_device(
    latent,
    context,
    condition,
    context_condition,
    norm_gain,
    shift_weight,
    scale_weight,
    gate_weight,
    query_weight,
    key_weight,
    value_weight,
    query_gain,
    key_gain,
    output_weight,
):
    head_split = lax.axis_size("tp")
    seq_index = lax.axis_index("sp")
    head_index = lax.axis_index("tp")
    row_slab = shift_weight.shape[0]
    columns = shift_weight.shape[1]
    conditions = jnp.stack([condition, context_condition])
    activated = jax.nn.silu(
        lax.dynamic_slice_in_dim(conditions, seq_index * row_slab, row_slab, 1)
    ).astype(jnp.bfloat16)
    part_shift = jnp.dot(activated, shift_weight, preferred_element_type=jnp.float32)
    part_scale = jnp.dot(activated, scale_weight, preferred_element_type=jnp.float32)
    part_gate = jnp.dot(activated, gate_weight, preferred_element_type=jnp.float32)

    def widen(member):
        blank = jnp.zeros((2, columns * head_split), jnp.float32)
        return lax.dynamic_update_slice_in_dim(blank, member, head_index * columns, 1)

    shifts, scales, gates = lax.psum(
        (widen(part_shift), widen(part_scale), widen(part_gate)), ("sp", "tp")
    )
    own_rows = latent.shape[0]
    tok_count = own_rows * head_split
    ctx_rows = context.shape[0]
    hidden = modulate(latent, norm_gain, shifts[0], scales[0])
    context_hidden = modulate(context, norm_gain, shifts[1], scales[1])
    q_heads = query_weight.shape[1] // CHANNEL_SPAN
    kv_heads = key_weight.shape[1] // CHANNEL_SPAN
    group_size = q_heads // kv_heads
    q_width = q_heads * CHANNEL_SPAN
    kv_width = kv_heads * CHANNEL_SPAN
    joined_weight = jnp.concatenate([query_weight, key_weight, value_weight], axis=1)
    projected = jnp.dot(
        lax.all_gather(hidden, "tp", axis=0, tiled=True),
        joined_weight,
        preferred_element_type=jnp.float32,
    )
    places = seq_index * tok_count + jnp.arange(tok_count, dtype=jnp.int32)
    probe_entries = rotate(headnorm(projected[:, :q_width], query_gain, q_heads), places).astype(
        jnp.bfloat16
    )
    probe_entries = probe_entries.reshape(tok_count, kv_heads, group_size, CHANNEL_SPAN)
    latent_keys = rotate(
        headnorm(projected[:, q_width : q_width + kv_width], key_gain, kv_heads), places
    ).astype(jnp.bfloat16)
    latent_values = projected[:, q_width + kv_width :].astype(jnp.bfloat16)
    own_pairs = jnp.concatenate([latent_keys.reshape(tok_count, kv_width), latent_values], axis=1)
    ctx_projected = jnp.dot(
        context_hidden, joined_weight[:, q_width:], preferred_element_type=jnp.float32
    )
    ctx_keys = (
        headnorm(ctx_projected[:, :kv_width], key_gain, kv_heads)
        .astype(jnp.bfloat16)
        .reshape(ctx_rows, kv_width)
    )
    ctx_pairs = jnp.concatenate(
        [ctx_keys, ctx_projected[:, kv_width:].astype(jnp.bfloat16)], axis=1
    )
    prefix_mapped = math.log(tok_count / (2.0 * ctx_rows))
    stat_shape = (tok_count, kv_heads, group_size)
    start_state = (
        jnp.full(stat_shape, -jnp.inf, jnp.float32),
        jnp.zeros(stat_shape, jnp.float32),
        jnp.zeros(stat_shape + (CHANNEL_SPAN,), jnp.float32),
    )
    ctx_whole = lax.all_gather(ctx_pairs, "sp", axis=0, tiled=True)
    ctx_state = group_walker(
        start_state,
        probe_entries,
        ctx_whole,
        jnp.full((ctx_whole.shape[0],), prefix_mapped, jnp.float32),
    )
    key_piece = lax.all_gather(own_pairs, "sp", axis=0, tiled=True)
    final_state = group_walker(
        ctx_state, probe_entries, key_piece, jnp.zeros((key_piece.shape[0],), jnp.float32)
    )
    _, row_total, weighted = final_state
    attended = (weighted / row_total[..., None]).astype(jnp.bfloat16).reshape(tok_count, q_width)
    branch = jnp.dot(
        lax.all_to_all(attended, "tp", split_axis=0, concat_axis=1, tiled=True),
        output_weight,
        preferred_element_type=jnp.float32,
    )
    return (latent.astype(jnp.float32) + gates[0] * branch).astype(jnp.bfloat16)


LOG2E = math.log2(math.e)


def whole_spec():
    return pl.BlockSpec(memory_space=pltpu.VMEM)


def kernel_call(body, out_shape, count, flops, scratch=()):
    return pl.pallas_call(
        body,
        out_shape=out_shape,
        in_specs=[whole_spec()] * count,
        out_specs=jax.tree.map(lambda unused: whole_spec(), out_shape),
        scratch_shapes=list(scratch),
        cost_estimate=pl.CostEstimate(flops=flops, transcendentals=0, bytes_accessed=0),
        compiler_params=pltpu.CompilerParams(vmem_limit_bytes=MODEST),
    )


ROOMY = 60 * 1024 * 1024
MODEST = 32 * 1024 * 1024


def hbm_spec():
    return pl.BlockSpec(memory_space=pltpu.HBM)


def start_loads(pairs, sems):
    copies = []
    for i, (source, target) in enumerate(pairs):
        copies.append(pltpu.make_async_copy(source, target, sems.at[i]))
        copies[-1].start()
    return copies


def opening_body(first_hbm, second_hbm, shift_hbm, scale_hbm, gate_hbm, out_ref, *scratch):
    first, second, *targets, sems = scratch
    row_slab = shift_hbm.shape[0]
    cut = pl.ds(pl.multiple_of(lax.axis_index("sp") * row_slab, row_slab), row_slab)
    copies = start_loads(
        [(first_hbm.at[:, cut], first), (second_hbm.at[:, cut], second)]
        + list(zip((shift_hbm, scale_hbm, gate_hbm), targets)),
        sems,
    )
    copies[0].wait()
    copies[1].wait()
    rows = lax.broadcasted_iota(jnp.int32, (16, row_slab), 0)
    pair = jnp.where(rows == 0, first[...], second[...])
    activated = (pair / (1.0 + jnp.exp(-pair))).astype(jnp.bfloat16)
    out_ref[6:8, :] = jnp.zeros((2, out_ref.shape[1]), jnp.float32)
    for i in range(3):
        copies[2 + i].wait()
        part = jnp.dot(activated, targets[i][...], preferred_element_type=jnp.float32)
        out_ref[2 * i : 2 * i + 2, :] = part[0:2]


def combine_body(one_ref, other_ref, out_ref):
    out_ref[...] = one_ref[...] + other_ref[...]


def combine(one, other, flops):
    return kernel_call(combine_body, jax.ShapeDtypeStruct(one.shape, one.dtype), 2, flops)(
        one, other
    )


def opening(first, second, *weights):
    row_slab, columns = weights[0].shape
    return pl.pallas_call(
        opening_body,
        out_shape=jax.ShapeDtypeStruct((8, columns), jnp.float32),
        in_specs=[hbm_spec()] * 5,
        out_specs=whole_spec(),
        scratch_shapes=[pltpu.VMEM((1, row_slab), jnp.float32)] * 2
        + [pltpu.VMEM((row_slab, columns), jnp.bfloat16)] * 3
        + [pltpu.SemaphoreType.DMA((5,))],
        cost_estimate=pl.CostEstimate(flops=10**8, transcendentals=0, bytes_accessed=0),
        compiler_params=pltpu.CompilerParams(vmem_limit_bytes=ROOMY),
    )(first, second, *weights)


def turn(field, cosine, sine):
    quarter = field.shape[0] // 4
    pieces = [field[i * quarter : (i + 1) * quarter] for i in range(4)]
    swapped = jnp.concatenate([pieces[1], pieces[0], pieces[3], pieces[2]], axis=0)
    return field * cosine + swapped * sine


def normed(raw, head_gain):
    return raw * lax.rsqrt(jnp.mean(raw * raw, axis=0, keepdims=True) + epsilon) * head_gain


def upright(ref):
    return jnp.broadcast_to(ref[...], (8, ref.shape[1])).T[:, 0:1]


def projection_body(
    kv_heads,
    own_ref,
    context_ref,
    key_ref,
    value_ref,
    core_ref,
    far_ref,
    both_ref,
    mod_ref,
    gain_ref,
    key_gain_ref,
    cosine_ref,
    sine_ref,
    keep_kv,
    keep_ctx,
    give_kv,
    hidden_out,
    made,
):
    span = CHANNEL_SPAN

    def vector(row):
        return jnp.concatenate([mod_ref[i, row : row + 1, :] for i in range(mod_ref.shape[0])], axis=1)

    gain = gain_ref[...]

    def hidden_of(ref, row):
        wide = ref[...].astype(jnp.float32)
        scaled = wide * lax.rsqrt(jnp.mean(wide * wide, axis=-1, keepdims=True) + epsilon)
        return (scaled * (gain * (1.0 + vector(2 + row))) + vector(row)).astype(jnp.bfloat16)

    key_gain = upright(key_gain_ref)
    blocks = (own_ref, core_ref, far_ref, both_ref)
    waiting = {}
    for j, ref in enumerate(blocks):
        hidden = hidden_of(ref, 0)
        hidden_out[j] = hidden
        rows = slice(j % 2 * span, (j % 2 + 1) * span)
        keys = jnp.dot(hidden, key_ref[...], preferred_element_type=jnp.float32).T
        values = jnp.dot(hidden, value_ref[...], preferred_element_type=jnp.float32).T
        for h in range(kv_heads):
            cut = slice(h * span, (h + 1) * span)
            turned = turn(normed(keys[cut], key_gain), cosine_ref[j], sine_ref[j])
            if j % 2:
                pair = jnp.concatenate([waiting[h], turned], axis=0)
                made[h, j // 2] = pair.T.astype(jnp.bfloat16)
            waiting[h] = turned
            made[h, len(blocks) // 2 + j // 2, rows, :] = values[cut].astype(jnp.bfloat16)
    hidden = hidden_of(context_ref, 1)
    keys = jnp.dot(hidden, key_ref[...], preferred_element_type=jnp.float32).T
    values = jnp.dot(hidden, value_ref[...], preferred_element_type=jnp.float32).T
    for h in range(kv_heads):
        cut = slice(h * span, (h + 1) * span)
        both = jnp.concatenate([normed(keys[cut], key_gain).T, values[cut]], axis=0)
        made[h, len(blocks)] = jnp.concatenate([both, jnp.zeros_like(both)], axis=1).astype(
            jnp.bfloat16
        )
    side = lax.rem(lax.axis_index("sp"), kv_heads)
    for i in range(give_kv.shape[0]):
        give_kv[i] = made[1 - side, i]
    for i in range(keep_kv.shape[0]):
        keep_kv[i] = made[side, i]
    keep_ctx[...] = made[side, len(blocks)]


def probe_body(
    kv_heads, hidden_ref, query_ref, query_gain_ref, cosine_ref, sine_ref, keep_q, give_q, made
):
    span = CHANNEL_SPAN
    heads = query_ref.shape[1] // span
    group = heads // kv_heads
    count = hidden_ref.shape[0]
    query_gain = upright(query_gain_ref)
    for j in range(count):
        rows = slice(j % 2 * span, (j % 2 + 1) * span)
        queries = jnp.dot(hidden_ref[j], query_ref[...], preferred_element_type=jnp.float32).T
        for h in range(heads):
            raw = queries[h * span : (h + 1) * span]
            turned = turn(normed(raw, query_gain), cosine_ref[j], sine_ref[j])
            kv, g = h // group, h % group
            made[kv, g * count // 2 + j // 2, rows, :] = turned.astype(jnp.bfloat16)
    side = lax.rem(lax.axis_index("sp"), kv_heads)
    q_tiles = give_q.shape[0]
    for i in range(q_tiles):
        give_q[i] = made[1 - side, i]
        keep_q[i], keep_q[q_tiles + i] = scaled_halves(made[side, i])


def merge_body(near_ref, ctx_ref, out_ref):
    last = near_ref.shape[0] - 1
    span = ctx_ref.shape[1] // 2
    for i in range(last):
        out_ref[i] = near_ref[i]
    out_ref[last] = jnp.concatenate([near_ref[last, :, 0:span], ctx_ref[:, 0:span]], axis=1)


def merge(near, ctx):
    return kernel_call(merge_body, jax.ShapeDtypeStruct(near.shape, near.dtype), 2, 10**6)(near, ctx)


def scaled_halves(tile):
    scale = (tile.shape[-2] // 2) ** (-0.5) * LOG2E
    wide = tile.astype(jnp.float32) * scale
    high = wide.astype(jnp.bfloat16)
    return high, (wide - high.astype(jnp.float32)).astype(jnp.bfloat16)


def ready_body(q_ref, out_ref):
    count = q_ref.shape[0]
    for i in range(count):
        out_ref[i], out_ref[count + i] = scaled_halves(q_ref[i])


def ready(probes):
    shape = jax.ShapeDtypeStruct((2 * probes.shape[0], *probes.shape[1:]), probes.dtype)
    return kernel_call(ready_body, shape, 1, 10**6)(probes)


def attention_body(plan, pieces, last, offset, *refs):
    q_refs, refs = refs[: len(plan)], refs[len(plan) :]
    kv_refs, refs = refs[:pieces], refs[pieces:]
    pairs = 2
    groups = 2
    span = q_refs[0].shape[1] // 2
    halves = (0, 1)
    states = {}
    queries = {}
    tiles = []
    for i, (q_ref, (started, wanted)) in enumerate(zip(q_refs, plan)):
        if started:
            old, refs = refs[:3], refs[3:]
        for g in range(groups):
            high, low = [
                jnp.concatenate(
                    [
                        q_ref[(level * groups + g) * pairs + p, half * span : (half + 1) * span, :]
                        for p in range(pairs)
                        for half in halves
                    ],
                    axis=1,
                )
                for level in halves
            ]
            blank = jnp.zeros_like(high)
            queries[i, g, 0] = jnp.concatenate([high, blank, low, blank], axis=0)
            queries[i, g, 1] = jnp.concatenate([blank, high, blank, low], axis=0)
            if started:
                states[i, g] = tuple(ref[g] for ref in old)
            tiles += [(i, g, place, part) for place in wanted for part in halves]
    tiles.sort(key=lambda tile: tile[2:])

    def scores(tile):
        i, g, place, part = tile
        ref = kv_refs[place]
        context = ref.shape[0] > 2 * pairs
        keys = [ref[p] for p in range(pairs)]
        if context:
            keys.append(ref[2 * pairs, 0:span, :])
        keys = jnp.concatenate(keys, axis=0)
        keys = jnp.concatenate([keys, keys], axis=1)
        found = jnp.dot(keys, queries[i, g, part], preferred_element_type=jnp.float32)
        if context:
            rows = found.shape[0] - span
            found = jnp.concatenate([found[:rows], found[rows:] + offset * LOG2E], axis=0)
        return found

    def soften(tile, found):
        place = tile[:2]
        peak = jnp.max(found, axis=0, keepdims=True)
        old = states.get(place)
        if old is not None:
            peak = jnp.maximum(peak, old[0])
        shares = jnp.exp2(found - peak)
        total = jnp.sum(shares, axis=0, keepdims=True)
        shrink = None
        if old is not None:
            shrink = jnp.exp2(old[0] - peak)
            total = total + old[1] * shrink
        states[place] = (peak, total, old[2] if old is not None else None)
        return shares.astype(jnp.bfloat16), shrink

    def gather(tile, shares, shrink):
        ref = kv_refs[tile[2]]
        rows = slice(tile[3] * span, (tile[3] + 1) * span)
        values = [ref[pairs + p, rows, :] for p in range(pairs)]
        if ref.shape[0] > 2 * pairs:
            values.append(ref[2 * pairs, span : 2 * span, rows])
        weighted = jnp.dot(
            jnp.concatenate(values, axis=1), shares, preferred_element_type=jnp.float32
        )
        peak, total, old = states[tile[:2]]
        if shrink is not None:
            weighted = weighted + old * shrink
        states[tile[:2]] = (peak, total, weighted)

    following = scores(tiles[0])
    waiting = None
    for i, tile in enumerate(tiles):
        found = following
        if i + 1 < len(tiles):
            following = scores(tiles[i + 1])
        shares, shrink = soften(tile, found)
        if waiting:
            gather(*waiting)
        waiting = (tile, shares, shrink)
    gather(*waiting)
    for (i, g), (peak, total, weighted) in states.items():
        if last:
            out_ref = refs[i]
            attended = (weighted / total).astype(jnp.bfloat16)
            own_rows = out_ref.shape[2]
            for j in range(out_ref.shape[0]):
                out_ref[j, g * span : (g + 1) * span, :] = attended[
                    :, j * own_rows : (j + 1) * own_rows
                ]
        else:
            for ref, value in zip(refs[3 * i : 3 * i + 3], (peak, total, weighted)):
                ref[g] = value


def attend(sources, pieces, offset, last=False):
    probes = [source[0] for source in sources]
    lanes = 2 * 2 * probes[0].shape[2]
    span = probes[0].shape[1] // 2
    plan = [(source[1] is not None, source[2]) for source in sources]
    keys = sum(pieces[i].shape[0] * pieces[i].shape[1] // 2 for source in sources for i in source[2])
    inputs = probes + pieces
    for source in sources:
        inputs += list(source[1] or ())
    if last:
        out = [jax.ShapeDtypeStruct((4, 2 * span, probes[0].shape[2]), jnp.bfloat16)]
    else:
        stat = jax.ShapeDtypeStruct((2, 1, lanes), jnp.float32)
        out = [stat, stat, jax.ShapeDtypeStruct((2, span, lanes), jnp.float32)]

    def body(*refs):
        attention_body(plan, len(pieces), last, offset, *refs)

    found = kernel_call(
        body, out * len(sources), len(inputs), 40 * 2 * lanes * keys * span
    )(*inputs)
    size = len(out)
    return [found[size * i : size * (i + 1)] for i in range(len(sources))]


def output_body(latent_ref, mod_ref, weight_ref, *refs):
    out_ref, lhs_ref = refs[-2:]
    parts = refs[:-2]
    head_index = lax.axis_index("tp")
    side = lax.rem(lax.axis_index("sp"), 2)
    rows = parts[0].shape[0]
    for i, ref in enumerate(parts):
        j, flip = i % (len(parts) // 2), i // (len(parts) // 2)
        place = jnp.bitwise_xor(head_index, j) * 2 + jnp.bitwise_xor(side, flip)
        lhs_ref[pl.ds(pl.multiple_of(place * rows, rows), rows), :] = ref[...]
    lhs = lhs_ref[...].T
    columns = mod_ref.shape[2]
    for i in range(mod_ref.shape[0]):
        cut = slice(i * columns, (i + 1) * columns)
        branch = jnp.dot(lhs, weight_ref[:, cut], preferred_element_type=jnp.float32)
        gate = mod_ref[i, 4:5, :]
        out_ref[:, cut] = (latent_ref[:, cut].astype(jnp.float32) + gate * branch).astype(
            jnp.bfloat16
        )


def fast_device(*args):
    return inner_device(*args)


def xor_move(member, axis, mask):
    size = lax.axis_size(axis)
    return lax.ppermute(member, axis, [(i, i ^ mask) for i in range(size)])


def cross_move(member, mask):
    seq_split, head_split = lax.axis_size("sp"), lax.axis_size("tp")
    pairs = [
        (i * head_split + j, (i ^ 1) * head_split + (j ^ mask))
        for i in range(seq_split)
        for j in range(head_split)
    ]
    return lax.ppermute(member, ("sp", "tp"), pairs)


def tables(seq_index, head_index, own_rows, head_split):
    quarter = CHANNEL_SPAN // 4
    blocks = jnp.bitwise_xor(jnp.arange(head_split, dtype=jnp.int32), head_index)
    places = (
        seq_index * own_rows * head_split
        + blocks[:, None] * own_rows
        + jnp.arange(own_rows, dtype=jnp.int32)
    )
    inverse = rope_base ** (-jnp.arange(quarter, dtype=jnp.float32) / quarter)
    grid_row = (places // GRID_W).astype(jnp.float32)[:, None, :] * inverse[:, None]
    grid_col = (places % GRID_W).astype(jnp.float32)[:, None, :] * inverse[:, None]
    row_sine, col_sine = jnp.sin(grid_row), jnp.sin(grid_col)
    row_cosine, col_cosine = jnp.cos(grid_row), jnp.cos(grid_col)
    cosine = jnp.concatenate([row_cosine, row_cosine, col_cosine, col_cosine], axis=1)
    sine = jnp.concatenate([-row_sine, row_sine, -col_sine, col_sine], axis=1)
    return cosine, sine


def inner_device(
    latent,
    context,
    condition,
    context_condition,
    norm_gain,
    shift_weight,
    scale_weight,
    gate_weight,
    query_weight,
    key_weight,
    value_weight,
    query_gain,
    key_gain,
    output_weight,
):
    head_split = lax.axis_size("tp")
    seq_split = lax.axis_size("sp")
    seq_index = lax.axis_index("sp")
    head_index = lax.axis_index("tp")
    own_rows, depth = latent.shape
    ctx_rows = context.shape[0]
    tok_count = own_rows * head_split
    q_heads = query_weight.shape[1] // CHANNEL_SPAN
    kv_heads = key_weight.shape[1] // CHANNEL_SPAN

    part = opening(
        condition.reshape(1, depth),
        context_condition.reshape(1, depth),
        shift_weight,
        scale_weight,
        gate_weight,
    )
    far = xor_move(latent, "tp", 2)
    near = xor_move(latent, "tp", 1)
    mask = seq_split // 2
    while mask:
        other = xor_move(part, "sp", mask)
        part = combine(part, other, 10**11 if 2 * mask == seq_split else 10**6)
        mask //= 2
    both = xor_move(far, "tp", 1)
    modulation = lax.all_gather(part, "tp", axis=0, tiled=False)
    cosine, sine = tables(seq_index, head_index, own_rows, head_split)
    q_tiles = q_heads // kv_heads * head_split // 2
    kv_tiles = head_split
    tile = (own_rows, own_rows)
    keep_kv, keep_ctx, give_kv, hidden = kernel_call(
        lambda *refs: projection_body(kv_heads, *refs),
        [
            jax.ShapeDtypeStruct(shape, jnp.bfloat16)
            for shape in (
                (kv_tiles, *tile),
                tile,
                (kv_tiles + 1, *tile),
                (head_split, own_rows, depth),
            )
        ],
        12,
        8 * tok_count * depth * kv_heads * CHANNEL_SPAN,
        [pltpu.VMEM((kv_heads, kv_tiles + 1, *tile), jnp.bfloat16)],
    )(
        latent,
        context,
        key_weight,
        value_weight,
        near,
        far,
        both,
        modulation,
        norm_gain.reshape(1, depth),
        key_gain.reshape(1, CHANNEL_SPAN),
        cosine,
        sine,
    )
    keep_q, give_q = kernel_call(
        lambda *refs: probe_body(kv_heads, *refs),
        [jax.ShapeDtypeStruct((count, *tile), jnp.bfloat16) for count in (2 * q_tiles, q_tiles)],
        5,
        4 * tok_count * depth * q_heads * CHANNEL_SPAN,
        [pltpu.VMEM((kv_heads, q_tiles, *tile), jnp.bfloat16)],
    )(hidden, query_weight, query_gain.reshape(1, CHANNEL_SPAN), cosine, sine)
    offset = math.log(tok_count / (2.0 * ctx_rows))
    near = xor_move(give_kv, "sp", 1)
    near_q = xor_move(give_q, "sp", 1)
    up = xor_move(keep_kv, "sp", 2)
    down = xor_move(keep_kv, "sp", 6)
    near = merge(near, keep_ctx)
    near_down = xor_move(near, "sp", 6)
    near_up = xor_move(near, "sp", 2)
    across = xor_move(down, "sp", 2)
    near_across = xor_move(near_down, "sp", 2)
    (own,) = attend([(keep_q, None, [0])], [keep_kv], offset)
    near_q = ready(near_q)
    own, other = attend([(keep_q, own, [1]), (near_q, None, [0, 1])], [keep_kv, near], offset)
    own, other = attend([(keep_q, own, [0, 1]), (near_q, other, [0, 1])], [up, down], offset)
    own, other = attend(
        [(keep_q, own, [0]), (near_q, other, [0, 1])], [near_up, near_down], offset
    )
    own, other = attend([(keep_q, own, [0]), (near_q, other, [0])], [across], offset)
    ((other,),) = attend([(near_q, other, [0])], [near_across], offset, True)
    ((own,),) = attend([(keep_q, own, [0, 1])], [near_down, near_across], offset, True)
    sent = [cross_move(other[j], j) for j in range(head_split)]
    parts = [own[0]] + [xor_move(own[j], "tp", j) for j in range(1, head_split)] + sent
    width = q_heads * CHANNEL_SPAN
    return kernel_call(
        output_body,
        jax.ShapeDtypeStruct(latent.shape, jnp.bfloat16),
        3 + len(parts),
        2 * own_rows * depth * width * head_split,
        [pltpu.VMEM((width * head_split, own_rows), jnp.bfloat16)],
    )(latent, modulation, output_weight, *parts)


def suits(mesh, latent, context, query_weight, key_weight):
    seq_split, head_split = mesh.shape["sp"], mesh.shape["tp"]
    own_rows = latent.shape[0] // (seq_split * head_split)
    ctx_rows = context.shape[0] // seq_split
    kv_heads = key_weight.shape[1] // CHANNEL_SPAN // head_split
    return (
        seq_split == 8
        and head_split == 4
        and own_rows == 2 * CHANNEL_SPAN
        and ctx_rows == CHANNEL_SPAN
        and kv_heads == 2
        and query_weight.shape[1] == 2 * key_weight.shape[1]
    )


def solution(mesh):
    in_specs = (
        P(("sp", "tp"), None),
        P("sp", None),
        P(),
        P(),
        P(),
        P("sp", "tp"),
        P("sp", "tp"),
        P("sp", "tp"),
        P(None, "tp"),
        P(None, "tp"),
        P(None, "tp"),
        P(),
        P(),
        P(),
    )
    out_specs = P(("sp", "tp"), None)

    def program(*args):
        fast = suits(mesh, args[0], args[1], args[8], args[9])
        step = jax.shard_map(
            fast_device if fast else general_device,
            mesh=mesh,
            in_specs=in_specs,
            out_specs=out_specs,
            check_vma=False,
        )
        return step(*args)

    return program
```

```python
import math

import jax
import jax.numpy as jnp
from jax import lax
from jax.experimental import pallas as pl
from jax.experimental.pallas import tpu as pltpu
from jax.sharding import PartitionSpec as P


CHANNEL_SPAN = 64
GRID_W = 64


epsilon = 1e-06
rope_base = 10000.0


def modulate(tok_rows, norm_gain, shift_row, scale_row):
    wide = tok_rows.astype(jnp.float32)
    normed = wide * lax.rsqrt(jnp.mean(wide * wide, axis=-1, keepdims=True) + epsilon)
    return (normed * norm_gain * (1.0 + scale_row) + shift_row).astype(jnp.bfloat16)


def headnorm(raw, gain, heads):
    field = raw.reshape(raw.shape[0], heads, -1)
    return field * lax.rsqrt(jnp.mean(field * field, axis=-1, keepdims=True) + epsilon) * gain


def rotate(field, places):
    count = field.shape[0]
    heads = field.shape[1]
    quarter = field.shape[2] // 4
    grid_row = (places // GRID_W).astype(jnp.float32)
    grid_col = (places % GRID_W).astype(jnp.float32)
    inverse = rope_base ** (-jnp.arange(quarter, dtype=jnp.float32) / quarter)
    angles = jnp.stack([grid_row[:, None] * inverse, grid_col[:, None] * inverse], axis=1)[:, None]
    cosine = jnp.cos(angles)
    sine = jnp.sin(angles)
    matcher_content_couples = field.reshape(count, heads, 2, 2, quarter)
    first = matcher_content_couples[:, :, :, 0]
    second = matcher_content_couples[:, :, :, 1]
    turned = jnp.stack([first * cosine - second * sine, second * cosine + first * sine], axis=3)
    return turned.reshape(count, heads, 4 * quarter)


def process_probe_group(
    accumulator_carry, probe_entries, matcher_content_couples, similarity_offset
):
    row_peak, row_total, weighted = accumulator_carry
    kv_heads = probe_entries.shape[1]
    head_size = probe_entries.shape[3]
    pair_width = kv_heads * head_size
    matcher_pieces = matcher_content_couples[:, :pair_width].reshape(
        matcher_content_couples.shape[0], kv_heads, head_size
    )
    value_rows = matcher_content_couples[:, pair_width:].reshape(
        matcher_content_couples.shape[0], kv_heads, head_size
    )
    similarity_matrix = (
        jnp.einsum(
            "dmvk,hmk->dmvh", probe_entries, matcher_pieces, preferred_element_type=jnp.float32
        )
        * head_size ** (-0.5)
        + similarity_offset
    )
    new_peak = jnp.maximum(row_peak, jnp.max(similarity_matrix, axis=-1))
    shares = jnp.exp(similarity_matrix - new_peak[..., None])
    shrink = jnp.exp(row_peak - new_peak)
    row_total = row_total * shrink + jnp.sum(shares, axis=-1)
    weighted = weighted * shrink[..., None] + jnp.einsum(
        "qkgn,nkd->qkgd",
        shares.astype(jnp.bfloat16),
        value_rows,
        preferred_element_type=jnp.float32,
    )
    return (new_peak, row_total, weighted)


def group_walker(accumulator_carry, probe_entries, matcher_content_couples, similarity_offset):
    pair_count = matcher_content_couples.shape[0]
    probe_group_total = -(-pair_count // 2048)
    while pair_count % probe_group_total:
        probe_group_total += 1
    if probe_group_total == 1:
        return process_probe_group(
            accumulator_carry, probe_entries, matcher_content_couples, similarity_offset
        )
    group_extent = pair_count // probe_group_total

    def scan_step(inner, slices):
        return (process_probe_group(inner, probe_entries, slices[0], slices[1]), None)

    result, _ = lax.scan(
        scan_step,
        accumulator_carry,
        (
            matcher_content_couples.reshape(
                probe_group_total, group_extent, matcher_content_couples.shape[1]
            ),
            similarity_offset.reshape(probe_group_total, group_extent),
        ),
    )
    return result


def general_device(
    latent,
    context,
    condition,
    context_condition,
    norm_gain,
    shift_weight,
    scale_weight,
    gate_weight,
    query_weight,
    key_weight,
    value_weight,
    query_gain,
    key_gain,
    output_weight,
):
    head_split = lax.axis_size("tp")
    seq_index = lax.axis_index("sp")
    head_index = lax.axis_index("tp")
    row_slab = shift_weight.shape[0]
    columns = shift_weight.shape[1]
    conditions = jnp.stack([condition, context_condition])
    activated = jax.nn.silu(
        lax.dynamic_slice_in_dim(conditions, seq_index * row_slab, row_slab, 1)
    ).astype(jnp.bfloat16)
    part_shift = jnp.dot(activated, shift_weight, preferred_element_type=jnp.float32)
    part_scale = jnp.dot(activated, scale_weight, preferred_element_type=jnp.float32)
    part_gate = jnp.dot(activated, gate_weight, preferred_element_type=jnp.float32)

    def widen(member):
        blank = jnp.zeros((2, columns * head_split), jnp.float32)
        return lax.dynamic_update_slice_in_dim(blank, member, head_index * columns, 1)

    shifts, scales, gates = lax.psum(
        (widen(part_shift), widen(part_scale), widen(part_gate)), ("sp", "tp")
    )
    own_rows = latent.shape[0]
    tok_count = own_rows * head_split
    ctx_rows = context.shape[0]
    hidden = modulate(latent, norm_gain, shifts[0], scales[0])
    context_hidden = modulate(context, norm_gain, shifts[1], scales[1])
    q_heads = query_weight.shape[1] // CHANNEL_SPAN
    kv_heads = key_weight.shape[1] // CHANNEL_SPAN
    group_size = q_heads // kv_heads
    q_width = q_heads * CHANNEL_SPAN
    kv_width = kv_heads * CHANNEL_SPAN
    joined_weight = jnp.concatenate([query_weight, key_weight, value_weight], axis=1)
    projected = jnp.dot(
        lax.all_gather(hidden, "tp", axis=0, tiled=True),
        joined_weight,
        preferred_element_type=jnp.float32,
    )
    places = seq_index * tok_count + jnp.arange(tok_count, dtype=jnp.int32)
    probe_entries = rotate(headnorm(projected[:, :q_width], query_gain, q_heads), places).astype(
        jnp.bfloat16
    )
    probe_entries = probe_entries.reshape(tok_count, kv_heads, group_size, CHANNEL_SPAN)
    latent_keys = rotate(
        headnorm(projected[:, q_width : q_width + kv_width], key_gain, kv_heads), places
    ).astype(jnp.bfloat16)
    latent_values = projected[:, q_width + kv_width :].astype(jnp.bfloat16)
    own_pairs = jnp.concatenate([latent_keys.reshape(tok_count, kv_width), latent_values], axis=1)
    ctx_projected = jnp.dot(
        context_hidden, joined_weight[:, q_width:], preferred_element_type=jnp.float32
    )
    ctx_keys = (
        headnorm(ctx_projected[:, :kv_width], key_gain, kv_heads)
        .astype(jnp.bfloat16)
        .reshape(ctx_rows, kv_width)
    )
    ctx_pairs = jnp.concatenate(
        [ctx_keys, ctx_projected[:, kv_width:].astype(jnp.bfloat16)], axis=1
    )
    prefix_mapped = math.log(tok_count / (2.0 * ctx_rows))
    stat_shape = (tok_count, kv_heads, group_size)
    start_state = (
        jnp.full(stat_shape, -jnp.inf, jnp.float32),
        jnp.zeros(stat_shape, jnp.float32),
        jnp.zeros(stat_shape + (CHANNEL_SPAN,), jnp.float32),
    )
    ctx_whole = lax.all_gather(ctx_pairs, "sp", axis=0, tiled=True)
    ctx_state = group_walker(
        start_state,
        probe_entries,
        ctx_whole,
        jnp.full((ctx_whole.shape[0],), prefix_mapped, jnp.float32),
    )
    key_piece = lax.all_gather(own_pairs, "sp", axis=0, tiled=True)
    final_state = group_walker(
        ctx_state, probe_entries, key_piece, jnp.zeros((key_piece.shape[0],), jnp.float32)
    )
    _, row_total, weighted = final_state
    attended = (weighted / row_total[..., None]).astype(jnp.bfloat16).reshape(tok_count, q_width)
    branch = jnp.dot(
        lax.all_to_all(attended, "tp", split_axis=0, concat_axis=1, tiled=True),
        output_weight,
        preferred_element_type=jnp.float32,
    )
    return (latent.astype(jnp.float32) + gates[0] * branch).astype(jnp.bfloat16)


LOG2E = math.log2(math.e)


def whole_spec():
    return pl.BlockSpec(memory_space=pltpu.VMEM)


def kernel_call(body, out_shape, count, flops, scratch=()):
    return pl.pallas_call(
        body,
        out_shape=out_shape,
        in_specs=[whole_spec()] * count,
        out_specs=jax.tree.map(lambda unused: whole_spec(), out_shape),
        scratch_shapes=list(scratch),
        cost_estimate=pl.CostEstimate(flops=flops, transcendentals=0, bytes_accessed=0),
        compiler_params=pltpu.CompilerParams(vmem_limit_bytes=MODEST),
    )


ROOMY = 60 * 1024 * 1024
MODEST = 32 * 1024 * 1024


def hbm_spec():
    return pl.BlockSpec(memory_space=pltpu.HBM)


def start_loads(pairs, sems):
    copies = []
    for i, (source, target) in enumerate(pairs):
        copies.append(pltpu.make_async_copy(source, target, sems.at[i]))
        copies[-1].start()
    return copies


def opening_body(first_hbm, second_hbm, shift_hbm, scale_hbm, gate_hbm, out_ref, *scratch):
    first, second, *targets, sems = scratch
    row_slab = shift_hbm.shape[0]
    cut = pl.ds(pl.multiple_of(lax.axis_index("sp") * row_slab, row_slab), row_slab)
    copies = start_loads(
        [(first_hbm.at[:, cut], first), (second_hbm.at[:, cut], second)]
        + list(zip((shift_hbm, scale_hbm, gate_hbm), targets)),
        sems,
    )
    copies[0].wait()
    copies[1].wait()
    rows = lax.broadcasted_iota(jnp.int32, (16, row_slab), 0)
    pair = jnp.where(rows == 0, first[...], second[...])
    activated = (pair / (1.0 + jnp.exp(-pair))).astype(jnp.bfloat16)
    out_ref[6:8, :] = jnp.zeros((2, out_ref.shape[1]), jnp.float32)
    for i in range(3):
        copies[2 + i].wait()
        part = jnp.dot(activated, targets[i][...], preferred_element_type=jnp.float32)
        out_ref[2 * i : 2 * i + 2, :] = part[0:2]


def combine_body(one_ref, other_ref, out_ref):
    out_ref[...] = one_ref[...] + other_ref[...]


def combine(one, other, flops):
    return kernel_call(combine_body, jax.ShapeDtypeStruct(one.shape, one.dtype), 2, flops)(
        one, other
    )


def stash_body(source, target, sem):
    copy = pltpu.make_async_copy(source, target, sem)
    copy.start()
    copy.wait()


def stash(member):
    return pl.pallas_call(
        stash_body,
        out_shape=jax.ShapeDtypeStruct(member.shape, member.dtype),
        in_specs=[hbm_spec()],
        out_specs=whole_spec(),
        scratch_shapes=[pltpu.SemaphoreType.DMA],
        cost_estimate=pl.CostEstimate(flops=10**6, transcendentals=0, bytes_accessed=0),
        compiler_params=pltpu.CompilerParams(vmem_limit_bytes=MODEST),
    )(member)


def opening(first, second, *weights):
    row_slab, columns = weights[0].shape
    return pl.pallas_call(
        opening_body,
        out_shape=jax.ShapeDtypeStruct((8, columns), jnp.float32),
        in_specs=[hbm_spec()] * 5,
        out_specs=whole_spec(),
        scratch_shapes=[pltpu.VMEM((1, row_slab), jnp.float32)] * 2
        + [pltpu.VMEM((row_slab, columns), jnp.bfloat16)] * 3
        + [pltpu.SemaphoreType.DMA((5,))],
        cost_estimate=pl.CostEstimate(flops=10**8, transcendentals=0, bytes_accessed=0),
        compiler_params=pltpu.CompilerParams(vmem_limit_bytes=ROOMY),
    )(first, second, *weights)


def turn(field, cosine, sine):
    quarter = field.shape[0] // 4
    pieces = [field[i * quarter : (i + 1) * quarter] for i in range(4)]
    swapped = jnp.concatenate([pieces[1], pieces[0], pieces[3], pieces[2]], axis=0)
    return field * cosine + swapped * sine


def normed(raw, head_gain):
    return raw * lax.rsqrt(jnp.mean(raw * raw, axis=0, keepdims=True) + epsilon) * head_gain


def upright(ref):
    return jnp.broadcast_to(ref[...], (8, ref.shape[1])).T[:, 0:1]


def projection_body(
    kv_heads,
    own_ref,
    context_ref,
    key_ref,
    value_ref,
    core_ref,
    far_ref,
    both_ref,
    mod_ref,
    gain_ref,
    key_gain_ref,
    cosine_ref,
    sine_ref,
    keep_kv,
    keep_ctx,
    give_kv,
    hidden_out,
    made,
):
    span = CHANNEL_SPAN

    def vector(row):
        return jnp.concatenate([mod_ref[i, row : row + 1, :] for i in range(mod_ref.shape[0])], axis=1)

    gain = gain_ref[...]

    def hidden_of(ref, row):
        wide = ref[...].astype(jnp.float32)
        scaled = wide * lax.rsqrt(jnp.mean(wide * wide, axis=-1, keepdims=True) + epsilon)
        return (scaled * (gain * (1.0 + vector(2 + row))) + vector(row)).astype(jnp.bfloat16)

    key_gain = upright(key_gain_ref)
    blocks = (own_ref, core_ref, far_ref, both_ref)
    waiting = {}
    for j, ref in enumerate(blocks):
        hidden = hidden_of(ref, 0)
        hidden_out[j] = hidden
        rows = slice(j % 2 * span, (j % 2 + 1) * span)
        keys = jnp.dot(hidden, key_ref[...], preferred_element_type=jnp.float32).T
        values = jnp.dot(hidden, value_ref[...], preferred_element_type=jnp.float32).T
        for h in range(kv_heads):
            cut = slice(h * span, (h + 1) * span)
            turned = turn(normed(keys[cut], key_gain), cosine_ref[j], sine_ref[j])
            if j % 2:
                pair = jnp.concatenate([waiting[h], turned], axis=0)
                made[h, j // 2] = pair.T.astype(jnp.bfloat16)
            waiting[h] = turned
            made[h, len(blocks) // 2 + j // 2, rows, :] = values[cut].astype(jnp.bfloat16)
    hidden = hidden_of(context_ref, 1)
    keys = jnp.dot(hidden, key_ref[...], preferred_element_type=jnp.float32).T
    values = jnp.dot(hidden, value_ref[...], preferred_element_type=jnp.float32).T
    for h in range(kv_heads):
        cut = slice(h * span, (h + 1) * span)
        both = jnp.concatenate([normed(keys[cut], key_gain).T, values[cut]], axis=0)
        made[h, len(blocks)] = jnp.concatenate([both, jnp.zeros_like(both)], axis=1).astype(
            jnp.bfloat16
        )
    side = lax.rem(lax.axis_index("sp"), kv_heads)
    for i in range(give_kv.shape[0]):
        give_kv[i] = made[1 - side, i]
    for i in range(keep_kv.shape[0]):
        keep_kv[i] = made[side, i]
    keep_ctx[...] = made[side, len(blocks)]


def probe_body(
    kv_heads, hidden_ref, query_ref, query_gain_ref, cosine_ref, sine_ref, keep_q, give_q, made
):
    span = CHANNEL_SPAN
    heads = query_ref.shape[1] // span
    group = heads // kv_heads
    count = hidden_ref.shape[0]
    query_gain = upright(query_gain_ref)
    for j in range(count):
        rows = slice(j % 2 * span, (j % 2 + 1) * span)
        queries = jnp.dot(hidden_ref[j], query_ref[...], preferred_element_type=jnp.float32).T
        for h in range(heads):
            raw = queries[h * span : (h + 1) * span]
            turned = turn(normed(raw, query_gain), cosine_ref[j], sine_ref[j])
            kv, g = h // group, h % group
            made[kv, g * count // 2 + j // 2, rows, :] = turned.astype(jnp.bfloat16)
    side = lax.rem(lax.axis_index("sp"), kv_heads)
    q_tiles = give_q.shape[0]
    for i in range(q_tiles):
        give_q[i] = made[1 - side, i]
        keep_q[i], keep_q[q_tiles + i] = scaled_halves(made[side, i])


def merge_body(near_ref, ctx_ref, out_ref):
    last = near_ref.shape[0] - 1
    span = ctx_ref.shape[1] // 2
    for i in range(last):
        out_ref[i] = near_ref[i]
    out_ref[last] = jnp.concatenate([near_ref[last, :, 0:span], ctx_ref[:, 0:span]], axis=1)


def merge(near, ctx):
    return kernel_call(merge_body, jax.ShapeDtypeStruct(near.shape, near.dtype), 2, 10**6)(near, ctx)


def scaled_halves(tile):
    scale = (tile.shape[-2] // 2) ** (-0.5) * LOG2E
    wide = tile.astype(jnp.float32) * scale
    high = wide.astype(jnp.bfloat16)
    return high, (wide - high.astype(jnp.float32)).astype(jnp.bfloat16)


def ready_body(q_ref, out_ref):
    count = q_ref.shape[0]
    for i in range(count):
        out_ref[i], out_ref[count + i] = scaled_halves(q_ref[i])


def ready(probes):
    shape = jax.ShapeDtypeStruct((2 * probes.shape[0], *probes.shape[1:]), probes.dtype)
    return kernel_call(ready_body, shape, 1, 10**6)(probes)


def attention_body(plan, pieces, last, offset, *refs):
    q_refs, refs = refs[: len(plan)], refs[len(plan) :]
    kv_refs, refs = refs[:pieces], refs[pieces:]
    pairs = 2
    groups = 2
    span = q_refs[0].shape[1] // 2
    halves = (0, 1)
    states = {}
    queries = {}
    tiles = []
    for i, (q_ref, (started, wanted)) in enumerate(zip(q_refs, plan)):
        if started:
            old, refs = refs[:3], refs[3:]
        for g in range(groups):
            high, low = [
                jnp.concatenate(
                    [
                        q_ref[(level * groups + g) * pairs + p, half * span : (half + 1) * span, :]
                        for p in range(pairs)
                        for half in halves
                    ],
                    axis=1,
                )
                for level in halves
            ]
            blank = jnp.zeros_like(high)
            queries[i, g, 0] = jnp.concatenate([high, blank, low, blank], axis=0)
            queries[i, g, 1] = jnp.concatenate([blank, high, blank, low], axis=0)
            if started:
                states[i, g] = tuple(ref[g] for ref in old)
            tiles += [(i, g, place, part) for place in wanted for part in halves]
    tiles.sort(key=lambda tile: tile[2:])

    def scores(tile):
        i, g, place, part = tile
        ref = kv_refs[place]
        context = ref.shape[0] > 2 * pairs
        keys = [ref[p] for p in range(pairs)]
        if context:
            keys.append(ref[2 * pairs, 0:span, :])
        keys = jnp.concatenate(keys, axis=0)
        keys = jnp.concatenate([keys, keys], axis=1)
        found = jnp.dot(keys, queries[i, g, part], preferred_element_type=jnp.float32)
        if context:
            rows = found.shape[0] - span
            found = jnp.concatenate([found[:rows], found[rows:] + offset * LOG2E], axis=0)
        return found

    def soften(tile, found):
        place = tile[:2]
        peak = jnp.max(found, axis=0, keepdims=True)
        old = states.get(place)
        if old is not None:
            peak = jnp.maximum(peak, old[0])
        shares = jnp.exp2(found - peak)
        total = jnp.sum(shares, axis=0, keepdims=True)
        shrink = None
        if old is not None:
            shrink = jnp.exp2(old[0] - peak)
            total = total + old[1] * shrink
        states[place] = (peak, total, old[2] if old is not None else None)
        return shares.astype(jnp.bfloat16), shrink

    def gather(tile, shares, shrink):
        ref = kv_refs[tile[2]]
        rows = slice(tile[3] * span, (tile[3] + 1) * span)
        values = [ref[pairs + p, rows, :] for p in range(pairs)]
        if ref.shape[0] > 2 * pairs:
            values.append(ref[2 * pairs, span : 2 * span, rows])
        weighted = jnp.dot(
            jnp.concatenate(values, axis=1), shares, preferred_element_type=jnp.float32
        )
        peak, total, old = states[tile[:2]]
        if shrink is not None:
            weighted = weighted + old * shrink
        states[tile[:2]] = (peak, total, weighted)

    following = scores(tiles[0])
    waiting = None
    for i, tile in enumerate(tiles):
        found = following
        if i + 1 < len(tiles):
            following = scores(tiles[i + 1])
        shares, shrink = soften(tile, found)
        if waiting:
            gather(*waiting)
        waiting = (tile, shares, shrink)
    gather(*waiting)
    for (i, g), (peak, total, weighted) in states.items():
        if last:
            out_ref = refs[i]
            attended = (weighted / total).astype(jnp.bfloat16)
            own_rows = out_ref.shape[2]
            for j in range(out_ref.shape[0]):
                out_ref[j, g * span : (g + 1) * span, :] = attended[
                    :, j * own_rows : (j + 1) * own_rows
                ]
        else:
            for ref, value in zip(refs[3 * i : 3 * i + 3], (peak, total, weighted)):
                ref[g] = value


def attend(sources, pieces, offset, last=False):
    probes = [source[0] for source in sources]
    lanes = 2 * 2 * probes[0].shape[2]
    span = probes[0].shape[1] // 2
    plan = [(source[1] is not None, source[2]) for source in sources]
    keys = sum(pieces[i].shape[0] * pieces[i].shape[1] // 2 for source in sources for i in source[2])
    inputs = probes + pieces
    for source in sources:
        inputs += list(source[1] or ())
    if last:
        out = [jax.ShapeDtypeStruct((4, 2 * span, probes[0].shape[2]), jnp.bfloat16)]
    else:
        stat = jax.ShapeDtypeStruct((2, 1, lanes), jnp.float32)
        out = [stat, stat, jax.ShapeDtypeStruct((2, span, lanes), jnp.float32)]

    def body(*refs):
        attention_body(plan, len(pieces), last, offset, *refs)

    found = kernel_call(
        body, out * len(sources), len(inputs), 40 * 2 * lanes * keys * span
    )(*inputs)
    size = len(out)
    return [found[size * i : size * (i + 1)] for i in range(len(sources))]


def output_body(latent_ref, mod_ref, weight_ref, *refs):
    out_ref, lhs_ref = refs[-2:]
    parts = refs[:-2]
    head_index = lax.axis_index("tp")
    side = lax.rem(lax.axis_index("sp"), 2)
    rows = parts[0].shape[0]
    for i, ref in enumerate(parts):
        j, flip = i % (len(parts) // 2), i // (len(parts) // 2)
        place = jnp.bitwise_xor(head_index, j) * 2 + jnp.bitwise_xor(side, flip)
        lhs_ref[pl.ds(pl.multiple_of(place * rows, rows), rows), :] = ref[...]
    lhs = lhs_ref[...].T
    columns = mod_ref.shape[2]
    for i in range(mod_ref.shape[0]):
        cut = slice(i * columns, (i + 1) * columns)
        branch = jnp.dot(lhs, weight_ref[:, cut], preferred_element_type=jnp.float32)
        gate = mod_ref[i, 4:5, :]
        out_ref[:, cut] = (latent_ref[:, cut].astype(jnp.float32) + gate * branch).astype(
            jnp.bfloat16
        )


def fast_device(*args):
    return inner_device(*args)


def xor_move(member, axis, mask):
    size = lax.axis_size(axis)
    return lax.ppermute(member, axis, [(i, i ^ mask) for i in range(size)])


def cross_move(member, mask):
    seq_split, head_split = lax.axis_size("sp"), lax.axis_size("tp")
    pairs = [
        (i * head_split + j, (i ^ 1) * head_split + (j ^ mask))
        for i in range(seq_split)
        for j in range(head_split)
    ]
    return lax.ppermute(member, ("sp", "tp"), pairs)


def tables(seq_index, head_index, own_rows, head_split):
    quarter = CHANNEL_SPAN // 4
    blocks = jnp.bitwise_xor(jnp.arange(head_split, dtype=jnp.int32), head_index)
    places = (
        seq_index * own_rows * head_split
        + blocks[:, None] * own_rows
        + jnp.arange(own_rows, dtype=jnp.int32)
    )
    inverse = rope_base ** (-jnp.arange(quarter, dtype=jnp.float32) / quarter)
    grid_row = (places // GRID_W).astype(jnp.float32)[:, None, :] * inverse[:, None]
    grid_col = (places % GRID_W).astype(jnp.float32)[:, None, :] * inverse[:, None]
    row_sine, col_sine = jnp.sin(grid_row), jnp.sin(grid_col)
    row_cosine, col_cosine = jnp.cos(grid_row), jnp.cos(grid_col)
    cosine = jnp.concatenate([row_cosine, row_cosine, col_cosine, col_cosine], axis=1)
    sine = jnp.concatenate([-row_sine, row_sine, -col_sine, col_sine], axis=1)
    return cosine, sine


def inner_device(
    latent,
    context,
    condition,
    context_condition,
    norm_gain,
    shift_weight,
    scale_weight,
    gate_weight,
    query_weight,
    key_weight,
    value_weight,
    query_gain,
    key_gain,
    output_weight,
):
    head_split = lax.axis_size("tp")
    seq_split = lax.axis_size("sp")
    seq_index = lax.axis_index("sp")
    head_index = lax.axis_index("tp")
    own_rows, depth = latent.shape
    ctx_rows = context.shape[0]
    tok_count = own_rows * head_split
    q_heads = query_weight.shape[1] // CHANNEL_SPAN
    kv_heads = key_weight.shape[1] // CHANNEL_SPAN

    part = opening(
        condition.reshape(1, depth),
        context_condition.reshape(1, depth),
        shift_weight,
        scale_weight,
        gate_weight,
    )
    far = xor_move(latent, "tp", 2)
    near = xor_move(latent, "tp", 1)
    mask = seq_split // 2
    while mask:
        other = xor_move(part, "sp", mask)
        if 2 * mask == seq_split:
            part = stash(part)
        part = combine(part, other, 10**11 if 2 * mask == seq_split else 10**6)
        mask //= 2
    both = xor_move(far, "tp", 1)
    modulation = lax.all_gather(part, "tp", axis=0, tiled=False)
    cosine, sine = tables(seq_index, head_index, own_rows, head_split)
    q_tiles = q_heads // kv_heads * head_split // 2
    kv_tiles = head_split
    tile = (own_rows, own_rows)
    keep_kv, keep_ctx, give_kv, hidden = kernel_call(
        lambda *refs: projection_body(kv_heads, *refs),
        [
            jax.ShapeDtypeStruct(shape, jnp.bfloat16)
            for shape in (
                (kv_tiles, *tile),
                tile,
                (kv_tiles + 1, *tile),
                (head_split, own_rows, depth),
            )
        ],
        12,
        8 * tok_count * depth * kv_heads * CHANNEL_SPAN,
        [pltpu.VMEM((kv_heads, kv_tiles + 1, *tile), jnp.bfloat16)],
    )(
        latent,
        context,
        key_weight,
        value_weight,
        near,
        far,
        both,
        modulation,
        norm_gain.reshape(1, depth),
        key_gain.reshape(1, CHANNEL_SPAN),
        cosine,
        sine,
    )
    keep_q, give_q = kernel_call(
        lambda *refs: probe_body(kv_heads, *refs),
        [jax.ShapeDtypeStruct((count, *tile), jnp.bfloat16) for count in (2 * q_tiles, q_tiles)],
        5,
        4 * tok_count * depth * q_heads * CHANNEL_SPAN,
        [pltpu.VMEM((kv_heads, q_tiles, *tile), jnp.bfloat16)],
    )(hidden, query_weight, query_gain.reshape(1, CHANNEL_SPAN), cosine, sine)
    offset = math.log(tok_count / (2.0 * ctx_rows))
    near = xor_move(give_kv, "sp", 1)
    near_q = xor_move(give_q, "sp", 1)
    up = xor_move(keep_kv, "sp", 2)
    down = xor_move(keep_kv, "sp", 6)
    near = merge(near, keep_ctx)
    near_down = xor_move(near, "sp", 6)
    near_up = xor_move(near, "sp", 2)
    across = xor_move(down, "sp", 2)
    near_across = xor_move(near_down, "sp", 2)
    (own,) = attend([(keep_q, None, [0])], [keep_kv], offset)
    near_q = ready(near_q)
    own, other = attend([(keep_q, own, [1]), (near_q, None, [0, 1])], [keep_kv, near], offset)
    own, other = attend([(keep_q, own, [0, 1]), (near_q, other, [0, 1])], [up, down], offset)
    own, other = attend(
        [(keep_q, own, [0]), (near_q, other, [0, 1])], [near_up, near_down], offset
    )
    own, other = attend(
        [(keep_q, own, [0, 1]), (near_q, other, [0])], [across, near_down], offset
    )
    ((other,),) = attend([(near_q, other, [0])], [near_across], offset, True)
    ((own,),) = attend([(keep_q, own, [0])], [near_across], offset, True)
    sent = [cross_move(other[j], j) for j in range(head_split)]
    parts = [own[0]] + [xor_move(own[j], "tp", j) for j in range(1, head_split)] + sent
    width = q_heads * CHANNEL_SPAN
    return kernel_call(
        output_body,
        jax.ShapeDtypeStruct(latent.shape, jnp.bfloat16),
        3 + len(parts),
        2 * own_rows * depth * width * head_split,
        [pltpu.VMEM((width * head_split, own_rows), jnp.bfloat16)],
    )(latent, modulation, output_weight, *parts)


def suits(mesh, latent, context, query_weight, key_weight):
    seq_split, head_split = mesh.shape["sp"], mesh.shape["tp"]
    own_rows = latent.shape[0] // (seq_split * head_split)
    ctx_rows = context.shape[0] // seq_split
    kv_heads = key_weight.shape[1] // CHANNEL_SPAN // head_split
    return (
        seq_split == 8
        and head_split == 4
        and own_rows == 2 * CHANNEL_SPAN
        and ctx_rows == CHANNEL_SPAN
        and kv_heads == 2
        and query_weight.shape[1] == 2 * key_weight.shape[1]
    )


def solution(mesh):
    in_specs = (
        P(("sp", "tp"), None),
        P("sp", None),
        P(),
        P(),
        P(),
        P("sp", "tp"),
        P("sp", "tp"),
        P("sp", "tp"),
        P(None, "tp"),
        P(None, "tp"),
        P(None, "tp"),
        P(),
        P(),
        P(),
    )
    out_specs = P(("sp", "tp"), None)

    def program(*args):
        fast = suits(mesh, args[0], args[1], args[8], args[9])
        step = jax.shard_map(
            fast_device if fast else general_device,
            mesh=mesh,
            in_specs=in_specs,
            out_specs=out_specs,
            check_vma=False,
        )
        return step(*args)

    return program
```
